128 devices in a mesh: ep: 64 (over z, y, x), tp: 2 (over core).
Axes of the slice: x: 4, y: 4, z: 4, core: 2. Of those that a mesh axis runs over, the one named last changes fastest.
Arguments:
- tokens: bfloat16 [1536, 2048], P('ep'), may hold values from -6 to 6
- norm_gain: bfloat16 [2048], replicated, may hold values from 0.099609375 to 1.8984375
- query_w: bfloat16 [2048, 1024], P(None, 'tp'), may hold values from -0.125 to 0.125
- key_w: bfloat16 [2048, 128], replicated, may hold values from -0.125 to 0.125
- value_w: bfloat16 [2048, 128], replicated, may hold values from -0.125 to 0.125
- forget_w: bfloat16 [2048, 16], replicated, may hold values from -0.125 to 0.125
- forget_bias: float32 [16], replicated, may hold values from 0 to 4
- query_gain: bfloat16 [64], replicated, may hold values from 0.099609375 to 1.8984375
- key_gain: bfloat16 [64], replicated, may hold values from 0.099609375 to 1.8984375
- cache_key: bfloat16 [1536, 2, 64, 1024], P('ep', 'tp'), may hold values from -6 to 6
- cache_value: bfloat16 [1536, 2, 64, 1024], P('ep', 'tp'), may hold values from -6 to 6
- cache_gate: float32 [1536, 16, 1024], P('ep', 'tp'), may hold values from -105 to 0, as said below
- cache_len: int32 [1536], P('ep'), may hold values from 256 to 1024
- out_w: bfloat16 [1024, 2048], P('tp'), may hold values from -0.1875 to 0.1875
- post_gain: bfloat16 [2048], replicated, may hold values from 0.099609375 to 1.8984375
- branch_gate: bfloat16 [2048], replicated, may hold values from -0.125 to 0.125
- dense_gate_w: bfloat16 [2048, 16384], P(None, ('ep', 'tp')), may hold values from -0.125 to 0.125
- dense_up_w: bfloat16 [2048, 16384], P(None, ('ep', 'tp')), may hold values from -1.3258252 to 1.3258252
- dense_down_w: bfloat16 [16384, 2048], P(('ep', 'tp')), may hold values from -0.046875 to 0.046875
- expert_choice: int32 [1536, 2], P('ep'), may hold values from 0 to 63, as said below
- route_weight: float32 [1536, 2], P('ep'), may hold values from 0.1 to 1
- expert_gate_w: bfloat16 [64, 2048, 1024], P('ep', None, 'tp'), may hold values from -0.125 to 0.125
- expert_up_w: bfloat16 [64, 2048, 1024], P('ep', None, 'tp'), may hold values from -0.125 to 0.125
- expert_down_w: bfloat16 [64, 1024, 2048], P('ep', 'tp'), may hold values from -0.1875 to 0.1875
Outputs:
- mixed_out: bfloat16 [1536, 2048], P('ep', 'tp')
- fresh_key: bfloat16 [1536, 2, 64], P('ep', 'tp')
- fresh_value: bfloat16 [1536, 2, 64], P('ep', 'tp')
- fresh_gate: float32 [1536, 16], P('ep', 'tp')
The draws below stay inside these ranges and needn't reach their ends.
Inputs may be any that keep to these rules, and one draw needn't show every extreme that they name: `cache_gate`: Non-increasing along positions. `expert_choice`: experts 16 * g to 16 * g + 15 form group g. A token names 2 different experts of one group. Among the 24 tokens of one index of ep, those at even offsets all choose one group and the others choose other groups; no expert is named more than 2 times by them, and some expert exactly 2 times.
All inputs are finite; a program needn't handle non-finite values.
Results may differ from the reference program's by a relative error of at most 0.014.
Values may be sent and summed in bfloat16 or wider, within the bound.
A program may use at most 128 MiB of HBM per device.

```python
import math
import jax
import jax.numpy as jnp
from jax import lax

D = 2048
HEADS = 16
KV = 2
HD = 64
FFE = 1024
FF2 = 16384
GROUPS = 4
TOPK = 2
SEQ_DEV = 24
STORED_SLOTS = 1024
BATCH_ENTRIES = 1536
EXPERTS = 64
EPG = 16
CAP = 2
N_EP = 64
N_TP = 2


def draw_cache_gate(key, part):
    derived_prng_seeds = jax.random.split(jax.random.fold_in(key, 11), 7)
    fast_share = 0.5
    is_fast = jax.random.uniform(derived_prng_seeds[0], (HEADS,)) < fast_share
    slow_rate = jax.random.uniform(derived_prng_seeds[1], (HEADS,), minval=0.3, maxval=0.8) / STORED_SLOTS
    fast_rate = 1.0 / jax.random.uniform(derived_prng_seeds[2], (HEADS,), minval=30.0, maxval=100.0)
    per_attender_fading = jnp.where(is_fast, fast_rate, slow_rate)
    batch_multiplier = jnp.exp(jax.random.uniform(derived_prng_seeds[3], (BATCH_ENTRIES, 1, 1), minval=math.log(0.6), maxval=math.log(1.6)))
    outer_level_logits = jax.random.uniform(derived_prng_seeds[4], (BATCH_ENTRIES, HEADS, STORED_SLOTS), minval=0.5, maxval=1.5)
    contiguous_first_slot = jax.random.randint(derived_prng_seeds[5], (BATCH_ENTRIES, 3), 0, STORED_SLOTS)
    contiguous_span = jax.random.uniform(derived_prng_seeds[6], (BATCH_ENTRIES, 3), minval=0.22, maxval=0.69)
    current_slot_offset = jnp.arange(STORED_SLOTS)[None, None, :]
    contiguous_tiles = jnp.sum(jnp.where(current_slot_offset == contiguous_first_slot[:, :, None], contiguous_span[:, :, None], 0.0), axis=1)
    increment_fading_exponent = -(per_attender_fading[None, :, None] * batch_multiplier * outer_level_logits) - contiguous_tiles[:, None, :]
    return jnp.cumsum(increment_fading_exponent, axis=2).astype(jnp.float32)


def draw_dense_up_w(key, part):
    base_key = jax.random.fold_in(key, 21)
    column = jnp.arange(FF2, dtype=jnp.float32) / FF2
    entries = jnp.clip(jax.random.normal(base_key, (D, FF2)), -6.0, 6.0)
    column_scale = jnp.exp(math.log(10.0) * column)
    return (entries * column_scale[None, :] * D ** (-0.5)).astype(jnp.bfloat16)


def draw_expert_choice(key, part):
    derived_prng_seeds = jax.random.split(jax.random.fold_in(key, 31), 3)
    blocks = BATCH_ENTRIES // SEQ_DEV
    even_group = jax.random.randint(derived_prng_seeds[0], (blocks, 1), 0, GROUPS)
    other_group = (even_group + 1 + jax.random.randint(derived_prng_seeds[1], (blocks, SEQ_DEV), 0, GROUPS - 1)) % GROUPS
    offset = jnp.arange(SEQ_DEV)[None, :]
    group_id = jnp.where(offset % 2 == 0, even_group, other_group)
    member_of = (group_id[:, :, None] == jnp.arange(GROUPS)[None, None, :]).astype(jnp.int32)
    rank_in = jnp.sum((jnp.cumsum(member_of, axis=1) - member_of) * member_of, axis=2)
    shift_by = jax.random.randint(derived_prng_seeds[2], (blocks, GROUPS), 0, EPG)
    start_at = jnp.sum(member_of * shift_by[:, None, :], axis=2)
    first_member = (start_at + rank_in) % EPG
    second = (first_member + 1) % EPG
    chosen = jnp.stack([group_id * EPG + first_member, group_id * EPG + second], axis=-1)
    return chosen.reshape(BATCH_ENTRIES, TOPK).astype(jnp.int32)


def place_ends(values, stream_key, least, high):
    dims = values.shape
    spot = [jax.random.randint(jax.random.fold_in(stream_key, axis), (), 0, dims[axis]) for axis in range(len(dims))]
    values = values.at[tuple(spot)].set(least)
    longest = dims.index(max(dims))
    spot[longest] = (spot[longest] + 1) % dims[longest]
    return values.at[tuple(spot)].set(high)


def levels(own_key, dims, cuts, smallest, top_value):
    level, own = 1.0, jax.random.fold_in(own_key, 6)
    for axis_at, blocks in cuts:
        steps = jnp.exp(jax.random.uniform(jax.random.fold_in(own, axis_at), (blocks,), jnp.float32, smallest / len(cuts), top_value / len(cuts)))
        level = level * jnp.repeat(steps, dims[axis_at] // blocks).reshape([-1 if axis == axis_at else 1 for axis in range(len(dims))])
    return level


def bell_draw(key, dims, scale, reach, pieces=(), held_as=jnp.bfloat16):
    values = scale * jax.random.normal(key, dims, jnp.float32)
    if pieces:
        values = values * levels(key, dims, pieces, -0.22, 0.18)
    return jnp.clip(values, -reach, reach).astype(held_as)


def setup_inputs(seed: int = 0) -> dict:
    streams_of = jax.random.split(jax.random.key(seed), 25)
    return {
        "tokens": bell_draw(streams_of[0], (BATCH_ENTRIES, D), 1.0, 6.0, ((0, 64),)),
        "norm_gain": jnp.clip(1.0 + 0.18 * jax.random.normal(streams_of[1], (D,), jnp.float32), 0.099609375, 1.8984375).astype(jnp.bfloat16),
        "query_w": bell_draw(streams_of[2], (D, HEADS * HD), D ** -0.5, 0.125, ((1, 2),)),
        "key_w": bell_draw(streams_of[3], (D, KV * HD), D ** -0.5, 0.125),
        "value_w": bell_draw(streams_of[4], (D, KV * HD), D ** -0.5, 0.125),
        "forget_w": bell_draw(streams_of[5], (D, HEADS), D ** -0.5, 0.125),
        "forget_bias": jnp.clip(jax.random.uniform(streams_of[6], (HEADS,), jnp.float32, 0.0, 4.0), 0.0, 4.0),
        "query_gain": jnp.clip(1.0 + 0.18 * jax.random.normal(streams_of[7], (HD,), jnp.float32), 0.099609375, 1.8984375).astype(jnp.bfloat16),
        "key_gain": jnp.clip(1.0 + 0.18 * jax.random.normal(streams_of[8], (HD,), jnp.float32), 0.099609375, 1.8984375).astype(jnp.bfloat16),
        "cache_key": bell_draw(streams_of[9], (BATCH_ENTRIES, KV, HD, STORED_SLOTS), 1.0, 6.0, ((0, 64), (1, 2))),
        "cache_value": bell_draw(streams_of[10], (BATCH_ENTRIES, KV, HD, STORED_SLOTS), 1.0, 6.0, ((0, 64), (1, 2))),
        "cache_gate": draw_cache_gate(jax.random.fold_in(streams_of[24], 71), 0),
        "cache_len": place_ends(jax.random.randint(streams_of[12], (BATCH_ENTRIES,), STORED_SLOTS // 4, STORED_SLOTS + 1), jax.random.fold_in(streams_of[12], 1), STORED_SLOTS // 4, STORED_SLOTS).astype(jnp.int32),
        "out_w": bell_draw(streams_of[13], (HEADS * HD, D), (HEADS * HD) ** -0.5, 0.1875, ((0, 2),)),
        "post_gain": jnp.clip(1.0 + 0.18 * jax.random.normal(streams_of[14], (D,), jnp.float32), 0.099609375, 1.8984375).astype(jnp.bfloat16),
        "branch_gate": bell_draw(streams_of[15], (D,), D ** -0.5, 0.125),
        "dense_gate_w": bell_draw(streams_of[16], (D, FF2), D ** -0.5, 0.125, ((1, 128),)),
        "dense_up_w": draw_dense_up_w(jax.random.fold_in(streams_of[24], 71), 0),
        "dense_down_w": bell_draw(streams_of[18], (FF2, D), FF2 ** -0.5, 0.046875, ((0, 128),)),
        "expert_choice": draw_expert_choice(jax.random.fold_in(streams_of[24], 71), 0),
        "route_weight": jnp.clip(0.1 + 0.9 * jax.random.uniform(streams_of[20], (BATCH_ENTRIES, TOPK), jnp.float32) ** levels(streams_of[20], (BATCH_ENTRIES, TOPK), ((0, 64),), -0.2, 0.2), 0.1, 1.0),
        "expert_gate_w": bell_draw(streams_of[21], (EXPERTS, D, FFE), D ** -0.5, 0.125, ((0, 64), (2, 2))),
        "expert_up_w": bell_draw(streams_of[22], (EXPERTS, D, FFE), D ** -0.5, 0.125, ((0, 64), (2, 2))),
        "expert_down_w": bell_draw(streams_of[23], (EXPERTS, FFE, D), FFE ** -0.5, 0.1875, ((0, 64), (1, 2))),
    }


norm_eps = 1e-06

def rms_scale(values, gain_vec):
    mean_square = lax.optimization_barrier(jnp.mean(values * values, axis=-1, keepdims=True))
    return values * lax.rsqrt(mean_square + norm_eps) * gain_vec

def rounded(values):
    return lax.optimization_barrier(values.astype(jnp.bfloat16)).astype(jnp.float32)

def attend(block_in):
    queries, new_keys, new_values, log_forget, keys_cached, values_cached, gates_cached, lengths = block_in
    row_count = queries.shape[0]
    repeat = HEADS // KV
    score_scale = HD ** (-0.5)
    grouped = queries.reshape(row_count, KV, repeat, HD).astype(jnp.float32)
    scores = jnp.einsum('sgrd,sgdl->sgrl', grouped, keys_cached.astype(jnp.float32)) * score_scale
    own_score = jnp.einsum('sgrd,sgd->sgr', grouped, new_keys.astype(jnp.float32)) * score_scale
    current_slot_offset = lax.broadcasted_iota(jnp.int32, (row_count, STORED_SLOTS), 1)
    at_last = (current_slot_offset == lengths[:, None] - 1)[:, None, :]
    previous = lax.optimization_barrier(jnp.sum(jnp.where(at_last, gates_cached, jnp.zeros_like(gates_cached)), axis=2))
    current = previous + log_forget
    decay_bias = (current[:, :, None] - gates_cached).reshape(row_count, KV, repeat, STORED_SLOTS)
    is_valid = (current_slot_offset < lengths[:, None])[:, None, None, :]
    logits = jnp.where(is_valid, scores + decay_bias, -jnp.inf)
    top_logit = jnp.maximum(lax.optimization_barrier(jnp.max(logits, axis=3)), own_score)
    weights = jnp.exp(logits - top_logit[..., None])
    own_weight = jnp.exp(own_score - top_logit)
    total_weight = lax.optimization_barrier(jnp.sum(weights, axis=3)) + own_weight
    cache_probs = (weights / total_weight[..., None]).astype(jnp.bfloat16)
    own_prob = (own_weight / total_weight).astype(jnp.bfloat16)
    mixed_heads = jnp.einsum('sgrl,sgdl->sgrd', cache_probs.astype(jnp.float32), values_cached.astype(jnp.float32))
    mixed_heads = mixed_heads + own_prob.astype(jnp.float32)[..., None] * new_values.astype(jnp.float32)[:, :, None, :]
    return (mixed_heads.reshape(row_count, HEADS * HD).astype(jnp.bfloat16), current)

def reference(tokens, norm_gain, query_w, key_w, value_w, forget_w, forget_bias, query_gain, key_gain, cache_key, cache_value, cache_gate, cache_len, out_w, post_gain, branch_gate, dense_gate_w, dense_up_w, dense_down_w, expert_choice, route_weight, expert_gate_w, expert_up_w, expert_down_w):
    token_count = tokens.shape[0]
    resid_in = tokens.astype(jnp.float32)
    normed = rms_scale(resid_in, norm_gain.astype(jnp.float32)).astype(jnp.bfloat16)
    queries = jnp.dot(normed, query_w, preferred_element_type=jnp.float32).reshape(token_count, HEADS, HD)
    queries = rms_scale(queries, query_gain.astype(jnp.float32)).astype(jnp.bfloat16)
    fresh_key = jnp.dot(normed, key_w, preferred_element_type=jnp.float32).reshape(token_count, KV, HD)
    fresh_key = rms_scale(fresh_key, key_gain.astype(jnp.float32)).astype(jnp.bfloat16)
    fresh_value = jnp.dot(normed, value_w, preferred_element_type=jnp.float32).astype(jnp.bfloat16).reshape(token_count, KV, HD)
    log_forget = jax.nn.log_sigmoid(jnp.dot(normed, forget_w, preferred_element_type=jnp.float32) + forget_bias)

    def blocks(array_in):
        return array_in.reshape((N_EP, SEQ_DEV) + array_in.shape[1:])
    heads_out, fresh_gate = lax.map(attend, tuple((blocks(array_in) for array_in in (queries, fresh_key, fresh_value, log_forget, cache_key, cache_value, cache_gate, cache_len))))
    heads_out = heads_out.reshape(token_count, HEADS * HD)
    fresh_gate = fresh_gate.reshape(token_count, HEADS)
    head_groups = heads_out.reshape(token_count, N_TP, -1)
    out_parts = out_w.reshape(N_TP, -1, D)
    attn_sum = jnp.zeros((token_count, D), jnp.float32)
    for group_index in range(N_TP):
        attn_sum = attn_sum + rounded(jnp.dot(head_groups[:, group_index], out_parts[group_index], preferred_element_type=jnp.float32))
    resid_out = rounded(resid_in + attn_sum)
    post_norm = rms_scale(resid_out, post_gain.astype(jnp.float32)).astype(jnp.bfloat16)
    branch = jax.nn.sigmoid(jnp.dot(post_norm, branch_gate, preferred_element_type=jnp.float32))
    hidden = jax.nn.silu(jnp.dot(post_norm, dense_gate_w, preferred_element_type=jnp.float32)) * jnp.dot(post_norm, dense_up_w, preferred_element_type=jnp.float32)
    inverse = lax.rsqrt(lax.optimization_barrier(jnp.mean(hidden * hidden, axis=1)) + norm_eps)
    dense_out = rounded(jnp.dot(hidden.astype(jnp.bfloat16), dense_down_w, preferred_element_type=jnp.float32) * inverse[:, None])
    route_total = token_count * TOPK
    route_ids = expert_choice.reshape(-1).astype(jnp.int32)
    limit = N_EP * CAP

    def one_expert(routed_acc, slices):
        gate_mat, up_mat, down_mat, expert_index = slices
        picked = jnp.nonzero(route_ids == expert_index, size=limit, fill_value=route_total)[0].astype(jnp.int32)
        slot_rows = post_norm[jnp.minimum(picked, route_total - 1) // TOPK]
        gate_val = jnp.dot(slot_rows, gate_mat, preferred_element_type=jnp.float32)
        up_val = jnp.dot(slot_rows, up_mat, preferred_element_type=jnp.float32)
        activated = (jax.nn.silu(gate_val) * up_val).astype(jnp.bfloat16)
        act_parts = activated.reshape(limit, N_TP, -1)
        down_parts = down_mat.reshape(N_TP, -1, D)
        expert_out = jnp.zeros((limit, D), jnp.float32)
        for group_index in range(N_TP):
            expert_out = expert_out + rounded(jnp.dot(act_parts[:, group_index], down_parts[group_index], preferred_element_type=jnp.float32))
        routed_acc = routed_acc.at[picked].set(rounded(expert_out), mode='drop')
        return (routed_acc, None)
    routed, _ = lax.scan(one_expert, jnp.zeros((route_total, D), jnp.float32), (expert_gate_w, expert_up_w, expert_down_w, jnp.arange(N_EP, dtype=jnp.int32)))
    expert_sum = lax.optimization_barrier(jnp.sum(route_weight[:, :, None] * routed.reshape(token_count, TOPK, D), axis=1))
    mixed_out = (resid_out + expert_sum + branch[:, None] * dense_out).astype(jnp.bfloat16)
    return (mixed_out, fresh_key, fresh_value, fresh_gate)
```

```python
import math
import functools

import jax
import jax.numpy as jnp
from jax import lax
from jax.experimental import pallas as pl
from jax.experimental.pallas import tpu as pltpu
from jax.sharding import PartitionSpec as P

FF2 = 16384
norm_eps = 1e-06
MESH = pl.DeviceIdType.MESH
f32, bf16 = jnp.float32, jnp.bfloat16


class Sems:
    def __init__(self, send, recv):
        self.send, self.recv, self.n = send, recv, 0
        self.sent = []

    def copy(self, src, dst, device):
        i = self.n
        self.n += 1
        cp = pltpu.make_async_remote_copy(
            src_ref=src,
            dst_ref=dst,
            send_sem=self.send.at[i],
            recv_sem=self.recv.at[i],
            device_id=device,
            device_id_type=MESH,
        )
        cp.start()
        self.sent.append(cp)
        return cp


def silu(v):
    return v / (1.0 + jnp.exp(-v))


def layer_kernel(
    partial_ref, tokens_ref, gain_ref, bgate_ref, meta_ref, comb_ref,
    dg_h, du_h, dd_h, eg_h, eu_h, ed_h,
    out_ref,
    partner_part, resid_s, pn_s, a1, xs, hid, wgu, wd, eg, eu, ed,
    meta_all, meta_tab, xg, dens, rl, rr, ql, qr, sl, sr, t2, r2, t3, r3,
    sq, sq1, sq2, sq2r, sq3, sq3r, ep_send, ep_recv, ret_f, ret_b, back,
    send_sem, recv_sem, load_sem, meta_sems, back_sems,
):
    me = lax.axis_index("ep")
    core = lax.axis_index("tp")
    other = 1 - core
    coords = (me % 4, (me // 4) % 4, me // 16)
    weights = (1, 4, 16)
    partner = (me, other)
    half = pl.multiple_of(core * 1024, 1024)
    ohalf = pl.multiple_of(other * 1024, 1024)
    ccol = pl.multiple_of(core * 128, 128)

    def peer(dim, k):
        v = coords[dim]
        return (me + (((v + k) % 4) - v) * weights[dim], core)

    sems = Sems(send_sem, recv_sem)

    loads = []
    for i, (src, dst) in enumerate((
        (dg_h, wgu.at[:, pl.ds(0, 128)]),
        (du_h, wgu.at[:, pl.ds(128, 128)]),
        (dd_h.at[:, pl.ds(half, 1024)], wd.at[pl.ds(ccol, 128)]),
        (eg_h, eg),
        (eu_h, eu),
        (ed_h, ed),
    )):
        cp = pltpu.make_async_copy(src, dst, load_sem.at[i])
        cp.start()
        loads.append(cp)

    barrier = pltpu.get_barrier_semaphore()
    pl.semaphore_signal(barrier, inc=1, device_id=partner, device_id_type=MESH)

    @pl.loop(1, 64)
    def _(i):
        pl.semaphore_signal(
            barrier, inc=1, device_id=((me + i) % 64, core), device_id_type=MESH
        )

    pl.semaphore_wait(barrier, 64)

    part_cp = sems.copy(partial_ref, partner_part, partner)
    wd_cp = sems.copy(dd_h.at[:, pl.ds(ohalf, 1024)], wd.at[pl.ds(ccol, 128)], partner)

    def meta_copy(d):
        return pltpu.make_async_remote_copy(
            src_ref=meta_ref,
            dst_ref=meta_all.at[me],
            send_sem=meta_sems.at[0],
            recv_sem=meta_sems.at[1],
            device_id=(d, core),
            device_id_type=MESH,
        )

    part_cp.wait_recv()
    attn = partial_ref[...].astype(f32) + partner_part[...].astype(f32)
    resid = (tokens_ref[...].astype(f32) + attn).astype(bf16).astype(f32)
    resid_s[...] = resid
    mean_square = jnp.mean(resid * resid, axis=-1, keepdims=True)
    gain = gain_ref[...].astype(f32)[None]
    post = (resid * lax.rsqrt(mean_square + norm_eps) * gain).astype(bf16)
    pn_s[...] = post
    a1[:, 0] = pn_s[:, :, pl.ds(half, 1024)]

    g1 = [
        [sems.copy(a1.at[p, 0], a1.at[p, 4 - k], peer(p, k)) for k in (1, 3, 2)]
        for p in range(3)
    ]

    @pl.loop(1, 64)
    def _(i):
        meta_copy((me + i) % 64).start()

    meta_all[me] = meta_ref[...]
    branch = jax.nn.sigmoid(
        jnp.sum(post.astype(f32) * bgate_ref[...].astype(f32)[None], axis=-1, keepdims=True)
    )

    g2 = []
    for p in range(3):
        for cp in g1[p]:
            cp.wait_recv()
        for pair in range(2):
            rows = jnp.concatenate(
                [a1[p, 2 * pair].astype(f32), a1[p, 2 * pair + 1].astype(f32)], axis=0
            )
            xs[core, 0, pl.ds(p * 128 + pair * 16, 16)] = rows.astype(bf16)
        line = xs.at[core, 0, pl.ds(p * 128, 32)]
        g2.append([
            sems.copy(line, xs.at[core, 0, pl.ds(p * 128 + (4 - k) * 32, 32)], peer((p + 1) % 3, k))
            for k in (1, 3, 2)
        ])

    g3, d2d = [], [[] for _ in range(4)]

    def share(slot, p, start, size):
        view = xs.at[core, slot, pl.ds(p * 128 + start, size)]
        d2d[slot].append(sems.copy(view, view, partner))

    for p in range(3):
        for cp in g2[p]:
            cp.wait_recv()
        cdim = (p + 2) % 3
        rows = pl.ds(p * 128, 128)
        g3.append((
            sems.copy(xs.at[core, 0, rows], xs.at[core, 1, rows], peer(cdim, 1)),
            sems.copy(xs.at[core, 0, rows], xs.at[core, 2, rows], peer(cdim, 3)),
        ))
        share(0, p, 0, 128)

    pltpu.make_async_copy(
        meta_all.at[pl.ds(0, 63)], meta_all.at[pl.ds(0, 63)], meta_sems.at[1]
    ).wait()
    for d in range(64):
        meta_tab[pl.ds(d, 1), :] = meta_all[d]
    table = meta_tab[...]
    lane = lax.broadcasted_iota(jnp.int32, (64, 128), 1)
    dev = lax.broadcasted_iota(jnp.int32, (64, 1), 0)
    shift = [((dev >> s) - coords[i]) & 3 for i, s in enumerate((0, 2, 4))]
    starts = []
    for p in range(3):
        ka, kb, kc = shift[p], shift[(p + 1) % 3], shift[(p + 2) % 3]
        slot = jnp.where(kc == 0, 0, jnp.where(kc == 1, 2, jnp.where(kc == 2, 3, 1)))
        starts.append(slot * 384 + p * 128 + kb * 32 + ka * 8)
    row_ids = []
    for s in range(2):
        want = (me * 2 + s).astype(f32)
        tok = jnp.sum(jnp.where(table == want, (lane >> 1) + 1, 0), axis=1, keepdims=True) - 1
        start = jnp.where(tok < 8, starts[0], jnp.where(tok < 16, starts[1], starts[2]))
        row_ids.append(jnp.where(tok < 0, -1, start + (tok & 7)))
    row_id = jnp.concatenate(row_ids, axis=0)
    cols = lax.broadcasted_iota(jnp.int32, (128, 384), 1)

    def select(slot):
        pick = jnp.where(row_id == cols + slot * 384, 1.0, 0.0).astype(bf16)
        for h in range(2):
            got = jnp.dot(pick, xs[h, slot], preferred_element_type=f32)
            if slot:
                got = xg[h] + got
            xg[h] = got

    h_cp = [None] * 4

    def up_proj(slot):
        v = jnp.dot(xs[0, slot], wgu[pl.ds(0, 1024)], preferred_element_type=f32)
        v = v + jnp.dot(xs[1, slot], wgu[pl.ds(1024, 1024)], preferred_element_type=f32)
        hid[slot, :, pl.ds(ccol, 128)] = (silu(v[:, :128]) * v[:, 128:]).astype(bf16)
        view = hid.at[slot, :, pl.ds(ccol, 128)]
        h_cp[slot] = sems.copy(view, view, partner)

    ones = jnp.ones((8, 256), bf16)

    def down_proj(slot):
        h_cp[slot].wait_recv()
        h = hid[slot]
        hf = h.astype(f32)
        dens[slot] = jnp.dot(h, wd[...], preferred_element_type=f32).astype(bf16)
        s = lax.dot_general(
            ones, (hf * hf).astype(bf16), (((1,), (1,)), ((), ())), preferred_element_type=f32
        )
        for p in range(3):
            sq[slot, p] = s[0:1, p * 128:(p + 1) * 128]

    def arrive(slot):
        for cp in d2d[slot]:
            cp.wait_recv()

    loads[0].wait()
    loads[1].wait()
    arrive(0)
    up_proj(0)
    select(0)

    relay = []
    for p in range(3):
        cdim = (p + 2) % 3
        g3[p][0].wait_recv()
        rows = pl.ds(p * 128, 64)
        relay.append(sems.copy(xs.at[core, 1, rows], xs.at[core, 3, rows], peer(cdim, 1)))
        share(1, p, 0, 128)
        g3[p][1].wait_recv()
        rows = pl.ds(p * 128 + 64, 64)
        relay.append(sems.copy(xs.at[core, 2, rows], xs.at[core, 3, rows], peer(cdim, 3)))
        share(2, p, 0, 128)

    arrive(1)
    up_proj(1)
    arrive(2)
    up_proj(2)
    loads[2].wait()
    wd_cp.wait_recv()
    select(1)
    down_proj(1)
    select(2)
    down_proj(2)

    s1 = []
    for p in range(3):
        cdim = (p + 2) % 3
        s1.append([
            sems.copy(dens.at[2, pl.ds(p * 128 + 64, 64)], rl.at[p, 1], peer(cdim, 1)),
            sems.copy(dens.at[1, pl.ds(p * 128, 64)], rr.at[p, 0], peer(cdim, 3)),
        ])

    for p in range(3):
        relay[2 * p].wait_recv()
        share(3, p, 0, 64)
        relay[2 * p + 1].wait_recv()
        share(3, p, 64, 64)
    arrive(3)
    up_proj(3)
    select(3)
    down_proj(3)
    far = []
    for p in range(3):
        cdim = (p + 2) % 3
        far.append((
            sems.copy(dens.at[3, pl.ds(p * 128, 64)], ql.at[p], peer(cdim, 1)),
            sems.copy(dens.at[3, pl.ds(p * 128 + 64, 64)], qr.at[p], peer(cdim, 3)),
        ))
        s1[p] += [
            sems.copy(sq.at[2, p], sq1.at[p, 0], peer(cdim, 1)),
            sems.copy(sq.at[1, p], sq1.at[p, 1], peer(cdim, 3)),
            sems.copy(sq.at[3, p], sq1.at[p, 2], peer(cdim, 2)),
        ]

    for i in (3, 4, 5):
        loads[i].wait()
    x0, x1 = xg[0].astype(bf16), xg[1].astype(bf16)
    gate = jnp.dot(x0, eg[pl.ds(0, 1024)], preferred_element_type=f32)
    gate = gate + jnp.dot(x1, eg[pl.ds(1024, 1024)], preferred_element_type=f32)
    up = jnp.dot(x0, eu[pl.ds(0, 1024)], preferred_element_type=f32)
    up = up + jnp.dot(x1, eu[pl.ds(1024, 1024)], preferred_element_type=f32)
    act = (silu(gate) * up).astype(bf16)
    ep_send[...] = jnp.dot(act, ed[:, pl.ds(ohalf, 1024)], preferred_element_type=f32).astype(bf16)
    ep_cp = sems.copy(ep_send, ep_recv, partner)
    mine = jnp.dot(act, ed[:, pl.ds(half, 1024)], preferred_element_type=f32).astype(bf16)

    for p in range(3):
        cdim = (p + 2) % 3
        far[p][0].wait_recv()
        sl[p] = (dens[2, pl.ds(p * 128, 64)].astype(f32) + ql[p].astype(f32)).astype(bf16)
        s1[p].append(sems.copy(sl.at[p], rl.at[p, 0], peer(cdim, 1)))
        far[p][1].wait_recv()
        sr[p] = (dens[1, pl.ds(p * 128 + 64, 64)].astype(f32) + qr[p].astype(f32)).astype(bf16)
        s1[p].append(sems.copy(sr.at[p], rr.at[p, 1], peer(cdim, 3)))

    ep_cp.wait_recv()
    rows = (mine.astype(f32) + ep_recv[...].astype(f32)).astype(bf16).astype(f32)
    for s in range(2):
        for t in range(8):
            ret_f[pl.ds(s * 8 + t, 64, stride=16), :] = rows[s * 64:(s + 1) * 64, t * 128:(t + 1) * 128]
    ret_b[...] = ret_f[...].astype(bf16).reshape(64, 16, 128)

    def back_copy(d):
        return pltpu.make_async_remote_copy(
            src_ref=ret_b.at[d],
            dst_ref=back.at[me],
            send_sem=back_sems.at[0],
            recv_sem=back_sems.at[1],
            device_id=(d, core),
            device_id_type=MESH,
        )

    @pl.loop(1, 64)
    def _(i):
        back_copy((me + i) % 64).start()

    back[me] = ret_b[me]
    down_proj(0)

    s2 = []
    for p in range(3):
        for cp in s1[p]:
            cp.wait_recv()
        total = dens[0, pl.ds(p * 128, 128)].astype(f32)
        total = total + jnp.concatenate([rl[p, 0], rl[p, 1]], axis=0).astype(f32)
        total = total + jnp.concatenate([rr[p, 0], rr[p, 1]], axis=0).astype(f32)
        for k in range(4):
            t2[p, k] = total[k * 32:(k + 1) * 32].astype(bf16)
        v = sq[0, p] + sq1[p, 0] + sq1[p, 1] + sq1[p, 2]
        sq2[p, 0] = v
        for k in range(1, 4):
            sq2[p, k] = pltpu.roll(v, 128 - 32 * k, 1)
        s2.append([
            sems.copy(t2.at[p, k], r2.at[p, k - 1], peer((p + 1) % 3, k)) for k in (1, 3, 2)
        ] + [
            sems.copy(sq2.at[p, k], sq2r.at[p, k - 1], peer((p + 1) % 3, k)) for k in (1, 3, 2)
        ])

    pltpu.make_async_copy(back.at[pl.ds(0, 63)], back.at[pl.ds(0, 63)], back_sems.at[1]).wait()
    ret_f[...] = back[...].reshape(1024, 128).astype(f32)
    mixes = []
    for t in range(8):
        m = 0.0
        for s in range(2):
            m = m + jnp.dot(
                comb_ref[s], ret_f[pl.ds(s * 8 + t, 64, stride=16), :],
                preferred_element_type=f32, precision=lax.Precision.HIGHEST,
            )
        mixes.append(m)
    expert_sum = jnp.concatenate(mixes, axis=1)

    s3 = []
    for p in range(3):
        for cp in s2[p]:
            cp.wait_recv()
        total = t2[p, 0].astype(f32)
        for k in range(3):
            total = total + r2[p, k].astype(f32)
        for k in range(4):
            t3[p, k] = total[k * 8:(k + 1) * 8].astype(bf16)
        v = sq2[p, 0] + sq2r[p, 0] + sq2r[p, 1] + sq2r[p, 2]
        sq3[p, 0] = v
        for k in range(1, 4):
            sq3[p, k] = pltpu.roll(v, 128 - 8 * k, 1)
        s3.append([
            sems.copy(t3.at[p, k], r3.at[p, k - 1], peer(p, k)) for k in (1, 3, 2)
        ] + [
            sems.copy(sq3.at[p, k], sq3r.at[p, k - 1], peer(p, k)) for k in (1, 3, 2)
        ])

    eye = lax.broadcasted_iota(jnp.int32, (8, 128), 0) == lax.broadcasted_iota(jnp.int32, (8, 128), 1)
    for p in range(3):
        for cp in s3[p]:
            cp.wait_recv()
        total = t3[p, 0].astype(f32)
        v = sq3[p, 0]
        for k in range(3):
            total = total + r3[p, k].astype(f32)
            v = v + sq3r[p, k]
        square = jnp.sum(jnp.where(eye, v, 0.0), axis=1, keepdims=True)
        dense = (total * lax.rsqrt(square / FF2 + norm_eps)).astype(bf16).astype(f32)
        mixed = resid_s[p, :, pl.ds(half, 1024)] + expert_sum[p * 8:(p + 1) * 8] + branch[p] * dense
        out_ref[p] = mixed.astype(bf16)

    for cp in sems.sent:
        cp.wait_send()
    pltpu.make_async_copy(
        meta_all.at[pl.ds(0, 63)], meta_all.at[pl.ds(0, 63)], meta_sems.at[0]
    ).wait()
    pltpu.make_async_copy(back.at[pl.ds(0, 63)], back.at[pl.ds(0, 63)], back_sems.at[0]).wait()


def layer_tail(partial, tokens, post_gain, branch_gate, meta, comb, dg, du, dd, eg, eu, ed):
    V = pltpu.VMEM
    vm = pl.BlockSpec(memory_space=pltpu.VMEM)
    hbm = pl.BlockSpec(memory_space=pl.ANY)
    scratch = [
        V((3, 8, 2048), bf16),
        V((3, 8, 2048), f32),
        V((3, 8, 2048), bf16),
        V((3, 4, 8, 1024), bf16),
        V((2, 4, 384, 1024), bf16),
        V((4, 384, 256), bf16),
        V((2048, 256), bf16),
        V((256, 1024), bf16),
        V((2048, 512), bf16),
        V((2048, 512), bf16),
        V((512, 2048), bf16),
        V((64, 1, 128), f32),
        V((64, 128), f32),
        V((2, 128, 1024), f32),
        V((4, 384, 1024), bf16),
        V((3, 2, 64, 1024), bf16),
        V((3, 2, 64, 1024), bf16),
        V((3, 64, 1024), bf16),
        V((3, 64, 1024), bf16),
        V((3, 64, 1024), bf16),
        V((3, 64, 1024), bf16),
        V((3, 4, 32, 1024), bf16),
        V((3, 3, 32, 1024), bf16),
        V((3, 4, 8, 1024), bf16),
        V((3, 3, 8, 1024), bf16),
        V((4, 3, 1, 128), f32),
        V((3, 3, 1, 128), f32),
        V((3, 4, 1, 128), f32),
        V((3, 3, 1, 128), f32),
        V((3, 4, 1, 128), f32),
        V((3, 3, 1, 128), f32),
        V((128, 1024), bf16),
        V((128, 1024), bf16),
        V((1024, 128), f32),
        V((64, 16, 128), bf16),
        V((64, 16, 128), bf16),
        pltpu.SemaphoreType.DMA((128,)),
        pltpu.SemaphoreType.DMA((128,)),
        pltpu.SemaphoreType.DMA((6,)),
        pltpu.SemaphoreType.DMA((2,)),
        pltpu.SemaphoreType.DMA((2,)),
    ]
    return pl.pallas_call(
        layer_kernel,
        out_shape=jax.ShapeDtypeStruct((3, 8, 1024), bf16),
        in_specs=[vm] * 6 + [hbm] * 6,
        out_specs=vm,
        scratch_shapes=scratch,
        compiler_params=pltpu.CompilerParams(
            collective_id=0, has_side_effects=True, vmem_limit_bytes=56 * 1024 * 1024
        ),
    )(partial, tokens, post_gain, branch_gate, meta, comb, dg, du, dd, eg, eu, ed)


def rms_scale(values, gain_vec):
    mean_square = jnp.mean(values * values, axis=-1, keepdims=True)
    return values * lax.rsqrt(mean_square + norm_eps) * gain_vec


def body(
    tokens,
    norm_gain,
    query_w,
    key_w,
    value_w,
    forget_w,
    forget_bias,
    query_gain,
    key_gain,
    cache_key,
    cache_value,
    cache_gate,
    cache_len,
    out_w,
    post_gain,
    branch_gate,
    dense_gate_w,
    dense_up_w,
    dense_down_w,
    expert_choice,
    route_weight,
    expert_gate_w,
    expert_up_w,
    expert_down_w,
):
    seq_count = tokens.shape[0]
    model_width = tokens.shape[1]
    heads_local = cache_gate.shape[1]
    kv_local = cache_key.shape[1]
    head_size = cache_key.shape[2]
    cache_span = cache_key.shape[3]
    ep_count = lax.axis_size("ep")
    tp_rank = lax.axis_index("tp")
    score_scale = head_size ** (-0.5)
    resid_in = tokens.astype(jnp.float32)
    normed = rms_scale(resid_in, norm_gain.astype(jnp.float32)).astype(jnp.bfloat16)
    queries = jnp.dot(normed, query_w, preferred_element_type=jnp.float32).reshape(
        seq_count, heads_local, head_size
    )
    queries = rms_scale(queries, query_gain.astype(jnp.float32)).astype(jnp.bfloat16)
    keys_all = jnp.dot(normed, key_w, preferred_element_type=jnp.float32).reshape(
        seq_count, -1, head_size
    )
    keys_all = rms_scale(keys_all, key_gain.astype(jnp.float32)).astype(jnp.bfloat16)
    values_all = (
        jnp.dot(normed, value_w, preferred_element_type=jnp.float32)
        .astype(jnp.bfloat16)
        .reshape(seq_count, -1, head_size)
    )
    fresh_key = lax.dynamic_slice_in_dim(keys_all, tp_rank * kv_local, kv_local, 1)
    fresh_value = lax.dynamic_slice_in_dim(values_all, tp_rank * kv_local, kv_local, 1)
    forget_all = jax.nn.log_sigmoid(
        jnp.dot(normed, forget_w, preferred_element_type=jnp.float32) + forget_bias
    )
    log_forget = lax.dynamic_slice_in_dim(forget_all, tp_rank * heads_local, heads_local, 1)
    repeat = heads_local // kv_local
    grouped = queries.reshape(seq_count, kv_local, repeat, head_size)
    scores = (
        jnp.einsum("sgrd,sgdl->sgrl", grouped, cache_key, preferred_element_type=jnp.float32)
        * score_scale
    )
    own_score = (
        jnp.einsum("sgrd,sgd->sgr", grouped, fresh_key, preferred_element_type=jnp.float32)
        * score_scale
    )
    current_slot_offset = lax.broadcasted_iota(jnp.int32, (seq_count, cache_span), 1)
    at_last = (current_slot_offset == cache_len[:, None] - 1)[:, None, :]
    previous = jnp.sum(jnp.where(at_last, cache_gate, jnp.zeros_like(cache_gate)), axis=2)
    current = previous + log_forget
    decay_bias = (current[:, :, None] - cache_gate).reshape(seq_count, kv_local, repeat, cache_span)
    is_valid = (current_slot_offset < cache_len[:, None])[:, None, None, :]
    logits = jnp.where(is_valid, scores + decay_bias, -jnp.inf)
    top_logit = jnp.maximum(jnp.max(logits, axis=3), own_score)
    weights = jnp.exp(logits - top_logit[..., None])
    own_weight = jnp.exp(own_score - top_logit)
    total_weight = jnp.sum(weights, axis=3) + own_weight
    cache_probs = (weights / total_weight[..., None]).astype(jnp.bfloat16)
    own_prob = (own_weight / total_weight).astype(jnp.bfloat16)
    mixed_heads = jnp.einsum(
        "sgrl,sgdl->sgrd", cache_probs, cache_value, preferred_element_type=jnp.float32
    )
    mixed_heads = (
        mixed_heads
        + own_prob.astype(jnp.float32)[..., None] * fresh_value.astype(jnp.float32)[:, :, None, :]
    )
    attn_heads = mixed_heads.reshape(seq_count, heads_local * head_size).astype(jnp.bfloat16)
    partial_value = jnp.dot(attn_heads, out_w, preferred_element_type=jnp.float32)
    capacity = 2
    route_ids = expert_choice.reshape(-1)
    member = (route_ids[:, None] == jnp.arange(ep_count)[None, :]).astype(jnp.int32)
    slot_index = jnp.sum((jnp.cumsum(member, axis=0) - member) * member, axis=1)
    target = route_ids * capacity + slot_index
    meta = jnp.pad(target.astype(jnp.float32), (0, 128 - target.shape[0]), constant_values=-1.0)
    target = target.reshape(seq_count, 2)
    places = jnp.arange(ep_count)[None, None, :] * 2 + jnp.arange(2)[:, None, None]
    comb = jnp.sum(
        jnp.where(target.T[:, None, :, None] == places[None], route_weight.T[:, None, :, None], 0.0),
        axis=0,
    )
    mixed = layer_tail(
        partial_value.astype(jnp.bfloat16).reshape(3, 8, model_width),
        tokens.reshape(3, 8, model_width),
        post_gain[None, :],
        branch_gate[None, :],
        meta[None, :],
        comb,
        dense_gate_w,
        dense_up_w,
        dense_down_w,
        expert_gate_w[0],
        expert_up_w[0],
        expert_down_w[0],
    )
    return (mixed.reshape(seq_count, 1024), fresh_key, fresh_value, current)


def solution(mesh):
    placed = (
        P("ep", None),
        P(),
        P(None, "tp"),
        P(),
        P(),
        P(),
        P(),
        P(),
        P(),
        P("ep", "tp", None, None),
        P("ep", "tp", None, None),
        P("ep", "tp", None),
        P("ep"),
        P("tp", None),
        P(),
        P(),
        P(None, ("ep", "tp")),
        P(None, ("ep", "tp")),
        P(("ep", "tp"), None),
        P("ep", None),
        P("ep", None),
        P("ep", None, "tp"),
        P("ep", None, "tp"),
        P("ep", "tp", None),
    )
    return jax.shard_map(
        body,
        mesh=mesh,
        in_specs=placed,
        out_specs=(P("ep", "tp"), P("ep", "tp", None), P("ep", "tp", None), P("ep", "tp")),
        check_vma=False,
    )
```

```python
import math
import functools

import jax
import jax.numpy as jnp
from jax import lax
from jax.experimental import pallas as pl
from jax.experimental.pallas import tpu as pltpu
from jax.sharding import PartitionSpec as P

FF2 = 16384
norm_eps = 1e-06
MESH = pl.DeviceIdType.MESH
f32, bf16 = jnp.float32, jnp.bfloat16


class Sems:
    def __init__(self, send, recv):
        self.send, self.recv, self.n = send, recv, 0
        self.sent = []

    def copy(self, src, dst, device):
        i = self.n
        self.n += 1
        cp = pltpu.make_async_remote_copy(
            src_ref=src,
            dst_ref=dst,
            send_sem=self.send.at[i],
            recv_sem=self.recv.at[i],
            device_id=device,
            device_id_type=MESH,
        )
        cp.start()
        self.sent.append(cp)
        return cp


def silu(v):
    return v / (1.0 + jnp.exp(-v))


def layer_kernel(
    len_ref, tokens_h, ngain_h, pgain_h, bgate_h, qgain_h, kgain_h, fbias_h, choice_h, rweight_h,
    qw_h, kw_h, vw_h, fw_h, kc_h, vc_h, cg_h, ow_h,
    dg_h, du_h, dd_h, eg_h, eu_h, ed_h,
    out_ref, fk_ref, fv_ref, fg_ref,
    tok_s, ngain_s, pgain_s, bgate_s, qgain_s, kgain_s, fbias_s, choice_s, rweight_s,
    qw, kw, vw, fw, kc, vc, cg, ow, rows_s, q_s, kf_s, vf_s, o_s, ah_s, meta_s, comb_s,
    partial_s, partner_part, resid_s, pn_s, a1, xs, hid, wgu, wd, eg, eu, ed,
    meta_all, meta_tab, xg, dens, rl, rr, ql, qr, sl, sr, t2, r2, t3, r3,
    sq, sq1, sq2, sq2r, sq3, sq3r, ep_send, ep_recv, ret_f, ret_b, back,
    send_sem, recv_sem, load_sem, small_sem, cache_sem, meta_sems, back_sems,
):
    me = lax.axis_index("ep")
    core = lax.axis_index("tp")
    other = 1 - core
    coords = (me % 4, (me // 4) % 4, me // 16)
    weights = (1, 4, 16)
    partner = (me, other)
    half = pl.multiple_of(core * 1024, 1024)
    ohalf = pl.multiple_of(other * 1024, 1024)
    ccol = pl.multiple_of(core * 128, 128)

    def peer(dim, k):
        v = coords[dim]
        return (me + (((v + k) % 4) - v) * weights[dim], core)

    sems = Sems(send_sem, recv_sem)

    barrier = pltpu.get_barrier_semaphore()
    pl.semaphore_signal(barrier, inc=1, device_id=partner, device_id_type=MESH)

    @pl.loop(1, 64)
    def _(i):
        pl.semaphore_signal(
            barrier, inc=1, device_id=((me + i) % 64, core), device_id_type=MESH
        )

    smalls = []
    for i, (src, dst) in enumerate((
        (tokens_h, tok_s), (ngain_h, ngain_s), (choice_h, choice_s), (rweight_h, rweight_s),
        (qw_h, qw), (kw_h, kw), (vw_h, vw), (fw_h, fw), (fbias_h, fbias_s),
        (qgain_h, qgain_s), (kgain_h, kgain_s), (pgain_h, pgain_s), (bgate_h, bgate_s),
    )):
        cp = pltpu.make_async_copy(src, dst, small_sem.at[i])
        cp.start()
        smalls.append(cp)

    def cache_copies(g):
        rows = pl.ds(g * 4, 4)
        return [
            pltpu.make_async_copy(src.at[rows], dst.at[rows], cache_sem.at[i, g])
            for i, (src, dst) in enumerate(((kc_h, kc), (cg_h, cg), (vc_h, vc)))
        ]

    for g in range(6):
        for cp in cache_copies(g):
            cp.start()
    loads = []
    for i, (src, dst) in enumerate((
        (dg_h, wgu.at[:, pl.ds(0, 128)]),
        (du_h, wgu.at[:, pl.ds(128, 128)]),
        (dd_h.at[:, pl.ds(half, 1024)], wd.at[pl.ds(ccol, 128)]),
        (eg_h, eg),
        (eu_h, eu),
        (ed_h, ed),
        (ow_h, ow),
    )):
        loads.append(pltpu.make_async_copy(src, dst, load_sem.at[i]))
    loads[6].start()

    def column(row):
        pick = lax.broadcasted_iota(jnp.int32, (24, 24), 0) == lax.broadcasted_iota(jnp.int32, (24, 24), 1)
        return jnp.sum(jnp.where(pick, row, jnp.zeros_like(row)), axis=1, keepdims=True)

    smalls[2].wait()
    smalls[3].wait()
    choice = choice_s[...].astype(f32)
    named = [choice[k:k + 1, :] for k in range(2)]
    named_col = [column(v) for v in named]
    earlier = lax.broadcasted_iota(jnp.int32, (24, 24), 0) < lax.broadcasted_iota(jnp.int32, (24, 24), 1)
    targets = []
    for k in range(2):
        again = jnp.zeros((1, 24), f32)
        for i in range(2):
            same = jnp.where(earlier & (named_col[i] == named[k]), 1.0, 0.0)
            again = again + jnp.sum(same, axis=0, keepdims=True)
        targets.append(named[k] * 2.0 + jnp.minimum(again, 1.0))
    meta_s[...] = jnp.full((1, 128), -1.0, f32)
    meta_s[:, pl.ds(0, 24)] = targets[0] + 128.0 * targets[1]
    target_col = [column(v) for v in targets]
    weight_col = [column(rweight_s[k:k + 1, :]) for k in range(2)]
    place = lax.broadcasted_iota(jnp.int32, (24, 64), 1).astype(f32) * 2.0
    for t in range(2):
        m = jnp.where(target_col[0] == place + t, weight_col[0], 0.0)
        comb_s[t] = m + jnp.where(target_col[1] == place + t, weight_col[1], 0.0)

    for i in (1, 11, 12):
        smalls[i].wait()
    for i, src in enumerate((ngain_s, pgain_s, bgate_s)):
        v = src[...].astype(f32)
        for t in range(16):
            rows_s[pl.ds(i, 1), pl.ds(t * 128, 128)] = v[t:t + 1]
    smalls[0].wait()
    toks = tok_s[...].astype(f32)
    mean_square = jnp.mean(toks * toks, axis=-1, keepdims=True)
    normed = (toks * lax.rsqrt(mean_square + norm_eps) * rows_s[pl.ds(0, 1), :]).astype(bf16)

    def head_norm(v, gain):
        return v * lax.rsqrt(jnp.mean(v * v, axis=-1, keepdims=True) + norm_eps) * gain

    smalls[4].wait()
    q_all = jnp.dot(normed, qw[...], preferred_element_type=f32)
    smalls[9].wait()
    qg = qgain_s[...].astype(f32)
    for h in range(8):
        q = head_norm(q_all[:, h * 64:(h + 1) * 64], qg).astype(bf16).astype(f32)
        q_s[pl.ds(h, 24, stride=8), :] = jnp.concatenate([q, jnp.zeros_like(q)], axis=1)
    smalls[5].wait()
    smalls[10].wait()
    k_all = jnp.dot(normed, kw[...], preferred_element_type=f32)
    k_own = head_norm(jnp.where(core == 0, k_all[:, :64], k_all[:, 64:]), kgain_s[...].astype(f32))
    fk_ref[...] = k_own.astype(bf16)
    kf_s[...] = k_own.astype(bf16).astype(f32)
    smalls[6].wait()
    v_all = jnp.dot(normed, vw[...], preferred_element_type=f32)
    v_own = jnp.where(core == 0, v_all[:, :64], v_all[:, 64:]).astype(bf16)
    fv_ref[...] = v_own
    vf_s[...] = v_own.astype(f32)
    smalls[7].wait()
    smalls[8].wait()
    forget = lax.dot_general(
        fw[...], normed, (((1,), (1,)), ((), ())), preferred_element_type=f32
    )
    pick16 = lax.broadcasted_iota(jnp.int32, (16, 16), 0) == lax.broadcasted_iota(jnp.int32, (16, 16), 1)
    forget = forget + jnp.sum(jnp.where(pick16, fbias_s[...], 0.0), axis=1, keepdims=True)
    log_forget = jnp.minimum(forget, 0.0) - jnp.log1p(jnp.exp(-jnp.abs(forget)))
    log_forget = jnp.where(core == 0, log_forget[:8], log_forget[8:])

    slot_at = lax.broadcasted_iota(jnp.int32, (8, 1024), 1)
    seq_lane = lax.broadcasted_iota(jnp.int32, (8, 24), 1)
    scale = 64 ** (-0.5)

    def attend(g, gates):
        for cp in cache_copies(g):
            cp.wait()
        for i in range(4):
            s = g * 4 + i
            rows = pl.ds(pl.multiple_of(s * 8, 8), 8)
            length = len_ref[s]
            q = q_s[rows, :][:, :64]
            score = jnp.dot(q.astype(bf16), kc[s], preferred_element_type=f32) * scale
            gate = cg[s]
            current = jnp.sum(jnp.where(slot_at == length - 1, gate, 0.0), axis=1, keepdims=True)
            current = current + jnp.sum(
                jnp.where(seq_lane == s, log_forget, 0.0), axis=1, keepdims=True
            )
            gates = jnp.where(seq_lane == s, current, gates)
            own = jnp.sum(q * kf_s[pl.ds(s, 1), :], axis=1, keepdims=True) * scale
            logit = jnp.where(slot_at < length, score + (current - gate), -jnp.inf)
            top = jnp.maximum(jnp.max(logit, axis=1, keepdims=True), own)
            w = jnp.exp(logit - top)
            own_w = jnp.exp(own - top)
            inv = 1.0 / (jnp.sum(w, axis=1, keepdims=True) + own_w)
            probs = (w * inv).astype(bf16)
            own_p = (own_w * inv).astype(bf16).astype(f32)
            o = lax.dot_general(
                probs, vc[s], (((1,), (1,)), ((), ())), preferred_element_type=f32
            )
            o = o + own_p * vf_s[pl.ds(s, 1), :]
            o_s[rows, :] = jnp.concatenate([o, jnp.zeros_like(o)], axis=1)
        return gates

    gates = lax.fori_loop(0, 6, attend, jnp.zeros((8, 24), f32))
    fg_ref[...] = gates
    for cp in loads[:6]:
        cp.start()
    for h in range(8):
        ah_s[:, pl.ds(h * 64, 64)] = o_s[pl.ds(h, 24, stride=8), :][:, :64]
    loads[6].wait()
    partial = jnp.dot(ah_s[...].astype(bf16), ow[...], preferred_element_type=f32)
    partial_s[...] = partial.reshape(3, 8, 2048).astype(bf16)

    pl.semaphore_wait(barrier, 64)

    part_cp = sems.copy(partial_s, partner_part, partner)
    wd_cp = sems.copy(dd_h.at[:, pl.ds(ohalf, 1024)], wd.at[pl.ds(ccol, 128)], partner)

    def meta_copy(d):
        return pltpu.make_async_remote_copy(
            src_ref=meta_s,
            dst_ref=meta_all.at[me],
            send_sem=meta_sems.at[0],
            recv_sem=meta_sems.at[1],
            device_id=(d, core),
            device_id_type=MESH,
        )

    part_cp.wait_recv()
    attn = partial_s[...].astype(f32) + partner_part[...].astype(f32)
    resid = (tok_s[...].astype(f32).reshape(3, 8, 2048) + attn).astype(bf16).astype(f32)
    resid_s[...] = resid
    mean_square = jnp.mean(resid * resid, axis=-1, keepdims=True)
    gain = rows_s[pl.ds(1, 1), :][None]
    post = (resid * lax.rsqrt(mean_square + norm_eps) * gain).astype(bf16)
    pn_s[...] = post
    a1[:, 0] = pn_s[:, :, pl.ds(half, 1024)]

    g1 = [
        [sems.copy(a1.at[p, 0], a1.at[p, 4 - k], peer(p, k)) for k in (1, 3, 2)]
        for p in range(3)
    ]

    @pl.loop(1, 64)
    def _(i):
        meta_copy((me + i) % 64).start()

    meta_all[me] = meta_s[...]
    branch = jax.nn.sigmoid(
        jnp.sum(post.astype(f32) * rows_s[pl.ds(2, 1), :][None], axis=-1, keepdims=True)
    )

    g2 = []
    for p in range(3):
        for cp in g1[p]:
            cp.wait_recv()
        for pair in range(2):
            rows = jnp.concatenate(
                [a1[p, 2 * pair].astype(f32), a1[p, 2 * pair + 1].astype(f32)], axis=0
            )
            xs[core, 0, pl.ds(p * 128 + pair * 16, 16)] = rows.astype(bf16)
        line = xs.at[core, 0, pl.ds(p * 128, 32)]
        g2.append([
            sems.copy(line, xs.at[core, 0, pl.ds(p * 128 + (4 - k) * 32, 32)], peer((p + 1) % 3, k))
            for k in (1, 3, 2)
        ])

    g3, d2d = [], [[] for _ in range(4)]

    def share(slot, p, start, size):
        view = xs.at[core, slot, pl.ds(p * 128 + start, size)]
        d2d[slot].append(sems.copy(view, view, partner))

    for p in range(3):
        for cp in g2[p]:
            cp.wait_recv()
        cdim = (p + 2) % 3
        rows = pl.ds(p * 128, 128)
        g3.append((
            sems.copy(xs.at[core, 0, rows], xs.at[core, 1, rows], peer(cdim, 1)),
            sems.copy(xs.at[core, 0, rows], xs.at[core, 2, rows], peer(cdim, 3)),
        ))
        share(0, p, 0, 128)

    pltpu.make_async_copy(
        meta_all.at[pl.ds(0, 63)], meta_all.at[pl.ds(0, 63)], meta_sems.at[1]
    ).wait()
    for d in range(64):
        meta_tab[pl.ds(d, 1), :] = meta_all[d]
    table = meta_tab[...].astype(jnp.int32)
    lane = lax.broadcasted_iota(jnp.int32, (64, 128), 1)
    dev = lax.broadcasted_iota(jnp.int32, (64, 1), 0)
    shift = [((dev >> s) - coords[i]) & 3 for i, s in enumerate((0, 2, 4))]
    starts = []
    for p in range(3):
        ka, kb, kc = shift[p], shift[(p + 1) % 3], shift[(p + 2) % 3]
        slot = jnp.where(kc == 0, 0, jnp.where(kc == 1, 2, jnp.where(kc == 2, 3, 1)))
        starts.append(slot * 384 + p * 128 + kb * 32 + ka * 8)
    row_ids = []
    for s in range(2):
        want = me * 2 + s
        hit = (lane < 24) & (((table & 127) == want) | ((table >> 7) == want))
        tok = jnp.sum(jnp.where(hit, lane + 1, 0), axis=1, keepdims=True) - 1
        start = jnp.where(tok < 8, starts[0], jnp.where(tok < 16, starts[1], starts[2]))
        row_ids.append(jnp.where(tok < 0, -1, start + (tok & 7)))
    row_id = jnp.concatenate(row_ids, axis=0)
    cols = lax.broadcasted_iota(jnp.int32, (128, 384), 1)

    def select(slot):
        pick = jnp.where(row_id == cols + slot * 384, 1.0, 0.0).astype(bf16)
        for h in range(2):
            got = jnp.dot(pick, xs[h, slot], preferred_element_type=f32)
            if slot:
                got = xg[h] + got
            xg[h] = got

    h_cp = [None] * 4

    def up_proj(slot):
        v = jnp.dot(xs[0, slot], wgu[pl.ds(0, 1024)], preferred_element_type=f32)
        v = v + jnp.dot(xs[1, slot], wgu[pl.ds(1024, 1024)], preferred_element_type=f32)
        hid[slot, :, pl.ds(ccol, 128)] = (silu(v[:, :128]) * v[:, 128:]).astype(bf16)
        view = hid.at[slot, :, pl.ds(ccol, 128)]
        h_cp[slot] = sems.copy(view, view, partner)

    ones = jnp.ones((8, 256), bf16)

    def down_proj(slot):
        h_cp[slot].wait_recv()
        h = hid[slot]
        hf = h.astype(f32)
        dens[slot] = jnp.dot(h, wd[...], preferred_element_type=f32).astype(bf16)
        s = lax.dot_general(
            ones, (hf * hf).astype(bf16), (((1,), (1,)), ((), ())), preferred_element_type=f32
        )
        for p in range(3):
            sq[slot, p] = s[0:1, p * 128:(p + 1) * 128]

    def arrive(slot):
        for cp in d2d[slot]:
            cp.wait_recv()

    loads[0].wait()
    loads[1].wait()
    arrive(0)
    up_proj(0)
    select(0)

    relay = []
    for p in range(3):
        cdim = (p + 2) % 3
        g3[p][0].wait_recv()
        rows = pl.ds(p * 128, 64)
        relay.append(sems.copy(xs.at[core, 1, rows], xs.at[core, 3, rows], peer(cdim, 1)))
        share(1, p, 0, 128)
        g3[p][1].wait_recv()
        rows = pl.ds(p * 128 + 64, 64)
        relay.append(sems.copy(xs.at[core, 2, rows], xs.at[core, 3, rows], peer(cdim, 3)))
        share(2, p, 0, 128)

    arrive(1)
    up_proj(1)
    arrive(2)
    up_proj(2)
    loads[2].wait()
    wd_cp.wait_recv()
    select(1)
    down_proj(1)
    select(2)
    down_proj(2)

    s1 = []
    for p in range(3):
        cdim = (p + 2) % 3
        s1.append([
            sems.copy(dens.at[2, pl.ds(p * 128 + 64, 64)], rl.at[p, 1], peer(cdim, 1)),
            sems.copy(dens.at[1, pl.ds(p * 128, 64)], rr.at[p, 0], peer(cdim, 3)),
        ])

    for p in range(3):
        relay[2 * p].wait_recv()
        share(3, p, 0, 64)
        relay[2 * p + 1].wait_recv()
        share(3, p, 64, 64)
    arrive(3)
    up_proj(3)
    select(3)
    down_proj(3)
    far = []
    for p in range(3):
        cdim = (p + 2) % 3
        far.append((
            sems.copy(dens.at[3, pl.ds(p * 128, 64)], ql.at[p], peer(cdim, 1)),
            sems.copy(dens.at[3, pl.ds(p * 128 + 64, 64)], qr.at[p], peer(cdim, 3)),
        ))
        s1[p] += [
            sems.copy(sq.at[2, p], sq1.at[p, 0], peer(cdim, 1)),
            sems.copy(sq.at[1, p], sq1.at[p, 1], peer(cdim, 3)),
            sems.copy(sq.at[3, p], sq1.at[p, 2], peer(cdim, 2)),
        ]

    for i in (3, 4, 5):
        loads[i].wait()
    x0, x1 = xg[0].astype(bf16), xg[1].astype(bf16)
    gate = jnp.dot(x0, eg[pl.ds(0, 1024)], preferred_element_type=f32)
    gate = gate + jnp.dot(x1, eg[pl.ds(1024, 1024)], preferred_element_type=f32)
    up = jnp.dot(x0, eu[pl.ds(0, 1024)], preferred_element_type=f32)
    up = up + jnp.dot(x1, eu[pl.ds(1024, 1024)], preferred_element_type=f32)
    act = (silu(gate) * up).astype(bf16)
    ep_send[...] = jnp.dot(act, ed[:, pl.ds(ohalf, 1024)], preferred_element_type=f32).astype(bf16)
    ep_cp = sems.copy(ep_send, ep_recv, partner)
    mine = jnp.dot(act, ed[:, pl.ds(half, 1024)], preferred_element_type=f32).astype(bf16)

    for p in range(3):
        cdim = (p + 2) % 3
        far[p][0].wait_recv()
        sl[p] = (dens[2, pl.ds(p * 128, 64)].astype(f32) + ql[p].astype(f32)).astype(bf16)
        s1[p].append(sems.copy(sl.at[p], rl.at[p, 0], peer(cdim, 1)))
        far[p][1].wait_recv()
        sr[p] = (dens[1, pl.ds(p * 128 + 64, 64)].astype(f32) + qr[p].astype(f32)).astype(bf16)
        s1[p].append(sems.copy(sr.at[p], rr.at[p, 1], peer(cdim, 3)))

    ep_cp.wait_recv()
    rows = (mine.astype(f32) + ep_recv[...].astype(f32)).astype(bf16).astype(f32)
    for s in range(2):
        for t in range(8):
            ret_f[pl.ds(s * 8 + t, 64, stride=16), :] = rows[s * 64:(s + 1) * 64, t * 128:(t + 1) * 128]
    ret_b[...] = ret_f[...].astype(bf16).reshape(64, 16, 128)

    def back_copy(d):
        return pltpu.make_async_remote_copy(
            src_ref=ret_b.at[d],
            dst_ref=back.at[me],
            send_sem=back_sems.at[0],
            recv_sem=back_sems.at[1],
            device_id=(d, core),
            device_id_type=MESH,
        )

    @pl.loop(1, 64)
    def _(i):
        back_copy((me + i) % 64).start()

    back[me] = ret_b[me]
    down_proj(0)

    s2 = []
    for p in range(3):
        for cp in s1[p]:
            cp.wait_recv()
        total = dens[0, pl.ds(p * 128, 128)].astype(f32)
        total = total + jnp.concatenate([rl[p, 0], rl[p, 1]], axis=0).astype(f32)
        total = total + jnp.concatenate([rr[p, 0], rr[p, 1]], axis=0).astype(f32)
        for k in range(4):
            t2[p, k] = total[k * 32:(k + 1) * 32].astype(bf16)
        v = sq[0, p] + sq1[p, 0] + sq1[p, 1] + sq1[p, 2]
        sq2[p, 0] = v
        for k in range(1, 4):
            sq2[p, k] = pltpu.roll(v, 128 - 32 * k, 1)
        s2.append([
            sems.copy(t2.at[p, k], r2.at[p, k - 1], peer((p + 1) % 3, k)) for k in (1, 3, 2)
        ] + [
            sems.copy(sq2.at[p, k], sq2r.at[p, k - 1], peer((p + 1) % 3, k)) for k in (1, 3, 2)
        ])

    pltpu.make_async_copy(back.at[pl.ds(0, 63)], back.at[pl.ds(0, 63)], back_sems.at[1]).wait()
    ret_f[...] = back[...].reshape(1024, 128).astype(f32)
    mixes = []
    for t in range(8):
        m = 0.0
        for s in range(2):
            m = m + jnp.dot(
                comb_s[s], ret_f[pl.ds(s * 8 + t, 64, stride=16), :],
                preferred_element_type=f32, precision=lax.Precision.HIGHEST,
            )
        mixes.append(m)
    expert_sum = jnp.concatenate(mixes, axis=1)

    s3 = []
    for p in range(3):
        for cp in s2[p]:
            cp.wait_recv()
        total = t2[p, 0].astype(f32)
        for k in range(3):
            total = total + r2[p, k].astype(f32)
        for k in range(4):
            t3[p, k] = total[k * 8:(k + 1) * 8].astype(bf16)
        v = sq2[p, 0] + sq2r[p, 0] + sq2r[p, 1] + sq2r[p, 2]
        sq3[p, 0] = v
        for k in range(1, 4):
            sq3[p, k] = pltpu.roll(v, 128 - 8 * k, 1)
        s3.append([
            sems.copy(t3.at[p, k], r3.at[p, k - 1], peer(p, k)) for k in (1, 3, 2)
        ] + [
            sems.copy(sq3.at[p, k], sq3r.at[p, k - 1], peer(p, k)) for k in (1, 3, 2)
        ])

    eye = lax.broadcasted_iota(jnp.int32, (8, 128), 0) == lax.broadcasted_iota(jnp.int32, (8, 128), 1)
    for p in range(3):
        for cp in s3[p]:
            cp.wait_recv()
        total = t3[p, 0].astype(f32)
        v = sq3[p, 0]
        for k in range(3):
            total = total + r3[p, k].astype(f32)
            v = v + sq3r[p, k]
        square = jnp.sum(jnp.where(eye, v, 0.0), axis=1, keepdims=True)
        dense = (total * lax.rsqrt(square / FF2 + norm_eps)).astype(bf16).astype(f32)
        mixed = resid_s[p, :, pl.ds(half, 1024)] + expert_sum[p * 8:(p + 1) * 8] + branch[p] * dense
        out_ref[p] = mixed.astype(bf16)

    for cp in sems.sent:
        cp.wait_send()
    pltpu.make_async_copy(
        meta_all.at[pl.ds(0, 63)], meta_all.at[pl.ds(0, 63)], meta_sems.at[0]
    ).wait()
    pltpu.make_async_copy(back.at[pl.ds(0, 63)], back.at[pl.ds(0, 63)], back_sems.at[0]).wait()


def fused_layer(lens, *args):
    V = pltpu.VMEM
    vm = pl.BlockSpec(memory_space=pltpu.VMEM)
    hbm = pl.BlockSpec(memory_space=pl.ANY)
    scratch = [
        V((24, 2048), bf16),
        V((16, 128), bf16),
        V((16, 128), bf16),
        V((16, 128), bf16),
        V((1, 64), bf16),
        V((1, 64), bf16),
        V((1, 16), f32),
        V((2, 24), jnp.int32),
        V((2, 24), f32),
        V((2048, 512), bf16),
        V((2048, 128), bf16),
        V((2048, 128), bf16),
        V((16, 2048), bf16),
        V((24, 64, 1024), bf16),
        V((24, 64, 1024), bf16),
        V((24, 8, 1024), f32),
        V((512, 2048), bf16),
        V((8, 2048), f32),
        V((192, 128), f32),
        V((24, 64), f32),
        V((24, 64), f32),
        V((192, 128), f32),
        V((24, 512), f32),
        V((1, 128), f32),
        V((2, 24, 64), f32),
        V((3, 8, 2048), bf16),
        V((3, 8, 2048), bf16),
        V((3, 8, 2048), f32),
        V((3, 8, 2048), bf16),
        V((3, 4, 8, 1024), bf16),
        V((2, 4, 384, 1024), bf16),
        V((4, 384, 256), bf16),
        V((2048, 256), bf16),
        V((256, 1024), bf16),
        V((2048, 512), bf16),
        V((2048, 512), bf16),
        V((512, 2048), bf16),
        V((64, 1, 128), f32),
        V((64, 128), f32),
        V((2, 128, 1024), f32),
        V((4, 384, 1024), bf16),
        V((3, 2, 64, 1024), bf16),
        V((3, 2, 64, 1024), bf16),
        V((3, 64, 1024), bf16),
        V((3, 64, 1024), bf16),
        V((3, 64, 1024), bf16),
        V((3, 64, 1024), bf16),
        V((3, 4, 32, 1024), bf16),
        V((3, 3, 32, 1024), bf16),
        V((3, 4, 8, 1024), bf16),
        V((3, 3, 8, 1024), bf16),
        V((4, 3, 1, 128), f32),
        V((3, 3, 1, 128), f32),
        V((3, 4, 1, 128), f32),
        V((3, 3, 1, 128), f32),
        V((3, 4, 1, 128), f32),
        V((3, 3, 1, 128), f32),
        V((128, 1024), bf16),
        V((128, 1024), bf16),
        V((1024, 128), f32),
        V((64, 16, 128), bf16),
        V((64, 16, 128), bf16),
        pltpu.SemaphoreType.DMA((128,)),
        pltpu.SemaphoreType.DMA((128,)),
        pltpu.SemaphoreType.DMA((7,)),
        pltpu.SemaphoreType.DMA((13,)),
        pltpu.SemaphoreType.DMA((3, 6)),
        pltpu.SemaphoreType.DMA((2,)),
        pltpu.SemaphoreType.DMA((2,)),
    ]
    return pl.pallas_call(
        layer_kernel,
        out_shape=(
            jax.ShapeDtypeStruct((3, 8, 1024), bf16),
            jax.ShapeDtypeStruct((24, 64), bf16),
            jax.ShapeDtypeStruct((24, 64), bf16),
            jax.ShapeDtypeStruct((8, 24), f32),
        ),
        in_specs=[pl.BlockSpec(memory_space=pltpu.SMEM)] + [hbm] * len(args),
        out_specs=(vm,) * 4,
        scratch_shapes=scratch,
        compiler_params=pltpu.CompilerParams(
            collective_id=0, has_side_effects=True, vmem_limit_bytes=56 * 1024 * 1024
        ),
    )(lens, *args)


def body(
    tokens,
    norm_gain,
    query_w,
    key_w,
    value_w,
    forget_w,
    forget_bias,
    query_gain,
    key_gain,
    cache_key,
    cache_value,
    cache_gate,
    cache_len,
    out_w,
    post_gain,
    branch_gate,
    dense_gate_w,
    dense_up_w,
    dense_down_w,
    expert_choice,
    route_weight,
    expert_gate_w,
    expert_up_w,
    expert_down_w,
):
    mixed, fresh_key, fresh_value, fresh_gate = fused_layer(
        cache_len,
        tokens,
        norm_gain.reshape(16, 128),
        post_gain.reshape(16, 128),
        branch_gate.reshape(16, 128),
        query_gain.reshape(1, 64),
        key_gain.reshape(1, 64),
        forget_bias.reshape(1, 16),
        expert_choice.T,
        route_weight.T,
        query_w,
        key_w,
        value_w,
        forget_w.T,
        cache_key.reshape(24, 64, 1024),
        cache_value.reshape(24, 64, 1024),
        cache_gate,
        out_w,
        dense_gate_w,
        dense_up_w,
        dense_down_w,
        expert_gate_w.reshape(2048, 512),
        expert_up_w.reshape(2048, 512),
        expert_down_w.reshape(512, 2048),
    )
    return (
        mixed.reshape(24, 1024),
        fresh_key.reshape(24, 1, 64),
        fresh_value.reshape(24, 1, 64),
        fresh_gate.T,
    )


def solution(mesh):
    placed = (
        P("ep", None),
        P(),
        P(None, "tp"),
        P(),
        P(),
        P(),
        P(),
        P(),
        P(),
        P("ep", "tp", None, None),
        P("ep", "tp", None, None),
        P("ep", "tp", None),
        P("ep"),
        P("tp", None),
        P(),
        P(),
        P(None, ("ep", "tp")),
        P(None, ("ep", "tp")),
        P(("ep", "tp"), None),
        P("ep", None),
        P("ep", None),
        P("ep", None, "tp"),
        P("ep", None, "tp"),
        P("ep", "tp", None),
    )
    return jax.shard_map(
        body,
        mesh=mesh,
        in_specs=placed,
        out_specs=(P("ep", "tp"), P("ep", "tp", None), P("ep", "tp", None), P("ep", "tp")),
        check_vma=False,
    )
```

```python
import math
import functools

import jax
import jax.numpy as jnp
from jax import lax
from jax.experimental import pallas as pl
from jax.experimental.pallas import tpu as pltpu
from jax.sharding import PartitionSpec as P

FF2 = 16384
norm_eps = 1e-06
MESH = pl.DeviceIdType.MESH
f32, bf16 = jnp.float32, jnp.bfloat16


class Sems:
    def __init__(self, send, recv):
        self.send, self.recv, self.n = send, recv, 0
        self.sent = []

    def copy(self, src, dst, device):
        i = self.n
        self.n += 1
        cp = pltpu.make_async_remote_copy(
            src_ref=src,
            dst_ref=dst,
            send_sem=self.send.at[i],
            recv_sem=self.recv.at[i],
            device_id=device,
            device_id_type=MESH,
        )
        cp.start()
        self.sent.append(cp)
        return cp


def silu(v):
    return v / (1.0 + jnp.exp(-v))


def layer_kernel(
    len_ref, tokens_h, ngain_h, pgain_h, bgate_h, qgain_h, kgain_h, fbias_h, choice_h, rweight_h,
    qw_h, kw_h, vw_h, fw_h, kc_h, vc_h, cg_h, ow_h,
    dg_h, du_h, dd_h, eg_h, eu_h, ed_h,
    out_ref, fk_ref, fv_ref, fg_ref,
    tok_s, ngain_s, pgain_s, bgate_s, qgain_s, kgain_s, fbias_s, choice_s, rweight_s,
    qw, kw, vw, fw, kc, vc, cg, ow, rows_s, q_s, kf_s, vf_s, o_s, ah_s, comb_s,
    partial_s, partner_part, resid_s, pn_s, a1, xs, hid, wgu, wd, eg, eu, ed,
    meta_all, meta_tab, xg, dens, rl, rr, ql, qr, sl, sr, t2, r2, t3, r3,
    sq, sq1, sq2, sq2r, sq3, sq3r, ep_send, ep_recv, ret_f, ret_b, back,
    send_sem, recv_sem, load_sem, small_sem, cache_sem, back_sems,
):
    me = lax.axis_index("ep")
    core = lax.axis_index("tp")
    other = 1 - core
    coords = (me % 4, (me // 4) % 4, me // 16)
    weights = (1, 4, 16)
    partner = (me, other)
    half = pl.multiple_of(core * 1024, 1024)
    ohalf = pl.multiple_of(other * 1024, 1024)
    ccol = pl.multiple_of(core * 128, 128)

    def peer(dim, k):
        v = coords[dim]
        return (me + (((v + k) % 4) - v) * weights[dim], core)

    sems = Sems(send_sem, recv_sem)

    barrier = pltpu.get_barrier_semaphore()
    pl.semaphore_signal(barrier, inc=1, device_id=partner, device_id_type=MESH)

    for dim in range(3):
        for k in (1, 2, 3):
            pl.semaphore_signal(barrier, inc=1, device_id=peer(dim, k), device_id_type=MESH)

    smalls = []
    for i, (src, dst) in enumerate((
        (tokens_h, tok_s), (ngain_h, ngain_s), (choice_h, choice_s), (rweight_h, rweight_s),
        (qw_h, qw), (kw_h, kw), (vw_h, vw), (fw_h, fw), (fbias_h, fbias_s),
        (qgain_h, qgain_s), (kgain_h, kgain_s), (pgain_h, pgain_s), (bgate_h, bgate_s),
    )):
        cp = pltpu.make_async_copy(src, dst, small_sem.at[i])
        cp.start()
        smalls.append(cp)

    def cache_copies(g):
        rows = pl.ds(g * 4, 4)
        return [
            pltpu.make_async_copy(src.at[rows], dst.at[rows], cache_sem.at[i, g])
            for i, (src, dst) in enumerate(((kc_h, kc), (cg_h, cg), (vc_h, vc)))
        ]

    loads = []
    for i, (src, dst) in enumerate((
        (dg_h, wgu.at[:, pl.ds(0, 128)]),
        (du_h, wgu.at[:, pl.ds(128, 128)]),
        (dd_h.at[:, pl.ds(half, 1024)], wd.at[pl.ds(ccol, 128)]),
        (eg_h, eg),
        (eu_h, eu),
        (ed_h, ed),
        (ow_h, ow),
    )):
        loads.append(pltpu.make_async_copy(src, dst, load_sem.at[i]))
    meta_all[0] = jnp.full((1, 128), -1.0, f32)

    def column(row):
        pick = lax.broadcasted_iota(jnp.int32, (24, 24), 0) == lax.broadcasted_iota(jnp.int32, (24, 24), 1)
        return jnp.sum(jnp.where(pick, row, jnp.zeros_like(row)), axis=1, keepdims=True)

    smalls[2].wait()
    smalls[3].wait()
    choice = choice_s[...].astype(f32)
    named = [choice[k:k + 1, :] for k in range(2)]
    named_col = [column(v) for v in named]
    earlier = lax.broadcasted_iota(jnp.int32, (24, 24), 0) < lax.broadcasted_iota(jnp.int32, (24, 24), 1)
    targets = []
    for k in range(2):
        again = jnp.zeros((1, 24), f32)
        for i in range(2):
            same = jnp.where(earlier & (named_col[i] == named[k]), 1.0, 0.0)
            again = again + jnp.sum(same, axis=0, keepdims=True)
        targets.append(named[k] * 2.0 + jnp.minimum(again, 1.0))
    meta_all[0, :, pl.ds(0, 24)] = targets[0] + 128.0 * targets[1]
    target_col = [column(v) for v in targets]
    weight_col = [column(rweight_s[k:k + 1, :]) for k in range(2)]
    place = lax.broadcasted_iota(jnp.int32, (24, 64), 1).astype(f32) * 2.0
    for t in range(2):
        m = jnp.where(target_col[0] == place + t, weight_col[0], 0.0)
        comb_s[t] = m + jnp.where(target_col[1] == place + t, weight_col[1], 0.0)

    smalls[4].wait()
    for g in range(6):
        for cp in cache_copies(g):
            cp.start()
    loads[6].start()

    for i in (1, 11, 12):
        smalls[i].wait()
    for i, src in enumerate((ngain_s, pgain_s, bgate_s)):
        v = src[...].astype(f32)
        for t in range(16):
            rows_s[pl.ds(i, 1), pl.ds(t * 128, 128)] = v[t:t + 1]
    smalls[0].wait()
    toks = tok_s[...].astype(f32)
    mean_square = jnp.mean(toks * toks, axis=-1, keepdims=True)
    normed = (toks * lax.rsqrt(mean_square + norm_eps) * rows_s[pl.ds(0, 1), :]).astype(bf16)

    def head_norm(v, gain):
        return v * lax.rsqrt(jnp.mean(v * v, axis=-1, keepdims=True) + norm_eps) * gain

    q_all = jnp.dot(normed, qw[...], preferred_element_type=f32)
    smalls[9].wait()
    qg = qgain_s[...].astype(f32)
    for h in range(8):
        q = head_norm(q_all[:, h * 64:(h + 1) * 64], qg).astype(bf16).astype(f32)
        q_s[pl.ds(h, 24, stride=8), :] = jnp.concatenate([q, jnp.zeros_like(q)], axis=1)
    smalls[5].wait()
    smalls[10].wait()
    k_all = jnp.dot(normed, kw[...], preferred_element_type=f32)
    k_own = head_norm(jnp.where(core == 0, k_all[:, :64], k_all[:, 64:]), kgain_s[...].astype(f32))
    fk_ref[...] = k_own.astype(bf16)
    kf_s[...] = k_own.astype(bf16).astype(f32)
    smalls[6].wait()
    v_all = jnp.dot(normed, vw[...], preferred_element_type=f32)
    v_own = jnp.where(core == 0, v_all[:, :64], v_all[:, 64:]).astype(bf16)
    fv_ref[...] = v_own
    vf_s[...] = v_own.astype(f32)
    smalls[7].wait()
    smalls[8].wait()
    forget = lax.dot_general(
        fw[...], normed, (((1,), (1,)), ((), ())), preferred_element_type=f32
    )
    pick16 = lax.broadcasted_iota(jnp.int32, (16, 16), 0) == lax.broadcasted_iota(jnp.int32, (16, 16), 1)
    forget = forget + jnp.sum(jnp.where(pick16, fbias_s[...], 0.0), axis=1, keepdims=True)
    log_forget = jnp.minimum(forget, 0.0) - jnp.log1p(jnp.exp(-jnp.abs(forget)))
    log_forget = jnp.where(core == 0, log_forget[:8], log_forget[8:])

    slot_at = lax.broadcasted_iota(jnp.int32, (8, 1024), 1)
    seq_lane = lax.broadcasted_iota(jnp.int32, (8, 24), 1)
    scale = 64 ** (-0.5)

    def attend(g, gates):
        for cp in cache_copies(g):
            cp.wait()
        for i in range(4):
            s = g * 4 + i
            rows = pl.ds(pl.multiple_of(s * 8, 8), 8)
            length = len_ref[s]
            q = q_s[rows, :][:, :64]
            score = jnp.dot(q.astype(bf16), kc[s], preferred_element_type=f32) * scale
            gate = cg[s]
            current = jnp.sum(jnp.where(slot_at == length - 1, gate, 0.0), axis=1, keepdims=True)
            current = current + jnp.sum(
                jnp.where(seq_lane == s, log_forget, 0.0), axis=1, keepdims=True
            )
            gates = jnp.where(seq_lane == s, current, gates)
            own = jnp.sum(q * kf_s[pl.ds(s, 1), :], axis=1, keepdims=True) * scale
            logit = jnp.where(slot_at < length, score + (current - gate), -jnp.inf)
            top = jnp.maximum(jnp.max(logit, axis=1, keepdims=True), own)
            w = jnp.exp(logit - top)
            own_w = jnp.exp(own - top)
            inv = 1.0 / (jnp.sum(w, axis=1, keepdims=True) + own_w)
            probs = (w * inv).astype(bf16)
            own_p = (own_w * inv).astype(bf16).astype(f32)
            o = lax.dot_general(
                probs, vc[s], (((1,), (1,)), ((), ())), preferred_element_type=f32
            )
            o = o + own_p * vf_s[pl.ds(s, 1), :]
            o_s[rows, :] = jnp.concatenate([o, jnp.zeros_like(o)], axis=1)
        return gates

    gates = lax.fori_loop(0, 6, attend, jnp.zeros((8, 24), f32))
    fg_ref[...] = gates
    for cp in loads[:6]:
        cp.start()
    for h in range(8):
        ah_s[:, pl.ds(h * 64, 64)] = o_s[pl.ds(h, 24, stride=8), :][:, :64]
    loads[6].wait()
    partial = jnp.dot(ah_s[...].astype(bf16), ow[...], preferred_element_type=f32)
    partial_s[...] = partial.reshape(3, 8, 2048).astype(bf16)

    pl.semaphore_wait(barrier, 10)

    part_cp = sems.copy(partial_s, partner_part, partner)
    wd_cp = sems.copy(dd_h.at[:, pl.ds(ohalf, 1024)], wd.at[pl.ds(ccol, 128)], partner)

    part_cp.wait_recv()
    attn = partial_s[...].astype(f32) + partner_part[...].astype(f32)
    resid = (tok_s[...].astype(f32).reshape(3, 8, 2048) + attn).astype(bf16).astype(f32)
    resid_s[...] = resid
    mean_square = jnp.mean(resid * resid, axis=-1, keepdims=True)
    gain = rows_s[pl.ds(1, 1), :][None]
    post = (resid * lax.rsqrt(mean_square + norm_eps) * gain).astype(bf16)
    pn_s[...] = post
    a1[:, 0] = pn_s[:, :, pl.ds(half, 1024)]

    def meta_stage(dim, size):
        return [
            sems.copy(meta_all.at[pl.ds(0, size)], meta_all.at[pl.ds((4 - k) * size, size)], peer(dim, k))
            for k in (1, 3, 2)
        ]

    meta_cp = meta_stage(0, 1)
    g1 = [
        [sems.copy(a1.at[p, 0], a1.at[p, 4 - k], peer(p, k)) for k in (1, 3, 2)]
        for p in range(3)
    ]

    branch = jax.nn.sigmoid(
        jnp.sum(post.astype(f32) * rows_s[pl.ds(2, 1), :][None], axis=-1, keepdims=True)
    )

    g2 = []
    for p in range(3):
        if p == 0:
            for cp in meta_cp:
                cp.wait_recv()
            meta_cp = meta_stage(1, 4)
        for cp in g1[p]:
            cp.wait_recv()
        for pair in range(2):
            rows = jnp.concatenate(
                [a1[p, 2 * pair].astype(f32), a1[p, 2 * pair + 1].astype(f32)], axis=0
            )
            xs[core, 0, pl.ds(p * 128 + pair * 16, 16)] = rows.astype(bf16)
        line = xs.at[core, 0, pl.ds(p * 128, 32)]
        g2.append([
            sems.copy(line, xs.at[core, 0, pl.ds(p * 128 + (4 - k) * 32, 32)], peer((p + 1) % 3, k))
            for k in (1, 3, 2)
        ])

    g3, d2d = [], [[] for _ in range(4)]

    def share(slot, p, start, size):
        view = xs.at[core, slot, pl.ds(p * 128 + start, size)]
        d2d[slot].append(sems.copy(view, view, partner))

    lo, hi = (lambda p: pl.ds(p * 128, 64)), (lambda p: pl.ds(p * 128 + 64, 64))
    for p in range(3):
        if p == 0:
            for cp in meta_cp:
                cp.wait_recv()
            meta_cp = meta_stage(2, 16)
        for cp in g2[p]:
            cp.wait_recv()
        cdim = (p + 2) % 3
        own = xs.at[core, 0]
        g3.append([
            sems.copy(own.at[rows], xs.at[core, slot, rows], peer(cdim, k))
            for slot, k, rows in ((1, 1, lo(p)), (2, 3, hi(p)), (1, 1, hi(p)), (2, 3, lo(p)))
        ])
        share(0, p, 0, 128)

    for cp in meta_cp:
        cp.wait_recv()
    for d in range(64):
        meta_tab[pl.ds(d, 1), :] = meta_all[d]
    table = meta_tab[...].astype(jnp.int32)
    lane = lax.broadcasted_iota(jnp.int32, (64, 128), 1)
    dev = lax.broadcasted_iota(jnp.int32, (64, 1), 0)
    shift = [(dev >> s) & 3 for s in (0, 2, 4)]
    starts = []
    for p in range(3):
        ka, kb, kc = shift[p], shift[(p + 1) % 3], shift[(p + 2) % 3]
        slot = jnp.where(kc == 0, 0, jnp.where(kc == 1, 2, jnp.where(kc == 2, 3, 1)))
        starts.append(slot * 384 + p * 128 + kb * 32 + ka * 8)
    row_ids = []
    for s in range(2):
        want = me * 2 + s
        hit = (lane < 24) & (((table & 127) == want) | ((table >> 7) == want))
        tok = jnp.sum(jnp.where(hit, lane + 1, 0), axis=1, keepdims=True) - 1
        start = jnp.where(tok < 8, starts[0], jnp.where(tok < 16, starts[1], starts[2]))
        row_ids.append(jnp.where(tok < 0, -1, start + (tok & 7)))
    row_id = jnp.concatenate(row_ids, axis=0)
    cols = lax.broadcasted_iota(jnp.int32, (128, 384), 1)

    def select(slot):
        pick = jnp.where(row_id == cols + slot * 384, 1.0, 0.0).astype(bf16)
        for h in range(2):
            got = jnp.dot(pick, xs[h, slot], preferred_element_type=f32)
            if slot:
                got = xg[h] + got
            xg[h] = got

    h_cp = [None] * 4

    def up_proj(slot):
        v = jnp.dot(xs[0, slot], wgu[pl.ds(0, 1024)], preferred_element_type=f32)
        v = v + jnp.dot(xs[1, slot], wgu[pl.ds(1024, 1024)], preferred_element_type=f32)
        hid[slot, :, pl.ds(ccol, 128)] = (silu(v[:, :128]) * v[:, 128:]).astype(bf16)
        view = hid.at[slot, :, pl.ds(ccol, 128)]
        h_cp[slot] = sems.copy(view, view, partner)

    ones = jnp.ones((8, 256), bf16)

    def down_proj(slot):
        h_cp[slot].wait_recv()
        h = hid[slot]
        hf = h.astype(f32)
        dens[slot] = jnp.dot(h, wd[...], preferred_element_type=f32).astype(bf16)
        s = lax.dot_general(
            ones, (hf * hf).astype(bf16), (((1,), (1,)), ((), ())), preferred_element_type=f32
        )
        for p in range(3):
            sq[slot, p] = s[0:1, p * 128:(p + 1) * 128]

    def arrive(slot):
        for cp in d2d[slot]:
            cp.wait_recv()

    loads[0].wait()
    loads[1].wait()
    arrive(0)
    up_proj(0)
    select(0)

    relay = []
    for p in range(3):
        cdim = (p + 2) % 3
        g3[p][0].wait_recv()
        relay.append(sems.copy(xs.at[core, 1, lo(p)], xs.at[core, 3, lo(p)], peer(cdim, 1)))
        g3[p][1].wait_recv()
        relay.append(sems.copy(xs.at[core, 2, hi(p)], xs.at[core, 3, hi(p)], peer(cdim, 3)))
        share(1, p, 0, 64)
        share(2, p, 64, 64)
    for p in range(3):
        g3[p][2].wait_recv()
        share(1, p, 64, 64)
        g3[p][3].wait_recv()
        share(2, p, 0, 64)

    arrive(1)
    up_proj(1)
    arrive(2)
    up_proj(2)
    loads[2].wait()
    wd_cp.wait_recv()
    select(1)
    down_proj(1)
    select(2)
    down_proj(2)

    s1 = []
    for p in range(3):
        cdim = (p + 2) % 3
        s1.append([
            sems.copy(dens.at[2, hi(p)], rl.at[p, hi(0)], peer(cdim, 1)),
            sems.copy(dens.at[1, lo(p)], rr.at[p, lo(0)], peer(cdim, 3)),
        ])

    for p in range(3):
        relay[2 * p].wait_recv()
        share(3, p, 0, 64)
        relay[2 * p + 1].wait_recv()
        share(3, p, 64, 64)
    arrive(3)
    up_proj(3)
    select(3)
    down_proj(3)
    far = []
    for p in range(3):
        cdim = (p + 2) % 3
        far.append([
            sems.copy(dens.at[3, pl.ds(p * 128 + q * 32, 32)], buf.at[p, q % 2], peer(cdim, k))
            for q, buf, k in ((1, ql, 1), (2, qr, 3), (0, ql, 1), (3, qr, 3))
        ])
        s1[p] += [
            sems.copy(sq.at[2, p], sq1.at[p, 0], peer(cdim, 1)),
            sems.copy(sq.at[1, p], sq1.at[p, 1], peer(cdim, 3)),
            sems.copy(sq.at[3, p], sq1.at[p, 2], peer(cdim, 2)),
        ]

    for i in (3, 4, 5):
        loads[i].wait()
    x0, x1 = xg[0].astype(bf16), xg[1].astype(bf16)
    gate = jnp.dot(x0, eg[pl.ds(0, 1024)], preferred_element_type=f32)
    gate = gate + jnp.dot(x1, eg[pl.ds(1024, 1024)], preferred_element_type=f32)
    up = jnp.dot(x0, eu[pl.ds(0, 1024)], preferred_element_type=f32)
    up = up + jnp.dot(x1, eu[pl.ds(1024, 1024)], preferred_element_type=f32)
    act = (silu(gate) * up).astype(bf16)
    ep_send[...] = jnp.dot(act, ed[:, pl.ds(ohalf, 1024)], preferred_element_type=f32).astype(bf16)
    ep_cp = sems.copy(ep_send, ep_recv, partner)
    mine = jnp.dot(act, ed[:, pl.ds(half, 1024)], preferred_element_type=f32).astype(bf16)

    sums = [[None] * 4 for _ in range(3)]
    for i, (q, near, came, out, to, k) in enumerate((
        (1, 2, ql, sl, rl, 1), (2, 1, qr, sr, rr, 3), (0, 2, ql, sl, rl, 1), (3, 1, qr, sr, rr, 3)
    )):
        for p in range(3):
            far[p][i].wait_recv()
            mix = dens[near, pl.ds(p * 128 + q * 32, 32)].astype(f32) + came[p, q % 2].astype(f32)
            out[p, q % 2] = mix.astype(bf16)
            sums[p][q] = sems.copy(
                out.at[p, q % 2], to.at[p, pl.ds(q * 32, 32)], peer((p + 2) % 3, k)
            )

    ep_cp.wait_recv()
    rows = (mine.astype(f32) + ep_recv[...].astype(f32)).astype(bf16).astype(f32)
    for s in range(2):
        for t in range(8):
            ret_f[pl.ds(s * 8 + t, 64, stride=16), :] = rows[s * 64:(s + 1) * 64, t * 128:(t + 1) * 128]
    ret_b[...] = ret_f[...].astype(bf16).reshape(64, 16, 128)

    @pl.loop(1, 64)
    def _(i):
        owner = (coords[0] + i % 4) % 4 + (coords[1] + (i // 4) % 4) % 4 * 4 + (coords[2] + i // 16) % 4 * 16
        pltpu.make_async_remote_copy(
            src_ref=ret_b.at[i],
            dst_ref=back.at[me],
            send_sem=back_sems.at[0],
            recv_sem=back_sems.at[1],
            device_id=(owner, core),
            device_id_type=MESH,
        ).start()

    back[me] = ret_b[0]
    down_proj(0)

    s2 = [[] for _ in range(3)]
    for p in range(3):
        for cp in s1[p]:
            cp.wait_recv()
        v = sq[0, p] + sq1[p, 0] + sq1[p, 1] + sq1[p, 2]
        sq2[p, 0] = v
        for k in range(1, 4):
            sq2[p, k] = pltpu.roll(v, 128 - 32 * k, 1)
            s2[p].append(sems.copy(sq2.at[p, k], sq2r.at[p, k - 1], peer((p + 1) % 3, k)))
    for q in (2, 1, 3, 0):
        for p in range(3):
            sums[p][q].wait_recv()
            rows = pl.ds(q * 32, 32)
            total = dens[0, pl.ds(p * 128 + q * 32, 32)].astype(f32)
            total = total + rl[p, rows].astype(f32) + rr[p, rows].astype(f32)
            t2[p, q] = total.astype(bf16)
            if q:
                s2[p].append(sems.copy(t2.at[p, q], r2.at[p, q - 1], peer((p + 1) % 3, q)))

    pltpu.make_async_copy(back.at[pl.ds(0, 63)], back.at[pl.ds(0, 63)], back_sems.at[1]).wait()
    ret_f[...] = back[...].reshape(1024, 128).astype(f32)
    mixes = []
    for t in range(8):
        m = 0.0
        for s in range(2):
            m = m + jnp.dot(
                comb_s[s], ret_f[pl.ds(s * 8 + t, 64, stride=16), :],
                preferred_element_type=f32, precision=lax.Precision.HIGHEST,
            )
        mixes.append(m)
    expert_sum = jnp.concatenate(mixes, axis=1)

    s3 = []
    for p in range(3):
        for cp in s2[p]:
            cp.wait_recv()
        total = t2[p, 0].astype(f32)
        for k in range(3):
            total = total + r2[p, k].astype(f32)
        for k in range(4):
            t3[p, k] = total[k * 8:(k + 1) * 8].astype(bf16)
        v = sq2[p, 0] + sq2r[p, 0] + sq2r[p, 1] + sq2r[p, 2]
        sq3[p, 0] = v
        for k in range(1, 4):
            sq3[p, k] = pltpu.roll(v, 128 - 8 * k, 1)
        s3.append([
            sems.copy(t3.at[p, k], r3.at[p, k - 1], peer(p, k)) for k in (1, 3, 2)
        ] + [
            sems.copy(sq3.at[p, k], sq3r.at[p, k - 1], peer(p, k)) for k in (1, 3, 2)
        ])

    eye = lax.broadcasted_iota(jnp.int32, (8, 128), 0) == lax.broadcasted_iota(jnp.int32, (8, 128), 1)
    for p in range(3):
        for cp in s3[p]:
            cp.wait_recv()
        total = t3[p, 0].astype(f32)
        v = sq3[p, 0]
        for k in range(3):
            total = total + r3[p, k].astype(f32)
            v = v + sq3r[p, k]
        square = jnp.sum(jnp.where(eye, v, 0.0), axis=1, keepdims=True)
        dense = (total * lax.rsqrt(square / FF2 + norm_eps)).astype(bf16).astype(f32)
        mixed = resid_s[p, :, pl.ds(half, 1024)] + expert_sum[p * 8:(p + 1) * 8] + branch[p] * dense
        out_ref[p] = mixed.astype(bf16)

    for cp in sems.sent:
        cp.wait_send()
    pltpu.make_async_copy(back.at[pl.ds(0, 63)], back.at[pl.ds(0, 63)], back_sems.at[0]).wait()


def fused_layer(lens, *args):
    V = pltpu.VMEM
    vm = pl.BlockSpec(memory_space=pltpu.VMEM)
    hbm = pl.BlockSpec(memory_space=pl.ANY)
    scratch = [
        V((24, 2048), bf16),
        V((16, 128), bf16),
        V((16, 128), bf16),
        V((16, 128), bf16),
        V((1, 64), bf16),
        V((1, 64), bf16),
        V((1, 16), f32),
        V((2, 24), jnp.int32),
        V((2, 24), f32),
        V((2048, 512), bf16),
        V((2048, 128), bf16),
        V((2048, 128), bf16),
        V((16, 2048), bf16),
        V((24, 64, 1024), bf16),
        V((24, 64, 1024), bf16),
        V((24, 8, 1024), f32),
        V((512, 2048), bf16),
        V((8, 2048), f32),
        V((192, 128), f32),
        V((24, 64), f32),
        V((24, 64), f32),
        V((192, 128), f32),
        V((24, 512), f32),
        V((2, 24, 64), f32),
        V((3, 8, 2048), bf16),
        V((3, 8, 2048), bf16),
        V((3, 8, 2048), f32),
        V((3, 8, 2048), bf16),
        V((3, 4, 8, 1024), bf16),
        V((2, 4, 384, 1024), bf16),
        V((4, 384, 256), bf16),
        V((2048, 256), bf16),
        V((256, 1024), bf16),
        V((2048, 512), bf16),
        V((2048, 512), bf16),
        V((512, 2048), bf16),
        V((64, 1, 128), f32),
        V((64, 128), f32),
        V((2, 128, 1024), f32),
        V((4, 384, 1024), bf16),
        V((3, 128, 1024), bf16),
        V((3, 128, 1024), bf16),
        V((3, 2, 32, 1024), bf16),
        V((3, 2, 32, 1024), bf16),
        V((3, 2, 32, 1024), bf16),
        V((3, 2, 32, 1024), bf16),
        V((3, 4, 32, 1024), bf16),
        V((3, 3, 32, 1024), bf16),
        V((3, 4, 8, 1024), bf16),
        V((3, 3, 8, 1024), bf16),
        V((4, 3, 1, 128), f32),
        V((3, 3, 1, 128), f32),
        V((3, 4, 1, 128), f32),
        V((3, 3, 1, 128), f32),
        V((3, 4, 1, 128), f32),
        V((3, 3, 1, 128), f32),
        V((128, 1024), bf16),
        V((128, 1024), bf16),
        V((1024, 128), f32),
        V((64, 16, 128), bf16),
        V((64, 16, 128), bf16),
        pltpu.SemaphoreType.DMA((192,)),
        pltpu.SemaphoreType.DMA((192,)),
        pltpu.SemaphoreType.DMA((7,)),
        pltpu.SemaphoreType.DMA((13,)),
        pltpu.SemaphoreType.DMA((3, 6)),
        pltpu.SemaphoreType.DMA((2,)),
    ]
    return pl.pallas_call(
        layer_kernel,
        out_shape=(
            jax.ShapeDtypeStruct((3, 8, 1024), bf16),
            jax.ShapeDtypeStruct((24, 64), bf16),
            jax.ShapeDtypeStruct((24, 64), bf16),
            jax.ShapeDtypeStruct((8, 24), f32),
        ),
        in_specs=[pl.BlockSpec(memory_space=pltpu.SMEM)] + [hbm] * len(args),
        out_specs=(vm,) * 4,
        scratch_shapes=scratch,
        compiler_params=pltpu.CompilerParams(
            collective_id=0, has_side_effects=True, vmem_limit_bytes=56 * 1024 * 1024
        ),
    )(lens, *args)


def finish(*arrays):
    def kernel(*refs):
        for src, dst in zip(refs[:4], refs[4:]):
            dst[...] = src[...]

    return pl.pallas_call(
        kernel,
        out_shape=tuple(jax.ShapeDtypeStruct(a.shape, a.dtype) for a in arrays),
        in_specs=[pl.BlockSpec(memory_space=pltpu.VMEM)] * 4,
        out_specs=(pl.BlockSpec(memory_space=pltpu.VMEM),) * 4,
    )(*arrays)


def body(
    tokens,
    norm_gain,
    query_w,
    key_w,
    value_w,
    forget_w,
    forget_bias,
    query_gain,
    key_gain,
    cache_key,
    cache_value,
    cache_gate,
    cache_len,
    out_w,
    post_gain,
    branch_gate,
    dense_gate_w,
    dense_up_w,
    dense_down_w,
    expert_choice,
    route_weight,
    expert_gate_w,
    expert_up_w,
    expert_down_w,
):
    mixed, fresh_key, fresh_value, fresh_gate = fused_layer(
        cache_len,
        tokens,
        norm_gain.reshape(16, 128),
        post_gain.reshape(16, 128),
        branch_gate.reshape(16, 128),
        query_gain.reshape(1, 64),
        key_gain.reshape(1, 64),
        forget_bias.reshape(1, 16),
        expert_choice.T,
        route_weight.T,
        query_w,
        key_w,
        value_w,
        forget_w.T,
        cache_key.reshape(24, 64, 1024),
        cache_value.reshape(24, 64, 1024),
        cache_gate,
        out_w,
        dense_gate_w,
        dense_up_w,
        dense_down_w,
        expert_gate_w.reshape(2048, 512),
        expert_up_w.reshape(2048, 512),
        expert_down_w.reshape(512, 2048),
    )
    mixed, fresh_key, fresh_value, fresh_gate = finish(
        mixed.reshape(24, 1024), fresh_key, fresh_value, fresh_gate
    )
    return (
        mixed,
        fresh_key.reshape(24, 1, 64),
        fresh_value.reshape(24, 1, 64),
        fresh_gate.T,
    )


def solution(mesh):
    placed = (
        P("ep", None),
        P(),
        P(None, "tp"),
        P(),
        P(),
        P(),
        P(),
        P(),
        P(),
        P("ep", "tp", None, None),
        P("ep", "tp", None, None),
        P("ep", "tp", None),
        P("ep"),
        P("tp", None),
        P(),
        P(),
        P(None, ("ep", "tp")),
        P(None, ("ep", "tp")),
        P(("ep", "tp"), None),
        P("ep", None),
        P("ep", None),
        P("ep", None, "tp"),
        P("ep", None, "tp"),
        P("ep", "tp", None),
    )
    return jax.shard_map(
        body,
        mesh=mesh,
        in_specs=placed,
        out_specs=(P("ep", "tp"), P("ep", "tp", None), P("ep", "tp", None), P("ep", "tp")),
        check_vma=False,
    )
```

```python
import math
import functools

import jax
import jax.numpy as jnp
from jax import lax
from jax.experimental import pallas as pl
from jax.experimental.pallas import tpu as pltpu
from jax.sharding import PartitionSpec as P

FF2 = 16384
norm_eps = 1e-06
GROUP = 8
MESH = pl.DeviceIdType.MESH
f32, bf16 = jnp.float32, jnp.bfloat16


class Sems:
    def __init__(self, send, recv):
        self.send, self.recv, self.n = send, recv, 0
        self.sent = []

    def copy(self, src, dst, device):
        i = self.n
        self.n += 1
        cp = pltpu.make_async_remote_copy(
            src_ref=src,
            dst_ref=dst,
            send_sem=self.send.at[i],
            recv_sem=self.recv.at[i],
            device_id=device,
            device_id_type=MESH,
        )
        cp.start()
        self.sent.append(cp)
        return cp


def silu(v):
    return v / (1.0 + jnp.exp(-v))


def layer_kernel(
    len_ref, tokens_h, ngain_h, pgain_h, bgate_h, qgain_h, kgain_h, fbias_h, choice_h, rweight_h,
    qw_h, kw_h, vw_h, fw_h, kc_h, vc_h, cg_h, ow_h,
    dg_h, du_h, dd_h, eg_h, eu_h, ed_h,
    out_ref, fk_ref, fv_ref, fg_ref,
    tok_s, ngain_s, pgain_s, bgate_s, qgain_s, kgain_s, fbias_s, choice_s, rweight_s,
    qw, kw, vw, fw, kc, vc, cg, ow, rows_s, q_s, kf_s, vf_s, o_s, ah_s, comb_s,
    partial_s, partner_part, resid_s, pn_s, a1, xs, hid, wgu, wd, eg, eu, ed,
    meta_all, meta_tab, xg, dens, rl, rr, ql, qr, sl, sr, t2, r2, t3, r3,
    sq, sq1, sq2, sq2r, sq3, sq3r, ep_send, ep_recv, ret_f, ret_b, back,
    send_sem, recv_sem, load_sem, small_sem, cache_sem, back_sems,
):
    me = lax.axis_index("ep")
    core = lax.axis_index("tp")
    other = 1 - core
    coords = (me % 4, (me // 4) % 4, me // 16)
    weights = (1, 4, 16)
    partner = (me, other)
    half = pl.multiple_of(core * 1024, 1024)
    ohalf = pl.multiple_of(other * 1024, 1024)
    ccol = pl.multiple_of(core * 128, 128)

    def peer(dim, k):
        v = coords[dim]
        return (me + (((v + k) % 4) - v) * weights[dim], core)

    sems = Sems(send_sem, recv_sem)

    barrier = pltpu.get_barrier_semaphore()
    pl.semaphore_signal(barrier, inc=1, device_id=partner, device_id_type=MESH)

    for dim in range(3):
        for k in (1, 2, 3):
            pl.semaphore_signal(barrier, inc=1, device_id=peer(dim, k), device_id_type=MESH)

    smalls = []
    for i, (src, dst) in enumerate((
        (tokens_h, tok_s), (ngain_h, ngain_s), (choice_h, choice_s), (rweight_h, rweight_s),
        (qw_h, qw), (kw_h, kw), (vw_h, vw), (fw_h, fw), (fbias_h, fbias_s),
        (qgain_h, qgain_s), (kgain_h, kgain_s), (pgain_h, pgain_s), (bgate_h, bgate_s),
    )):
        cp = pltpu.make_async_copy(src, dst, small_sem.at[i])
        cp.start()
        smalls.append(cp)

    def cache_copies(g):
        rows = pl.ds(g * GROUP, GROUP)
        return [
            pltpu.make_async_copy(src.at[rows], dst.at[rows], cache_sem.at[i, g])
            for i, (src, dst) in enumerate(((kc_h, kc), (cg_h, cg), (vc_h, vc)))
        ]

    loads = []
    for i, (src, dst) in enumerate((
        (dg_h, wgu.at[:, pl.ds(0, 128)]),
        (du_h, wgu.at[:, pl.ds(128, 128)]),
        (dd_h.at[:, pl.ds(half, 1024)], wd.at[pl.ds(ccol, 128)]),
        (eg_h, eg),
        (eu_h, eu),
        (ed_h, ed),
        (ow_h, ow),
    )):
        loads.append(pltpu.make_async_copy(src, dst, load_sem.at[i]))
    meta_all[0] = jnp.full((1, 128), -1.0, f32)

    def column(row):
        pick = lax.broadcasted_iota(jnp.int32, (24, 24), 0) == lax.broadcasted_iota(jnp.int32, (24, 24), 1)
        return jnp.sum(jnp.where(pick, row, jnp.zeros_like(row)), axis=1, keepdims=True)

    smalls[2].wait()
    smalls[3].wait()
    choice = choice_s[...].astype(f32)
    named = [choice[k:k + 1, :] for k in range(2)]
    named_col = [column(v) for v in named]
    earlier = lax.broadcasted_iota(jnp.int32, (24, 24), 0) < lax.broadcasted_iota(jnp.int32, (24, 24), 1)
    targets = []
    for k in range(2):
        again = jnp.zeros((1, 24), f32)
        for i in range(2):
            same = jnp.where(earlier & (named_col[i] == named[k]), 1.0, 0.0)
            again = again + jnp.sum(same, axis=0, keepdims=True)
        targets.append(named[k] * 2.0 + jnp.minimum(again, 1.0))
    meta_all[0, :, pl.ds(0, 24)] = targets[0] + 128.0 * targets[1]
    target_col = [column(v) for v in targets]
    weight_col = [column(rweight_s[k:k + 1, :]) for k in range(2)]
    place = lax.broadcasted_iota(jnp.int32, (24, 64), 1).astype(f32) * 2.0
    for t in range(2):
        m = jnp.where(target_col[0] == place + t, weight_col[0], 0.0)
        comb_s[t] = m + jnp.where(target_col[1] == place + t, weight_col[1], 0.0)

    smalls[4].wait()
    for g in range(24 // GROUP):
        for cp in cache_copies(g):
            cp.start()
    loads[6].start()

    for i in (1, 11, 12):
        smalls[i].wait()
    for i, src in enumerate((ngain_s, pgain_s, bgate_s)):
        v = src[...].astype(f32)
        for t in range(16):
            rows_s[pl.ds(i, 1), pl.ds(t * 128, 128)] = v[t:t + 1]
    smalls[0].wait()
    toks = tok_s[...].astype(f32)
    mean_square = jnp.mean(toks * toks, axis=-1, keepdims=True)
    normed = (toks * lax.rsqrt(mean_square + norm_eps) * rows_s[pl.ds(0, 1), :]).astype(bf16)

    def head_norm(v, gain):
        return v * lax.rsqrt(jnp.mean(v * v, axis=-1, keepdims=True) + norm_eps) * gain

    q_all = jnp.dot(normed, qw[...], preferred_element_type=f32)
    smalls[9].wait()
    qg = qgain_s[...].astype(f32)
    for h in range(8):
        q = head_norm(q_all[:, h * 64:(h + 1) * 64], qg).astype(bf16).astype(f32)
        q_s[pl.ds(h, 24, stride=8), :] = jnp.concatenate([q, jnp.zeros_like(q)], axis=1)
    smalls[5].wait()
    smalls[10].wait()
    k_all = jnp.dot(normed, kw[...], preferred_element_type=f32)
    k_own = head_norm(jnp.where(core == 0, k_all[:, :64], k_all[:, 64:]), kgain_s[...].astype(f32))
    fk_ref[...] = k_own.astype(bf16)
    kf_s[...] = k_own.astype(bf16).astype(f32)
    smalls[6].wait()
    v_all = jnp.dot(normed, vw[...], preferred_element_type=f32)
    v_own = jnp.where(core == 0, v_all[:, :64], v_all[:, 64:]).astype(bf16)
    fv_ref[...] = v_own
    vf_s[...] = v_own.astype(f32)
    smalls[7].wait()
    smalls[8].wait()
    forget = lax.dot_general(
        fw[...], normed, (((1,), (1,)), ((), ())), preferred_element_type=f32
    )
    pick16 = lax.broadcasted_iota(jnp.int32, (16, 16), 0) == lax.broadcasted_iota(jnp.int32, (16, 16), 1)
    forget = forget + jnp.sum(jnp.where(pick16, fbias_s[...], 0.0), axis=1, keepdims=True)
    log_forget = jnp.minimum(forget, 0.0) - jnp.log1p(jnp.exp(-jnp.abs(forget)))
    log_forget = jnp.where(core == 0, log_forget[:8], log_forget[8:])

    slot_at = lax.broadcasted_iota(jnp.int32, (8, 1024), 1)
    seq_lane = lax.broadcasted_iota(jnp.int32, (8, 24), 1)
    scale = 64 ** (-0.5)

    def score_group(g, gates):
        for cp in cache_copies(g):
            cp.wait()
        for i in range(GROUP):
            s = g * GROUP + i
            rows = pl.ds(pl.multiple_of(s * 8, 8), 8)
            length = len_ref[s]
            q = q_s[rows, :][:, :64]
            score = jnp.dot(q.astype(bf16), kc[s], preferred_element_type=f32) * scale
            gate = cg[s]
            current = jnp.sum(jnp.where(slot_at == length - 1, gate, 0.0), axis=1, keepdims=True)
            current = current + jnp.sum(
                jnp.where(seq_lane == s, log_forget, 0.0), axis=1, keepdims=True
            )
            gates = jnp.where(seq_lane == s, current, gates)
            own = jnp.sum(q * kf_s[pl.ds(s, 1), :], axis=1, keepdims=True) * scale
            logit = jnp.where(slot_at < length, score + (current - gate), -jnp.inf)
            top = jnp.maximum(jnp.max(logit, axis=1, keepdims=True), own)
            cg[s] = logit - top
            o_s[rows, :] = jnp.broadcast_to(own - top, (8, 128))
        return gates

    def mix_group(g, carry):
        for i in range(GROUP):
            s = g * GROUP + i
            rows = pl.ds(pl.multiple_of(s * 8, 8), 8)
            w = jnp.exp(cg[s])
            own_w = jnp.exp(o_s[rows, :][:, :64])
            inv = 1.0 / (jnp.sum(w, axis=1, keepdims=True) + own_w)
            o = lax.dot_general(
                w.astype(bf16), vc[s], (((1,), (1,)), ((), ())), preferred_element_type=f32
            )
            o = (o + own_w.astype(bf16).astype(f32) * vf_s[pl.ds(s, 1), :]) * inv
            o_s[rows, :] = jnp.concatenate([o, jnp.zeros_like(o)], axis=1)
        return carry

    gates = lax.fori_loop(0, 24 // GROUP, score_group, jnp.zeros((8, 24), f32))
    lax.fori_loop(0, 24 // GROUP, mix_group, 0)
    fg_ref[...] = gates
    for cp in loads[:6]:
        cp.start()
    for h in range(8):
        ah_s[:, pl.ds(h * 64, 64)] = o_s[pl.ds(h, 24, stride=8), :][:, :64]
    loads[6].wait()
    partial = jnp.dot(ah_s[...].astype(bf16), ow[...], preferred_element_type=f32)
    partial_s[...] = partial.reshape(3, 8, 2048).astype(bf16)

    pl.semaphore_wait(barrier, 10)

    part_cp = sems.copy(partial_s, partner_part, partner)
    wd_cp = sems.copy(dd_h.at[:, pl.ds(ohalf, 1024)], wd.at[pl.ds(ccol, 128)], partner)

    part_cp.wait_recv()
    attn = partial_s[...].astype(f32) + partner_part[...].astype(f32)
    resid = (tok_s[...].astype(f32).reshape(3, 8, 2048) + attn).astype(bf16).astype(f32)
    resid_s[...] = resid
    mean_square = jnp.mean(resid * resid, axis=-1, keepdims=True)
    gain = rows_s[pl.ds(1, 1), :][None]
    post = (resid * lax.rsqrt(mean_square + norm_eps) * gain).astype(bf16)
    pn_s[...] = post
    a1[:, 0] = pn_s[:, :, pl.ds(half, 1024)]

    def meta_stage(dim, size):
        return [
            sems.copy(meta_all.at[pl.ds(0, size)], meta_all.at[pl.ds((4 - k) * size, size)], peer(dim, k))
            for k in (1, 3, 2)
        ]

    meta_cp = meta_stage(0, 1)
    g1 = [
        [sems.copy(a1.at[p, 0], a1.at[p, 4 - k], peer(p, k)) for k in (1, 3, 2)]
        for p in range(3)
    ]

    branch = jax.nn.sigmoid(
        jnp.sum(post.astype(f32) * rows_s[pl.ds(2, 1), :][None], axis=-1, keepdims=True)
    )

    g2 = []
    for p in range(3):
        if p == 0:
            for cp in meta_cp:
                cp.wait_recv()
            meta_cp = meta_stage(1, 4)
        for cp in g1[p]:
            cp.wait_recv()
        for pair in range(2):
            rows = jnp.concatenate(
                [a1[p, 2 * pair].astype(f32), a1[p, 2 * pair + 1].astype(f32)], axis=0
            )
            xs[core, 0, pl.ds(p * 128 + pair * 16, 16)] = rows.astype(bf16)
        line = xs.at[core, 0, pl.ds(p * 128, 32)]
        g2.append([
            sems.copy(line, xs.at[core, 0, pl.ds(p * 128 + (4 - k) * 32, 32)], peer((p + 1) % 3, k))
            for k in (1, 3, 2)
        ])

    g3, d2d = [], [[] for _ in range(4)]

    def share(slot, p, start, size):
        view = xs.at[core, slot, pl.ds(p * 128 + start, size)]
        d2d[slot].append(sems.copy(view, view, partner))

    lo, hi = (lambda p: pl.ds(p * 128, 64)), (lambda p: pl.ds(p * 128 + 64, 64))
    for p in range(3):
        if p == 0:
            for cp in meta_cp:
                cp.wait_recv()
            meta_cp = meta_stage(2, 16)
        for cp in g2[p]:
            cp.wait_recv()
        cdim = (p + 2) % 3
        own = xs.at[core, 0]
        g3.append([
            sems.copy(own.at[rows], xs.at[core, slot, rows], peer(cdim, k))
            for slot, k, rows in ((1, 1, lo(p)), (2, 3, hi(p)), (1, 1, hi(p)), (2, 3, lo(p)))
        ])
        share(0, p, 0, 128)

    for cp in meta_cp:
        cp.wait_recv()
    for d in range(64):
        meta_tab[pl.ds(d, 1), :] = meta_all[d]
    table = meta_tab[...].astype(jnp.int32)
    lane = lax.broadcasted_iota(jnp.int32, (64, 128), 1)
    dev = lax.broadcasted_iota(jnp.int32, (64, 1), 0)
    shift = [(dev >> s) & 3 for s in (0, 2, 4)]
    starts = []
    for p in range(3):
        ka, kb, kc = shift[p], shift[(p + 1) % 3], shift[(p + 2) % 3]
        slot = jnp.where(kc == 0, 0, jnp.where(kc == 1, 2, jnp.where(kc == 2, 3, 1)))
        starts.append(slot * 384 + p * 128 + kb * 32 + ka * 8)
    row_ids = []
    for s in range(2):
        want = me * 2 + s
        hit = (lane < 24) & (((table & 127) == want) | ((table >> 7) == want))
        tok = jnp.sum(jnp.where(hit, lane + 1, 0), axis=1, keepdims=True) - 1
        start = jnp.where(tok < 8, starts[0], jnp.where(tok < 16, starts[1], starts[2]))
        row_ids.append(jnp.where(tok < 0, -1, start + (tok & 7)))
    row_id = jnp.concatenate(row_ids, axis=0)
    cols = lax.broadcasted_iota(jnp.int32, (128, 384), 1)

    def select(slot):
        pick = jnp.where(row_id == cols + slot * 384, 1.0, 0.0).astype(bf16)
        for h in range(2):
            got = jnp.dot(pick, xs[h, slot], preferred_element_type=f32)
            if slot:
                got = xg[h] + got
            xg[h] = got

    h_cp = [None] * 4

    def up_proj(slot):
        v = jnp.dot(xs[0, slot], wgu[pl.ds(0, 1024)], preferred_element_type=f32)
        v = v + jnp.dot(xs[1, slot], wgu[pl.ds(1024, 1024)], preferred_element_type=f32)
        hid[slot, :, pl.ds(ccol, 128)] = (silu(v[:, :128]) * v[:, 128:]).astype(bf16)
        view = hid.at[slot, :, pl.ds(ccol, 128)]
        h_cp[slot] = sems.copy(view, view, partner)

    ones = jnp.ones((8, 256), bf16)

    def down_proj(slot):
        h_cp[slot].wait_recv()
        dens[slot] = jnp.dot(hid[slot], wd[...], preferred_element_type=f32).astype(bf16)

    def squares(slot):
        hf = hid[slot].astype(f32)
        s = lax.dot_general(
            ones, (hf * hf).astype(bf16), (((1,), (1,)), ((), ())), preferred_element_type=f32
        )
        for p in range(3):
            sq[slot, p] = s[0:1, p * 128:(p + 1) * 128]

    def arrive(slot):
        for cp in d2d[slot]:
            cp.wait_recv()

    loads[0].wait()
    loads[1].wait()
    arrive(0)
    up_proj(0)
    select(0)

    relay = []
    for p in range(3):
        cdim = (p + 2) % 3
        g3[p][0].wait_recv()
        relay.append(sems.copy(xs.at[core, 1, lo(p)], xs.at[core, 3, lo(p)], peer(cdim, 1)))
        g3[p][1].wait_recv()
        relay.append(sems.copy(xs.at[core, 2, hi(p)], xs.at[core, 3, hi(p)], peer(cdim, 3)))
        share(1, p, 0, 64)
        share(2, p, 64, 64)
    for p in range(3):
        g3[p][2].wait_recv()
        share(1, p, 64, 64)
        g3[p][3].wait_recv()
        share(2, p, 0, 64)

    arrive(1)
    up_proj(1)
    arrive(2)
    up_proj(2)
    loads[2].wait()
    wd_cp.wait_recv()
    down_proj(1)
    for p in range(3):
        relay[2 * p].wait_recv()
        share(3, p, 0, 64)
        relay[2 * p + 1].wait_recv()
        share(3, p, 64, 64)
    down_proj(2)

    s1 = []
    for p in range(3):
        cdim = (p + 2) % 3
        s1.append([
            sems.copy(dens.at[2, hi(p)], rl.at[p, hi(0)], peer(cdim, 1)),
            sems.copy(dens.at[1, lo(p)], rr.at[p, lo(0)], peer(cdim, 3)),
        ])

    arrive(3)
    up_proj(3)
    select(1)
    select(2)
    down_proj(3)
    far = []
    for p in range(3):
        cdim = (p + 2) % 3
        far.append([
            sems.copy(dens.at[3, pl.ds(p * 128 + q * 32, 32)], buf.at[p, q % 2], peer(cdim, k))
            for q, buf, k in ((1, ql, 1), (2, qr, 3), (0, ql, 1), (3, qr, 3))
        ])
    select(3)
    for slot in (1, 2, 3):
        squares(slot)
    for p in range(3):
        cdim = (p + 2) % 3
        s1[p] += [
            sems.copy(sq.at[2, p], sq1.at[p, 0], peer(cdim, 1)),
            sems.copy(sq.at[1, p], sq1.at[p, 1], peer(cdim, 3)),
            sems.copy(sq.at[3, p], sq1.at[p, 2], peer(cdim, 2)),
        ]

    for i in (3, 4, 5):
        loads[i].wait()
    x0, x1 = xg[0].astype(bf16), xg[1].astype(bf16)
    gate = jnp.dot(x0, eg[pl.ds(0, 1024)], preferred_element_type=f32)
    gate = gate + jnp.dot(x1, eg[pl.ds(1024, 1024)], preferred_element_type=f32)
    up = jnp.dot(x0, eu[pl.ds(0, 1024)], preferred_element_type=f32)
    up = up + jnp.dot(x1, eu[pl.ds(1024, 1024)], preferred_element_type=f32)
    act = (silu(gate) * up).astype(bf16)
    ep_send[...] = jnp.dot(act, ed[:, pl.ds(ohalf, 1024)], preferred_element_type=f32).astype(bf16)
    ep_cp = sems.copy(ep_send, ep_recv, partner)
    mine = jnp.dot(act, ed[:, pl.ds(half, 1024)], preferred_element_type=f32).astype(bf16)

    down_proj(0)
    squares(0)

    sums = [[None] * 4 for _ in range(3)]
    for i, (q, near, came, out, to, k) in enumerate((
        (1, 2, ql, sl, rl, 1), (2, 1, qr, sr, rr, 3), (0, 2, ql, sl, rl, 1), (3, 1, qr, sr, rr, 3)
    )):
        for p in range(3):
            far[p][i].wait_recv()
            mix = dens[near, pl.ds(p * 128 + q * 32, 32)].astype(f32) + came[p, q % 2].astype(f32)
            out[p, q % 2] = mix.astype(bf16)
            sums[p][q] = sems.copy(
                out.at[p, q % 2], to.at[p, pl.ds(q * 32, 32)], peer((p + 2) % 3, k)
            )

    ep_cp.wait_recv()
    rows = (mine.astype(f32) + ep_recv[...].astype(f32)).astype(bf16).astype(f32)
    for s in range(2):
        for t in range(8):
            ret_f[pl.ds(s * 8 + t, 64, stride=16), :] = rows[s * 64:(s + 1) * 64, t * 128:(t + 1) * 128]
    ret_b[...] = ret_f[...].astype(bf16).reshape(64, 16, 128)

    s2 = [[] for _ in range(3)]
    for p in range(3):
        for cp in s1[p]:
            cp.wait_recv()
        v = sq[0, p] + sq1[p, 0] + sq1[p, 1] + sq1[p, 2]
        sq2[p, 0] = v
        for k in range(1, 4):
            sq2[p, k] = pltpu.roll(v, 128 - 32 * k, 1)
            s2[p].append(sems.copy(sq2.at[p, k], sq2r.at[p, k - 1], peer((p + 1) % 3, k)))
    for q in (2, 1, 3, 0):
        for p in range(3):
            sums[p][q].wait_recv()
            rows = pl.ds(q * 32, 32)
            total = dens[0, pl.ds(p * 128 + q * 32, 32)].astype(f32)
            total = total + rl[p, rows].astype(f32) + rr[p, rows].astype(f32)
            t2[p, q] = total.astype(bf16)
            if q:
                s2[p].append(sems.copy(t2.at[p, q], r2.at[p, q - 1], peer((p + 1) % 3, q)))

    @pl.loop(1, 64)
    def _(i):
        owner = (coords[0] + i % 4) % 4 + (coords[1] + (i // 4) % 4) % 4 * 4 + (coords[2] + i // 16) % 4 * 16
        pltpu.make_async_remote_copy(
            src_ref=ret_b.at[i],
            dst_ref=back.at[me],
            send_sem=back_sems.at[0],
            recv_sem=back_sems.at[1],
            device_id=(owner, core),
            device_id_type=MESH,
        ).start()

    back[me] = ret_b[0]
    s3 = []
    for p in range(3):
        for cp in s2[p]:
            cp.wait_recv()
        total = t2[p, 0].astype(f32)
        for k in range(3):
            total = total + r2[p, k].astype(f32)
        for k in range(4):
            t3[p, k] = total[k * 8:(k + 1) * 8].astype(bf16)
        v = sq2[p, 0] + sq2r[p, 0] + sq2r[p, 1] + sq2r[p, 2]
        sq3[p, 0] = v
        for k in range(1, 4):
            sq3[p, k] = pltpu.roll(v, 128 - 8 * k, 1)
        s3.append([
            sems.copy(t3.at[p, k], r3.at[p, k - 1], peer(p, k)) for k in (1, 3, 2)
        ] + [
            sems.copy(sq3.at[p, k], sq3r.at[p, k - 1], peer(p, k)) for k in (1, 3, 2)
        ])

    pltpu.make_async_copy(back.at[pl.ds(0, 63)], back.at[pl.ds(0, 63)], back_sems.at[1]).wait()
    ret_f[...] = back[...].reshape(1024, 128).astype(f32)
    mixes = []
    for t in range(8):
        m = 0.0
        for s in range(2):
            m = m + jnp.dot(
                comb_s[s], ret_f[pl.ds(s * 8 + t, 64, stride=16), :],
                preferred_element_type=f32, precision=lax.Precision.HIGHEST,
            )
        mixes.append(m)
    expert_sum = jnp.concatenate(mixes, axis=1)

    eye = lax.broadcasted_iota(jnp.int32, (8, 128), 0) == lax.broadcasted_iota(jnp.int32, (8, 128), 1)
    for p in range(3):
        for cp in s3[p]:
            cp.wait_recv()
        total = t3[p, 0].astype(f32)
        v = sq3[p, 0]
        for k in range(3):
            total = total + r3[p, k].astype(f32)
            v = v + sq3r[p, k]
        square = jnp.sum(jnp.where(eye, v, 0.0), axis=1, keepdims=True)
        dense = (total * lax.rsqrt(square / FF2 + norm_eps)).astype(bf16).astype(f32)
        mixed = resid_s[p, :, pl.ds(half, 1024)] + expert_sum[p * 8:(p + 1) * 8] + branch[p] * dense
        out_ref[p] = mixed.astype(bf16)

    for cp in sems.sent:
        cp.wait_send()
    pltpu.make_async_copy(back.at[pl.ds(0, 63)], back.at[pl.ds(0, 63)], back_sems.at[0]).wait()


def fused_layer(lens, *args):
    V = pltpu.VMEM
    vm = pl.BlockSpec(memory_space=pltpu.VMEM)
    hbm = pl.BlockSpec(memory_space=pl.ANY)
    scratch = [
        V((24, 2048), bf16),
        V((16, 128), bf16),
        V((16, 128), bf16),
        V((16, 128), bf16),
        V((1, 64), bf16),
        V((1, 64), bf16),
        V((1, 16), f32),
        V((2, 24), jnp.int32),
        V((2, 24), f32),
        V((2048, 512), bf16),
        V((2048, 128), bf16),
        V((2048, 128), bf16),
        V((16, 2048), bf16),
        V((24, 64, 1024), bf16),
        V((24, 64, 1024), bf16),
        V((24, 8, 1024), f32),
        V((512, 2048), bf16),
        V((8, 2048), f32),
        V((192, 128), f32),
        V((24, 64), f32),
        V((24, 64), f32),
        V((192, 128), f32),
        V((24, 512), f32),
        V((2, 24, 64), f32),
        V((3, 8, 2048), bf16),
        V((3, 8, 2048), bf16),
        V((3, 8, 2048), f32),
        V((3, 8, 2048), bf16),
        V((3, 4, 8, 1024), bf16),
        V((2, 4, 384, 1024), bf16),
        V((4, 384, 256), bf16),
        V((2048, 256), bf16),
        V((256, 1024), bf16),
        V((2048, 512), bf16),
        V((2048, 512), bf16),
        V((512, 2048), bf16),
        V((64, 1, 128), f32),
        V((64, 128), f32),
        V((2, 128, 1024), f32),
        V((4, 384, 1024), bf16),
        V((3, 128, 1024), bf16),
        V((3, 128, 1024), bf16),
        V((3, 2, 32, 1024), bf16),
        V((3, 2, 32, 1024), bf16),
        V((3, 2, 32, 1024), bf16),
        V((3, 2, 32, 1024), bf16),
        V((3, 4, 32, 1024), bf16),
        V((3, 3, 32, 1024), bf16),
        V((3, 4, 8, 1024), bf16),
        V((3, 3, 8, 1024), bf16),
        V((4, 3, 1, 128), f32),
        V((3, 3, 1, 128), f32),
        V((3, 4, 1, 128), f32),
        V((3, 3, 1, 128), f32),
        V((3, 4, 1, 128), f32),
        V((3, 3, 1, 128), f32),
        V((128, 1024), bf16),
        V((128, 1024), bf16),
        V((1024, 128), f32),
        V((64, 16, 128), bf16),
        V((64, 16, 128), bf16),
        pltpu.SemaphoreType.DMA((192,)),
        pltpu.SemaphoreType.DMA((192,)),
        pltpu.SemaphoreType.DMA((7,)),
        pltpu.SemaphoreType.DMA((13,)),
        pltpu.SemaphoreType.DMA((3, 24 // GROUP)),
        pltpu.SemaphoreType.DMA((2,)),
    ]
    return pl.pallas_call(
        layer_kernel,
        out_shape=(
            pltpu.VMEM((3, 8, 1024), bf16),
            pltpu.VMEM((24, 64), bf16),
            pltpu.VMEM((24, 64), bf16),
            pltpu.VMEM((8, 24), f32),
        ),
        in_specs=[pl.BlockSpec(memory_space=pltpu.SMEM)] + [hbm] * len(args),
        out_specs=(vm,) * 4,
        scratch_shapes=scratch,
        compiler_params=pltpu.CompilerParams(
            collective_id=0, has_side_effects=True, vmem_limit_bytes=56 * 1024 * 1024
        ),
    )(lens, *args)


def finish(*arrays):
    def kernel(*refs):
        for src, dst in zip(refs[:4], refs[4:]):
            dst[...] = src[...]

    return pl.pallas_call(
        kernel,
        out_shape=tuple(jax.ShapeDtypeStruct(a.shape, a.dtype) for a in arrays),
        in_specs=[pl.BlockSpec(memory_space=pltpu.VMEM)] * 4,
        out_specs=(pl.BlockSpec(memory_space=pltpu.VMEM),) * 4,
    )(*arrays)


def body(
    tokens,
    norm_gain,
    query_w,
    key_w,
    value_w,
    forget_w,
    forget_bias,
    query_gain,
    key_gain,
    cache_key,
    cache_value,
    cache_gate,
    cache_len,
    out_w,
    post_gain,
    branch_gate,
    dense_gate_w,
    dense_up_w,
    dense_down_w,
    expert_choice,
    route_weight,
    expert_gate_w,
    expert_up_w,
    expert_down_w,
):
    mixed, fresh_key, fresh_value, fresh_gate = fused_layer(
        cache_len,
        tokens,
        norm_gain.reshape(16, 128),
        post_gain.reshape(16, 128),
        branch_gate.reshape(16, 128),
        query_gain.reshape(1, 64),
        key_gain.reshape(1, 64),
        forget_bias.reshape(1, 16),
        expert_choice.T,
        route_weight.T,
        query_w,
        key_w,
        value_w,
        forget_w.T,
        cache_key.reshape(24, 64, 1024),
        cache_value.reshape(24, 64, 1024),
        cache_gate,
        out_w,
        dense_gate_w,
        dense_up_w,
        dense_down_w,
        expert_gate_w.reshape(2048, 512),
        expert_up_w.reshape(2048, 512),
        expert_down_w.reshape(512, 2048),
    )
    mixed, fresh_key, fresh_value, fresh_gate = finish(
        mixed.reshape(24, 1024), fresh_key, fresh_value, fresh_gate
    )
    return (
        mixed,
        fresh_key.reshape(24, 1, 64),
        fresh_value.reshape(24, 1, 64),
        fresh_gate.T,
    )


def solution(mesh):
    placed = (
        P("ep", None),
        P(),
        P(None, "tp"),
        P(),
        P(),
        P(),
        P(),
        P(),
        P(),
        P("ep", "tp", None, None),
        P("ep", "tp", None, None),
        P("ep", "tp", None),
        P("ep"),
        P("tp", None),
        P(),
        P(),
        P(None, ("ep", "tp")),
        P(None, ("ep", "tp")),
        P(("ep", "tp"), None),
        P("ep", None),
        P("ep", None),
        P("ep", None, "tp"),
        P("ep", None, "tp"),
        P("ep", "tp", None),
    )
    return jax.shard_map(
        body,
        mesh=mesh,
        in_specs=placed,
        out_specs=(P("ep", "tp"), P("ep", "tp", None), P("ep", "tp", None), P("ep", "tp")),
        check_vma=False,
    )
```

```python
import math
import functools

import jax
import jax.numpy as jnp
from jax import lax
from jax.experimental import pallas as pl
from jax.experimental.pallas import tpu as pltpu
from jax.sharding import PartitionSpec as P

FF2 = 16384
norm_eps = 1e-06
GROUP = 8
MESH = pl.DeviceIdType.MESH
f32, bf16 = jnp.float32, jnp.bfloat16


class Sems:
    def __init__(self, send, recv):
        self.send, self.recv, self.n = send, recv, 0
        self.sent = []

    def copy(self, src, dst, device):
        i = self.n
        self.n += 1
        cp = pltpu.make_async_remote_copy(
            src_ref=src,
            dst_ref=dst,
            send_sem=self.send.at[i],
            recv_sem=self.recv.at[i],
            device_id=device,
            device_id_type=MESH,
        )
        cp.start()
        self.sent.append(cp)
        return cp


def silu(v):
    return v / (1.0 + jnp.exp(-v))


def layer_kernel(
    len_ref, tokens_h, ngain_h, pgain_h, bgate_h, qgain_h, kgain_h, fbias_h, choice_h, rweight_h,
    qw_h, kw_h, vw_h, fw_h, kc_h, vc_h, cg_h, ow_h,
    dg_h, du_h, dd_h, eg_h, eu_h, ed_h,
    out_ref, fk_ref, fv_ref, fg_ref,
    tok_s, ngain_s, pgain_s, bgate_s, qgain_s, kgain_s, fbias_s, choice_s, rweight_s,
    qw, kw, vw, fw, kc, vc, cg, ow, rows_s, q_s, kf_s, vf_s, o_s, ah_s, comb_s,
    partial_s, partner_part, resid_s, pn_s, a1, xs, hid, wgu, wd, eg, eu, ed,
    meta_all, meta_tab, xg, dens, rl, rr, ql, qr, sl, sr, t2, r2, t3, r3,
    sq, sq1, sq2, sq2r, sq3, sq3r, ep_send, ep_recv, ret_f, ret_b, back,
    send_sem, recv_sem, load_sem, small_sem, cache_sem, back_sems,
):
    me = lax.axis_index("ep")
    core = lax.axis_index("tp")
    other = 1 - core
    coords = (me % 4, (me // 4) % 4, me // 16)
    weights = (1, 4, 16)
    partner = (me, other)
    half = pl.multiple_of(core * 1024, 1024)
    ohalf = pl.multiple_of(other * 1024, 1024)
    ccol = pl.multiple_of(core * 128, 128)

    def peer(dim, k):
        v = coords[dim]
        return (me + (((v + k) % 4) - v) * weights[dim], core)

    sems = Sems(send_sem, recv_sem)

    barrier = pltpu.get_barrier_semaphore()
    pl.semaphore_signal(barrier, inc=1, device_id=partner, device_id_type=MESH)

    for dim in range(3):
        for k in (1, 2, 3):
            pl.semaphore_signal(barrier, inc=1, device_id=peer(dim, k), device_id_type=MESH)

    smalls = []
    for i, (src, dst) in enumerate((
        (tokens_h, tok_s), (ngain_h, ngain_s), (choice_h, choice_s), (rweight_h, rweight_s),
        (qw_h, qw), (kw_h, kw), (vw_h, vw), (fw_h, fw), (fbias_h, fbias_s),
        (qgain_h, qgain_s), (kgain_h, kgain_s), (pgain_h, pgain_s), (bgate_h, bgate_s),
    )):
        cp = pltpu.make_async_copy(src, dst, small_sem.at[i])
        cp.start()
        smalls.append(cp)

    def cache_copies(g):
        rows = pl.ds(g * GROUP, GROUP)
        return [
            pltpu.make_async_copy(src.at[rows], dst.at[rows], cache_sem.at[i, g])
            for i, (src, dst) in enumerate(((kc_h, kc), (cg_h, cg), (vc_h, vc)))
        ]

    loads = []
    for i, (src, dst) in enumerate((
        (dg_h, wgu.at[:, pl.ds(0, 128)]),
        (du_h, wgu.at[:, pl.ds(128, 128)]),
        (dd_h.at[:, pl.ds(half, 1024)], wd.at[pl.ds(ccol, 128)]),
        (eg_h, eg),
        (eu_h, eu),
        (ed_h, ed),
        (ow_h, ow),
    )):
        loads.append(pltpu.make_async_copy(src, dst, load_sem.at[i]))
    smalls[4].wait()
    for g in range(24 // GROUP):
        for cp in cache_copies(g):
            cp.start()
    loads[6].start()

    for i in (1, 11, 12):
        smalls[i].wait()
    for i, src in enumerate((ngain_s, pgain_s, bgate_s)):
        v = src[...].astype(f32)
        for t in range(16):
            rows_s[pl.ds(i, 1), pl.ds(t * 128, 128)] = v[t:t + 1]
    smalls[0].wait()
    toks = tok_s[...].astype(f32)
    mean_square = jnp.mean(toks * toks, axis=-1, keepdims=True)
    normed = (toks * lax.rsqrt(mean_square + norm_eps) * rows_s[pl.ds(0, 1), :]).astype(bf16)

    def head_norm(v, gain):
        return v * lax.rsqrt(jnp.mean(v * v, axis=-1, keepdims=True) + norm_eps) * gain

    q_all = jnp.dot(normed, qw[...], preferred_element_type=f32)
    smalls[9].wait()
    qg = qgain_s[...].astype(f32)
    for h in range(8):
        q = head_norm(q_all[:, h * 64:(h + 1) * 64], qg).astype(bf16).astype(f32)
        q_s[pl.ds(h, 24, stride=8), :] = jnp.concatenate([q, jnp.zeros_like(q)], axis=1)
    smalls[5].wait()
    smalls[10].wait()
    k_all = jnp.dot(normed, kw[...], preferred_element_type=f32)
    k_own = head_norm(jnp.where(core == 0, k_all[:, :64], k_all[:, 64:]), kgain_s[...].astype(f32))
    fk_ref[...] = k_own.astype(bf16)
    kf_s[...] = k_own.astype(bf16).astype(f32)
    smalls[6].wait()
    v_all = jnp.dot(normed, vw[...], preferred_element_type=f32)
    v_own = jnp.where(core == 0, v_all[:, :64], v_all[:, 64:]).astype(bf16)
    fv_ref[...] = v_own
    vf_s[...] = v_own.astype(f32)
    smalls[7].wait()
    smalls[8].wait()
    forget = lax.dot_general(
        fw[...], normed, (((1,), (1,)), ((), ())), preferred_element_type=f32
    )
    pick16 = lax.broadcasted_iota(jnp.int32, (16, 16), 0) == lax.broadcasted_iota(jnp.int32, (16, 16), 1)
    forget = forget + jnp.sum(jnp.where(pick16, fbias_s[...], 0.0), axis=1, keepdims=True)
    log_forget = jnp.minimum(forget, 0.0) - jnp.log1p(jnp.exp(-jnp.abs(forget)))
    log_forget = jnp.where(core == 0, log_forget[:8], log_forget[8:])

    slot_at = lax.broadcasted_iota(jnp.int32, (8, 1024), 1)
    seq_lane = lax.broadcasted_iota(jnp.int32, (8, 24), 1)
    scale = 64 ** (-0.5)

    def score_group(g, gates):
        for cp in cache_copies(g):
            cp.wait()
        for i in range(GROUP):
            s = g * GROUP + i
            rows = pl.ds(pl.multiple_of(s * 8, 8), 8)
            length = len_ref[s]
            q = q_s[rows, :][:, :64]
            score = jnp.dot(q.astype(bf16), kc[s], preferred_element_type=f32) * scale
            gate = cg[s]
            current = jnp.sum(jnp.where(slot_at == length - 1, gate, 0.0), axis=1, keepdims=True)
            current = current + jnp.sum(
                jnp.where(seq_lane == s, log_forget, 0.0), axis=1, keepdims=True
            )
            gates = jnp.where(seq_lane == s, current, gates)
            own = jnp.sum(q * kf_s[pl.ds(s, 1), :], axis=1, keepdims=True) * scale
            logit = jnp.where(slot_at < length, score + (current - gate), -jnp.inf)
            top = jnp.maximum(jnp.max(logit, axis=1, keepdims=True), own)
            cg[s] = logit - top
            o_s[rows, :] = jnp.broadcast_to(own - top, (8, 128))
        return gates

    def mix_group(g, carry):
        for i in range(GROUP):
            s = g * GROUP + i
            rows = pl.ds(pl.multiple_of(s * 8, 8), 8)
            w = jnp.exp(cg[s])
            own_w = jnp.exp(o_s[rows, :][:, :64])
            inv = 1.0 / (jnp.sum(w, axis=1, keepdims=True) + own_w)
            o = lax.dot_general(
                w.astype(bf16), vc[s], (((1,), (1,)), ((), ())), preferred_element_type=f32
            )
            o = (o + own_w.astype(bf16).astype(f32) * vf_s[pl.ds(s, 1), :]) * inv
            o_s[rows, :] = jnp.concatenate([o, jnp.zeros_like(o)], axis=1)
        return carry

    gates = lax.fori_loop(0, 24 // GROUP, score_group, jnp.zeros((8, 24), f32))
    lax.fori_loop(0, 24 // GROUP, mix_group, 0)
    fg_ref[...] = gates
    for cp in loads[:6]:
        cp.start()
    for h in range(8):
        ah_s[:, pl.ds(h * 64, 64)] = o_s[pl.ds(h, 24, stride=8), :][:, :64]
    loads[6].wait()
    partial = jnp.dot(ah_s[...].astype(bf16), ow[...], preferred_element_type=f32)
    partial_s[...] = partial.reshape(3, 8, 2048).astype(bf16)

    pl.semaphore_wait(barrier, 10)

    part_cp = sems.copy(partial_s, partner_part, partner)
    wd_cp = sems.copy(dd_h.at[:, pl.ds(ohalf, 1024)], wd.at[pl.ds(ccol, 128)], partner)

    meta_all[0] = jnp.full((1, 128), -1.0, f32)

    def column(row):
        pick = lax.broadcasted_iota(jnp.int32, (24, 24), 0) == lax.broadcasted_iota(jnp.int32, (24, 24), 1)
        return jnp.sum(jnp.where(pick, row, jnp.zeros_like(row)), axis=1, keepdims=True)

    smalls[2].wait()
    smalls[3].wait()
    choice = choice_s[...].astype(f32)
    named = [choice[k:k + 1, :] for k in range(2)]
    named_col = [column(v) for v in named]
    earlier = lax.broadcasted_iota(jnp.int32, (24, 24), 0) < lax.broadcasted_iota(jnp.int32, (24, 24), 1)
    targets = []
    for k in range(2):
        again = jnp.zeros((1, 24), f32)
        for i in range(2):
            same = jnp.where(earlier & (named_col[i] == named[k]), 1.0, 0.0)
            again = again + jnp.sum(same, axis=0, keepdims=True)
        targets.append(named[k] * 2.0 + jnp.minimum(again, 1.0))
    meta_all[0, :, pl.ds(0, 24)] = targets[0] + 128.0 * targets[1]
    target_col = [column(v) for v in targets]
    weight_col = [column(rweight_s[k:k + 1, :]) for k in range(2)]
    place = lax.broadcasted_iota(jnp.int32, (24, 64), 1).astype(f32) * 2.0
    for t in range(2):
        m = jnp.where(target_col[0] == place + t, weight_col[0], 0.0)
        comb_s[t] = m + jnp.where(target_col[1] == place + t, weight_col[1], 0.0)

    part_cp.wait_recv()
    attn = partial_s[...].astype(f32) + partner_part[...].astype(f32)
    resid = (tok_s[...].astype(f32).reshape(3, 8, 2048) + attn).astype(bf16).astype(f32)
    resid_s[...] = resid
    mean_square = jnp.mean(resid * resid, axis=-1, keepdims=True)
    gain = rows_s[pl.ds(1, 1), :][None]
    post = (resid * lax.rsqrt(mean_square + norm_eps) * gain).astype(bf16)
    pn_s[...] = post
    a1[:, 0] = pn_s[:, :, pl.ds(half, 1024)]

    def meta_stage(dim, size):
        return [
            sems.copy(meta_all.at[pl.ds(0, size)], meta_all.at[pl.ds((4 - k) * size, size)], peer(dim, k))
            for k in (1, 3, 2)
        ]

    meta_cp = meta_stage(0, 1)
    g1 = [
        [sems.copy(a1.at[p, 0], a1.at[p, 4 - k], peer(p, k)) for k in (1, 3, 2)]
        for p in range(3)
    ]

    branch = jax.nn.sigmoid(
        jnp.sum(post.astype(f32) * rows_s[pl.ds(2, 1), :][None], axis=-1, keepdims=True)
    )

    g2 = []
    for p in range(3):
        if p == 0:
            for cp in meta_cp:
                cp.wait_recv()
            meta_cp = meta_stage(1, 4)
        for cp in g1[p]:
            cp.wait_recv()
        for pair in range(2):
            rows = jnp.concatenate(
                [a1[p, 2 * pair].astype(f32), a1[p, 2 * pair + 1].astype(f32)], axis=0
            )
            xs[core, 0, pl.ds(p * 128 + pair * 16, 16)] = rows.astype(bf16)
        line = xs.at[core, 0, pl.ds(p * 128, 32)]
        g2.append([
            sems.copy(line, xs.at[core, 0, pl.ds(p * 128 + (4 - k) * 32, 32)], peer((p + 1) % 3, k))
            for k in (1, 3, 2)
        ])

    g3, d2d = [], [[] for _ in range(4)]

    def share(slot, p, start, size):
        view = xs.at[core, slot, pl.ds(p * 128 + start, size)]
        d2d[slot].append(sems.copy(view, view, partner))

    lo, hi = (lambda p: pl.ds(p * 128, 64)), (lambda p: pl.ds(p * 128 + 64, 64))
    first, second = (lambda p: pl.ds(p * 128, 32)), (lambda p: pl.ds(p * 128 + 32, 32))
    own = xs.at[core, 0]
    early = [
        [
            sems.copy(own.at[first(p)], xs.at[core, slot, first(p)], peer((p + 2) % 3, k))
            for slot, k in ((1, 1), (2, 3))
        ]
        for p in range(3)
    ]
    for p in range(3):
        if p == 0:
            for cp in meta_cp:
                cp.wait_recv()
            meta_cp = meta_stage(2, 16)
        for cp in g2[p]:
            cp.wait_recv()
        cdim = (p + 2) % 3
        g3.append([
            sems.copy(own.at[rows], xs.at[core, slot, rows], peer(cdim, k))
            for slot, k, rows in ((1, 1, second(p)), (2, 3, hi(p)), (1, 1, hi(p)), (2, 3, second(p)))
        ])
        share(0, p, 0, 128)

    for cp in meta_cp:
        cp.wait_recv()
    for d in range(64):
        meta_tab[pl.ds(d, 1), :] = meta_all[d]
    table = meta_tab[...].astype(jnp.int32)
    lane = lax.broadcasted_iota(jnp.int32, (64, 128), 1)
    dev = lax.broadcasted_iota(jnp.int32, (64, 1), 0)
    shift = [(dev >> s) & 3 for s in (0, 2, 4)]
    starts = []
    for p in range(3):
        ka, kb, kc = shift[p], shift[(p + 1) % 3], shift[(p + 2) % 3]
        slot = jnp.where(kc == 0, 0, jnp.where(kc == 1, 2, jnp.where(kc == 2, 3, 1)))
        starts.append(slot * 384 + p * 128 + kb * 32 + ka * 8)
    row_ids = []
    for s in range(2):
        want = me * 2 + s
        hit = (lane < 24) & (((table & 127) == want) | ((table >> 7) == want))
        tok = jnp.sum(jnp.where(hit, lane + 1, 0), axis=1, keepdims=True) - 1
        start = jnp.where(tok < 8, starts[0], jnp.where(tok < 16, starts[1], starts[2]))
        row_ids.append(jnp.where(tok < 0, -1, start + (tok & 7)))
    row_id = jnp.concatenate(row_ids, axis=0)
    cols = lax.broadcasted_iota(jnp.int32, (128, 384), 1)

    def select(slot):
        pick = jnp.where(row_id == cols + slot * 384, 1.0, 0.0).astype(bf16)
        for h in range(2):
            got = jnp.dot(pick, xs[h, slot], preferred_element_type=f32)
            if slot:
                got = xg[h] + got
            xg[h] = got

    h_cp = [None] * 4

    def up_proj(slot):
        v = jnp.dot(xs[0, slot], wgu[pl.ds(0, 1024)], preferred_element_type=f32)
        v = v + jnp.dot(xs[1, slot], wgu[pl.ds(1024, 1024)], preferred_element_type=f32)
        hid[slot, :, pl.ds(ccol, 128)] = (silu(v[:, :128]) * v[:, 128:]).astype(bf16)
        view = hid.at[slot, :, pl.ds(ccol, 128)]
        h_cp[slot] = sems.copy(view, view, partner)

    ones = jnp.ones((8, 256), bf16)

    def far_up(p):
        rows = pl.ds(p * 128, 128)
        v = jnp.dot(xs[0, 3, rows], wgu[pl.ds(0, 1024)], preferred_element_type=f32)
        v = v + jnp.dot(xs[1, 3, rows], wgu[pl.ds(1024, 1024)], preferred_element_type=f32)
        hid[3, rows, pl.ds(ccol, 128)] = (silu(v[:, :128]) * v[:, 128:]).astype(bf16)
        view = hid.at[3, rows, pl.ds(ccol, 128)]
        return sems.copy(view, view, partner)

    def down_proj(slot):
        h_cp[slot].wait_recv()
        dens[slot] = jnp.dot(hid[slot], wd[...], preferred_element_type=f32).astype(bf16)

    def squares(slot):
        hf = hid[slot].astype(f32)
        s = lax.dot_general(
            ones, (hf * hf).astype(bf16), (((1,), (1,)), ((), ())), preferred_element_type=f32
        )
        for p in range(3):
            sq[slot, p] = s[0:1, p * 128:(p + 1) * 128]

    def arrive(slot):
        for cp in d2d[slot]:
            cp.wait_recv()

    loads[0].wait()
    loads[1].wait()
    arrive(0)
    up_proj(0)
    select(0)

    relay = []
    for p in range(3):
        cdim = (p + 2) % 3
        early[p][0].wait_recv()
        g3[p][0].wait_recv()
        relay.append(sems.copy(xs.at[core, 1, lo(p)], xs.at[core, 3, lo(p)], peer(cdim, 1)))
        g3[p][1].wait_recv()
        relay.append(sems.copy(xs.at[core, 2, hi(p)], xs.at[core, 3, hi(p)], peer(cdim, 3)))
        share(1, p, 0, 64)
        share(2, p, 64, 64)
    for p in range(3):
        g3[p][2].wait_recv()
        share(1, p, 64, 64)
        early[p][1].wait_recv()
        g3[p][3].wait_recv()
        share(2, p, 0, 64)

    arrive(1)
    up_proj(1)
    arrive(2)
    up_proj(2)
    loads[2].wait()
    wd_cp.wait_recv()
    down_proj(1)
    for p in range(3):
        relay[2 * p].wait_recv()
        share(3, p, 0, 64)
        relay[2 * p + 1].wait_recv()
        share(3, p, 64, 64)
    down_proj(2)

    s1 = []
    for p in range(3):
        cdim = (p + 2) % 3
        s1.append([
            sems.copy(dens.at[2, hi(p)], rl.at[p, hi(0)], peer(cdim, 1)),
            sems.copy(dens.at[1, lo(p)], rr.at[p, lo(0)], peer(cdim, 3)),
        ])

    far_cp = []
    for p in range(3):
        for cp in d2d[3][2 * p:2 * p + 2]:
            cp.wait_recv()
        far_cp.append(far_up(p))
    select(1)
    select(2)
    far = []
    for p in range(3):
        cdim = (p + 2) % 3
        far_cp[p].wait_recv()
        rows = pl.ds(p * 128, 128)
        dens[3, rows] = jnp.dot(hid[3, rows], wd[...], preferred_element_type=f32).astype(bf16)
        far.append([
            sems.copy(dens.at[3, pl.ds(p * 128 + q * 32, 32)], buf.at[p, q % 2], peer(cdim, k))
            for q, buf, k in ((1, ql, 1), (2, qr, 3), (0, ql, 1), (3, qr, 3))
        ])
    select(3)
    for slot in (1, 2, 3):
        squares(slot)
    for p in range(3):
        cdim = (p + 2) % 3
        s1[p] += [
            sems.copy(sq.at[2, p], sq1.at[p, 0], peer(cdim, 1)),
            sems.copy(sq.at[1, p], sq1.at[p, 1], peer(cdim, 3)),
            sems.copy(sq.at[3, p], sq1.at[p, 2], peer(cdim, 2)),
        ]

    for i in (3, 4, 5):
        loads[i].wait()
    x0, x1 = xg[0].astype(bf16), xg[1].astype(bf16)
    gate = jnp.dot(x0, eg[pl.ds(0, 1024)], preferred_element_type=f32)
    gate = gate + jnp.dot(x1, eg[pl.ds(1024, 1024)], preferred_element_type=f32)
    up = jnp.dot(x0, eu[pl.ds(0, 1024)], preferred_element_type=f32)
    up = up + jnp.dot(x1, eu[pl.ds(1024, 1024)], preferred_element_type=f32)
    act = (silu(gate) * up).astype(bf16)
    ep_send[...] = jnp.dot(act, ed[:, pl.ds(ohalf, 1024)], preferred_element_type=f32).astype(bf16)
    ep_cp = sems.copy(ep_send, ep_recv, partner)
    mine = jnp.dot(act, ed[:, pl.ds(half, 1024)], preferred_element_type=f32).astype(bf16)

    down_proj(0)
    squares(0)

    sums = [[None] * 4 for _ in range(3)]
    for i, (q, near, came, out, to, k) in enumerate((
        (1, 2, ql, sl, rl, 1), (2, 1, qr, sr, rr, 3), (0, 2, ql, sl, rl, 1), (3, 1, qr, sr, rr, 3)
    )):
        for p in range(3):
            far[p][i].wait_recv()
            mix = dens[near, pl.ds(p * 128 + q * 32, 32)].astype(f32) + came[p, q % 2].astype(f32)
            out[p, q % 2] = mix.astype(bf16)
            sums[p][q] = sems.copy(
                out.at[p, q % 2], to.at[p, pl.ds(q * 32, 32)], peer((p + 2) % 3, k)
            )

    ep_cp.wait_recv()
    rows = (mine.astype(f32) + ep_recv[...].astype(f32)).astype(bf16).astype(f32)
    for s in range(2):
        for t in range(8):
            ret_f[pl.ds(s * 8 + t, 64, stride=16), :] = rows[s * 64:(s + 1) * 64, t * 128:(t + 1) * 128]
    ret_b[...] = ret_f[...].astype(bf16).reshape(64, 16, 128)

    s2 = [[] for _ in range(3)]
    for p in range(3):
        for cp in s1[p]:
            cp.wait_recv()
        v = sq[0, p] + sq1[p, 0] + sq1[p, 1] + sq1[p, 2]
        sq2[p, 0] = v
        for k in range(1, 4):
            sq2[p, k] = pltpu.roll(v, 128 - 32 * k, 1)
            s2[p].append(sems.copy(sq2.at[p, k], sq2r.at[p, k - 1], peer((p + 1) % 3, k)))
    for q in (2, 1, 3, 0):
        for p in range(3):
            sums[p][q].wait_recv()
            rows = pl.ds(q * 32, 32)
            total = dens[0, pl.ds(p * 128 + q * 32, 32)].astype(f32)
            total = total + rl[p, rows].astype(f32) + rr[p, rows].astype(f32)
            t2[p, q] = total.astype(bf16)
            if q:
                s2[p].append(sems.copy(t2.at[p, q], r2.at[p, q - 1], peer((p + 1) % 3, q)))

    @pl.loop(1, 64)
    def _(i):
        owner = (coords[0] + i % 4) % 4 + (coords[1] + (i // 4) % 4) % 4 * 4 + (coords[2] + i // 16) % 4 * 16
        pltpu.make_async_remote_copy(
            src_ref=ret_b.at[i],
            dst_ref=back.at[me],
            send_sem=back_sems.at[0],
            recv_sem=back_sems.at[1],
            device_id=(owner, core),
            device_id_type=MESH,
        ).start()

    back[me] = ret_b[0]
    s3 = []
    for p in range(3):
        for cp in s2[p]:
            cp.wait_recv()
        total = t2[p, 0].astype(f32)
        for k in range(3):
            total = total + r2[p, k].astype(f32)
        for k in range(4):
            t3[p, k] = total[k * 8:(k + 1) * 8].astype(bf16)
        v = sq2[p, 0] + sq2r[p, 0] + sq2r[p, 1] + sq2r[p, 2]
        sq3[p, 0] = v
        for k in range(1, 4):
            sq3[p, k] = pltpu.roll(v, 128 - 8 * k, 1)
        s3.append([
            sems.copy(t3.at[p, k], r3.at[p, k - 1], peer(p, k)) for k in (1, 3, 2)
        ] + [
            sems.copy(sq3.at[p, k], sq3r.at[p, k - 1], peer(p, k)) for k in (1, 3, 2)
        ])

    pltpu.make_async_copy(back.at[pl.ds(0, 63)], back.at[pl.ds(0, 63)], back_sems.at[1]).wait()
    ret_f[...] = back[...].reshape(1024, 128).astype(f32)
    mixes = []
    for t in range(8):
        m = 0.0
        for s in range(2):
            m = m + jnp.dot(
                comb_s[s], ret_f[pl.ds(s * 8 + t, 64, stride=16), :],
                preferred_element_type=f32, precision=lax.Precision.HIGHEST,
            )
        mixes.append(m)
    expert_sum = jnp.concatenate(mixes, axis=1)

    eye = lax.broadcasted_iota(jnp.int32, (8, 128), 0) == lax.broadcasted_iota(jnp.int32, (8, 128), 1)
    for p in range(3):
        for cp in s3[p]:
            cp.wait_recv()
        total = t3[p, 0].astype(f32)
        v = sq3[p, 0]
        for k in range(3):
            total = total + r3[p, k].astype(f32)
            v = v + sq3r[p, k]
        square = jnp.sum(jnp.where(eye, v, 0.0), axis=1, keepdims=True)
        dense = (total * lax.rsqrt(square / FF2 + norm_eps)).astype(bf16).astype(f32)
        mixed = resid_s[p, :, pl.ds(half, 1024)] + expert_sum[p * 8:(p + 1) * 8] + branch[p] * dense
        out_ref[p] = mixed.astype(bf16)

    for cp in sems.sent:
        cp.wait_send()
    pltpu.make_async_copy(back.at[pl.ds(0, 63)], back.at[pl.ds(0, 63)], back_sems.at[0]).wait()


def fused_layer(lens, *args):
    V = pltpu.VMEM
    vm = pl.BlockSpec(memory_space=pltpu.VMEM)
    hbm = pl.BlockSpec(memory_space=pl.ANY)
    scratch = [
        V((24, 2048), bf16),
        V((16, 128), bf16),
        V((16, 128), bf16),
        V((16, 128), bf16),
        V((1, 64), bf16),
        V((1, 64), bf16),
        V((1, 16), f32),
        V((2, 24), jnp.int32),
        V((2, 24), f32),
        V((2048, 512), bf16),
        V((2048, 128), bf16),
        V((2048, 128), bf16),
        V((16, 2048), bf16),
        V((24, 64, 1024), bf16),
        V((24, 64, 1024), bf16),
        V((24, 8, 1024), f32),
        V((512, 2048), bf16),
        V((8, 2048), f32),
        V((192, 128), f32),
        V((24, 64), f32),
        V((24, 64), f32),
        V((192, 128), f32),
        V((24, 512), f32),
        V((2, 24, 64), f32),
        V((3, 8, 2048), bf16),
        V((3, 8, 2048), bf16),
        V((3, 8, 2048), f32),
        V((3, 8, 2048), bf16),
        V((3, 4, 8, 1024), bf16),
        V((2, 4, 384, 1024), bf16),
        V((4, 384, 256), bf16),
        V((2048, 256), bf16),
        V((256, 1024), bf16),
        V((2048, 512), bf16),
        V((2048, 512), bf16),
        V((512, 2048), bf16),
        V((64, 1, 128), f32),
        V((64, 128), f32),
        V((2, 128, 1024), f32),
        V((4, 384, 1024), bf16),
        V((3, 128, 1024), bf16),
        V((3, 128, 1024), bf16),
        V((3, 2, 32, 1024), bf16),
        V((3, 2, 32, 1024), bf16),
        V((3, 2, 32, 1024), bf16),
        V((3, 2, 32, 1024), bf16),
        V((3, 4, 32, 1024), bf16),
        V((3, 3, 32, 1024), bf16),
        V((3, 4, 8, 1024), bf16),
        V((3, 3, 8, 1024), bf16),
        V((4, 3, 1, 128), f32),
        V((3, 3, 1, 128), f32),
        V((3, 4, 1, 128), f32),
        V((3, 3, 1, 128), f32),
        V((3, 4, 1, 128), f32),
        V((3, 3, 1, 128), f32),
        V((128, 1024), bf16),
        V((128, 1024), bf16),
        V((1024, 128), f32),
        V((64, 16, 128), bf16),
        V((64, 16, 128), bf16),
        pltpu.SemaphoreType.DMA((192,)),
        pltpu.SemaphoreType.DMA((192,)),
        pltpu.SemaphoreType.DMA((7,)),
        pltpu.SemaphoreType.DMA((13,)),
        pltpu.SemaphoreType.DMA((3, 24 // GROUP)),
        pltpu.SemaphoreType.DMA((2,)),
    ]
    return pl.pallas_call(
        layer_kernel,
        out_shape=(
            jax.ShapeDtypeStruct((3, 8, 1024), bf16),
            jax.ShapeDtypeStruct((24, 64), bf16),
            jax.ShapeDtypeStruct((24, 64), bf16),
            jax.ShapeDtypeStruct((8, 24), f32),
        ),
        in_specs=[pl.BlockSpec(memory_space=pltpu.SMEM)] + [hbm] * len(args),
        out_specs=(vm,) * 4,
        scratch_shapes=scratch,
        compiler_params=pltpu.CompilerParams(
            collective_id=0, has_side_effects=True, vmem_limit_bytes=56 * 1024 * 1024
        ),
    )(lens, *args)


def finish(*arrays):
    def kernel(*refs):
        for src, dst in zip(refs[:4], refs[4:]):
            dst[...] = src[...]

    return pl.pallas_call(
        kernel,
        out_shape=tuple(jax.ShapeDtypeStruct(a.shape, a.dtype) for a in arrays),
        in_specs=[pl.BlockSpec(memory_space=pltpu.VMEM)] * 4,
        out_specs=(pl.BlockSpec(memory_space=pltpu.VMEM),) * 4,
    )(*arrays)


def body(
    tokens,
    norm_gain,
    query_w,
    key_w,
    value_w,
    forget_w,
    forget_bias,
    query_gain,
    key_gain,
    cache_key,
    cache_value,
    cache_gate,
    cache_len,
    out_w,
    post_gain,
    branch_gate,
    dense_gate_w,
    dense_up_w,
    dense_down_w,
    expert_choice,
    route_weight,
    expert_gate_w,
    expert_up_w,
    expert_down_w,
):
    mixed, fresh_key, fresh_value, fresh_gate = fused_layer(
        cache_len,
        tokens,
        norm_gain.reshape(16, 128),
        post_gain.reshape(16, 128),
        branch_gate.reshape(16, 128),
        query_gain.reshape(1, 64),
        key_gain.reshape(1, 64),
        forget_bias.reshape(1, 16),
        expert_choice.T,
        route_weight.T,
        query_w,
        key_w,
        value_w,
        forget_w.T,
        cache_key.reshape(24, 64, 1024),
        cache_value.reshape(24, 64, 1024),
        cache_gate,
        out_w,
        dense_gate_w,
        dense_up_w,
        dense_down_w,
        expert_gate_w.reshape(2048, 512),
        expert_up_w.reshape(2048, 512),
        expert_down_w.reshape(512, 2048),
    )
    mixed, fresh_key, fresh_value, fresh_gate = finish(
        mixed.reshape(24, 1024), fresh_key, fresh_value, fresh_gate
    )
    return (
        mixed,
        fresh_key.reshape(24, 1, 64),
        fresh_value.reshape(24, 1, 64),
        fresh_gate.T,
    )


def solution(mesh):
    placed = (
        P("ep", None),
        P(),
        P(None, "tp"),
        P(),
        P(),
        P(),
        P(),
        P(),
        P(),
        P("ep", "tp", None, None),
        P("ep", "tp", None, None),
        P("ep", "tp", None),
        P("ep"),
        P("tp", None),
        P(),
        P(),
        P(None, ("ep", "tp")),
        P(None, ("ep", "tp")),
        P(("ep", "tp"), None),
        P("ep", None),
        P("ep", None),
        P("ep", None, "tp"),
        P("ep", None, "tp"),
        P("ep", "tp", None),
    )
    return jax.shard_map(
        body,
        mesh=mesh,
        in_specs=placed,
        out_specs=(P("ep", "tp"), P("ep", "tp", None), P("ep", "tp", None), P("ep", "tp")),
        check_vma=False,
    )
```

```python
import math
import functools

import jax
import jax.numpy as jnp
from jax import lax
from jax.experimental import pallas as pl
from jax.experimental.pallas import tpu as pltpu
from jax.sharding import PartitionSpec as P

FF2 = 16384
norm_eps = 1e-06
GROUP = 8
MESH = pl.DeviceIdType.MESH
f32, bf16 = jnp.float32, jnp.bfloat16


class Sems:
    def __init__(self, send, recv):
        self.send, self.recv, self.n = send, recv, 0
        self.sent = []

    def copy(self, src, dst, device):
        i = self.n
        self.n += 1
        cp = pltpu.make_async_remote_copy(
            src_ref=src,
            dst_ref=dst,
            send_sem=self.send.at[i],
            recv_sem=self.recv.at[i],
            device_id=device,
            device_id_type=MESH,
        )
        cp.start()
        self.sent.append(cp)
        return cp


def silu(v):
    return v / (1.0 + jnp.exp(-v))


def layer_kernel(
    len_ref, tokens_h, ngain_h, pgain_h, bgate_h, qgain_h, kgain_h, fbias_h, choice_h, rweight_h,
    qw_h, kw_h, vw_h, fw_h, kc_h, vc_h, cg_h, ow_h,
    dg_h, du_h, dd_h, eg_h, eu_h, ed_h,
    out_ref, fk_ref, fv_ref, fg_ref,
    tok_s, ngain_s, pgain_s, bgate_s, qgain_s, kgain_s, fbias_s, choice_s, rweight_s,
    qw, kw, vw, fw, kc, vc, cg, ow, rows_s, q_s, kf_s, vf_s, o_s, ah_s, comb_s,
    partial_s, partner_part, resid_s, pn_s, a1, xs, hid, wgu, wd, eg, eu, ed,
    meta_all, meta_tab, xg, dens, rl, rr, ql, qr, sl, sr, t2, r2, t3, r3,
    sq, sq1, sq2, sq2r, sq3, sq3r, ep_send, ep_recv, ret_f, ret_b, back,
    send_sem, recv_sem, load_sem, small_sem, cache_sem, back_sems,
):
    me = lax.axis_index("ep")
    core = lax.axis_index("tp")
    other = 1 - core
    coords = (me % 4, (me // 4) % 4, me // 16)
    weights = (1, 4, 16)
    partner = (me, other)
    half = pl.multiple_of(core * 1024, 1024)
    ohalf = pl.multiple_of(other * 1024, 1024)
    ccol = pl.multiple_of(core * 128, 128)

    def peer(dim, k):
        v = coords[dim]
        return (me + (((v + k) % 4) - v) * weights[dim], core)

    sems = Sems(send_sem, recv_sem)

    barrier = pltpu.get_barrier_semaphore()
    pl.semaphore_signal(barrier, inc=1, device_id=partner, device_id_type=MESH)

    for dim in range(3):
        for k in (1, 2, 3):
            pl.semaphore_signal(barrier, inc=1, device_id=peer(dim, k), device_id_type=MESH)

    smalls = []
    for i, (src, dst) in enumerate((
        (tokens_h, tok_s), (ngain_h, ngain_s), (choice_h, choice_s), (rweight_h, rweight_s),
        (qw_h, qw), (kw_h, kw), (vw_h, vw), (fw_h, fw), (fbias_h, fbias_s),
        (qgain_h, qgain_s), (kgain_h, kgain_s), (pgain_h, pgain_s), (bgate_h, bgate_s),
    )):
        cp = pltpu.make_async_copy(src, dst, small_sem.at[i])
        cp.start()
        smalls.append(cp)

    def cache_copies(g):
        rows = pl.ds(g * GROUP, GROUP)
        return [
            pltpu.make_async_copy(src.at[rows], dst.at[rows], cache_sem.at[i, g])
            for i, (src, dst) in enumerate(((kc_h, kc), (cg_h, cg), (vc_h, vc)))
        ]

    loads = []
    for i, (src, dst) in enumerate((
        (dg_h, wgu.at[:, pl.ds(0, 128)]),
        (du_h, wgu.at[:, pl.ds(128, 128)]),
        (dd_h.at[:, pl.ds(half, 1024)], wd.at[pl.ds(ccol, 128)]),
        (eg_h, eg),
        (eu_h, eu),
        (ed_h, ed),
        (ow_h, ow),
    )):
        loads.append(pltpu.make_async_copy(src, dst, load_sem.at[i]))
    smalls[4].wait()
    for g in range(24 // GROUP):
        for cp in cache_copies(g):
            cp.start()
    loads[6].start()

    for i in (1, 11, 12):
        smalls[i].wait()
    for i, src in enumerate((ngain_s, pgain_s, bgate_s)):
        v = src[...].astype(f32)
        for t in range(16):
            rows_s[pl.ds(i, 1), pl.ds(t * 128, 128)] = v[t:t + 1]
    smalls[0].wait()
    toks = tok_s[...].astype(f32)
    mean_square = jnp.mean(toks * toks, axis=-1, keepdims=True)
    normed = (toks * lax.rsqrt(mean_square + norm_eps) * rows_s[pl.ds(0, 1), :]).astype(bf16)

    def head_norm(v, gain):
        return v * lax.rsqrt(jnp.mean(v * v, axis=-1, keepdims=True) + norm_eps) * gain

    q_all = jnp.dot(normed, qw[...], preferred_element_type=f32)
    smalls[9].wait()
    qg = qgain_s[...].astype(f32)
    for h in range(8):
        q = head_norm(q_all[:, h * 64:(h + 1) * 64], qg).astype(bf16).astype(f32)
        q_s[pl.ds(h, 24, stride=8), :] = jnp.concatenate([q, jnp.zeros_like(q)], axis=1)
    smalls[5].wait()
    smalls[10].wait()
    k_all = jnp.dot(normed, kw[...], preferred_element_type=f32)
    k_own = head_norm(jnp.where(core == 0, k_all[:, :64], k_all[:, 64:]), kgain_s[...].astype(f32))
    fk_ref[...] = k_own.astype(bf16)
    kf_s[...] = k_own.astype(bf16).astype(f32)
    smalls[6].wait()
    v_all = jnp.dot(normed, vw[...], preferred_element_type=f32)
    v_own = jnp.where(core == 0, v_all[:, :64], v_all[:, 64:]).astype(bf16)
    fv_ref[...] = v_own
    vf_s[...] = v_own.astype(f32)
    smalls[7].wait()
    smalls[8].wait()
    forget = lax.dot_general(
        fw[...], normed, (((1,), (1,)), ((), ())), preferred_element_type=f32
    )
    pick16 = lax.broadcasted_iota(jnp.int32, (16, 16), 0) == lax.broadcasted_iota(jnp.int32, (16, 16), 1)
    forget = forget + jnp.sum(jnp.where(pick16, fbias_s[...], 0.0), axis=1, keepdims=True)
    log_forget = jnp.minimum(forget, 0.0) - jnp.log1p(jnp.exp(-jnp.abs(forget)))
    log_forget = jnp.where(core == 0, log_forget[:8], log_forget[8:])

    slot_at = lax.broadcasted_iota(jnp.int32, (8, 1024), 1)
    seq_lane = lax.broadcasted_iota(jnp.int32, (8, 24), 1)
    scale = 64 ** (-0.5)

    def score_group(g, gates):
        for cp in cache_copies(g):
            cp.wait()
        for i in range(GROUP):
            s = g * GROUP + i
            rows = pl.ds(pl.multiple_of(s * 8, 8), 8)
            length = len_ref[s]
            q = q_s[rows, :][:, :64]
            score = jnp.dot(q.astype(bf16), kc[s], preferred_element_type=f32) * scale
            gate = cg[s]
            current = jnp.sum(jnp.where(slot_at == length - 1, gate, 0.0), axis=1, keepdims=True)
            current = current + jnp.sum(
                jnp.where(seq_lane == s, log_forget, 0.0), axis=1, keepdims=True
            )
            gates = jnp.where(seq_lane == s, current, gates)
            own = jnp.sum(q * kf_s[pl.ds(s, 1), :], axis=1, keepdims=True) * scale
            logit = jnp.where(slot_at < length, score + (current - gate), -jnp.inf)
            top = jnp.maximum(jnp.max(logit, axis=1, keepdims=True), own)
            cg[s] = logit - top
            o_s[rows, :] = jnp.broadcast_to(own - top, (8, 128))
        return gates

    def mix_group(g, carry):
        for i in range(GROUP):
            s = g * GROUP + i
            rows = pl.ds(pl.multiple_of(s * 8, 8), 8)
            w = jnp.exp(cg[s])
            own_w = jnp.exp(o_s[rows, :][:, :64])
            inv = 1.0 / (jnp.sum(w, axis=1, keepdims=True) + own_w)
            o = lax.dot_general(
                w.astype(bf16), vc[s], (((1,), (1,)), ((), ())), preferred_element_type=f32
            )
            o = (o + own_w.astype(bf16).astype(f32) * vf_s[pl.ds(s, 1), :]) * inv
            o_s[rows, :] = jnp.concatenate([o, jnp.zeros_like(o)], axis=1)
        return carry

    gates = lax.fori_loop(0, 24 // GROUP, score_group, jnp.zeros((8, 24), f32))
    lax.fori_loop(0, 24 // GROUP, mix_group, 0)
    fg_ref[...] = gates
    for cp in loads[:6]:
        cp.start()
    for h in range(8):
        ah_s[:, pl.ds(h * 64, 64)] = o_s[pl.ds(h, 24, stride=8), :][:, :64]
    loads[6].wait()
    partial = jnp.dot(ah_s[...].astype(bf16), ow[...], preferred_element_type=f32)
    partial_s[...] = partial.reshape(3, 8, 2048).astype(bf16)

    pl.semaphore_wait(barrier, 10)

    part_cp = sems.copy(partial_s, partner_part, partner)
    wd_cp = sems.copy(dd_h.at[:, pl.ds(ohalf, 1024)], wd.at[pl.ds(ccol, 128)], partner)

    meta_all[0] = jnp.full((1, 128), -1.0, f32)

    def column(row):
        pick = lax.broadcasted_iota(jnp.int32, (24, 24), 0) == lax.broadcasted_iota(jnp.int32, (24, 24), 1)
        return jnp.sum(jnp.where(pick, row, jnp.zeros_like(row)), axis=1, keepdims=True)

    smalls[2].wait()
    smalls[3].wait()
    choice = choice_s[...].astype(f32)
    named = [choice[k:k + 1, :] for k in range(2)]
    named_col = [column(v) for v in named]
    earlier = lax.broadcasted_iota(jnp.int32, (24, 24), 0) < lax.broadcasted_iota(jnp.int32, (24, 24), 1)
    targets = []
    for k in range(2):
        again = jnp.zeros((1, 24), f32)
        for i in range(2):
            same = jnp.where(earlier & (named_col[i] == named[k]), 1.0, 0.0)
            again = again + jnp.sum(same, axis=0, keepdims=True)
        targets.append(named[k] * 2.0 + jnp.minimum(again, 1.0))
    meta_all[0, :, pl.ds(0, 24)] = targets[0] + 128.0 * targets[1]
    target_col = [column(v) for v in targets]
    weight_col = [column(rweight_s[k:k + 1, :]) for k in range(2)]
    place = lax.broadcasted_iota(jnp.int32, (24, 64), 1).astype(f32) * 2.0
    for t in range(2):
        m = jnp.where(target_col[0] == place + t, weight_col[0], 0.0)
        comb_s[t] = m + jnp.where(target_col[1] == place + t, weight_col[1], 0.0)

    part_cp.wait_recv()
    attn = partial_s[...].astype(f32) + partner_part[...].astype(f32)
    resid = (tok_s[...].astype(f32).reshape(3, 8, 2048) + attn).astype(bf16).astype(f32)
    resid_s[...] = resid
    mean_square = jnp.mean(resid * resid, axis=-1, keepdims=True)
    gain = rows_s[pl.ds(1, 1), :][None]
    post = (resid * lax.rsqrt(mean_square + norm_eps) * gain).astype(bf16)
    pn_s[...] = post
    a1[:, 0] = pn_s[:, :, pl.ds(half, 1024)]

    def meta_stage(dim, size):
        return [
            sems.copy(meta_all.at[pl.ds(0, size)], meta_all.at[pl.ds((4 - k) * size, size)], peer(dim, k))
            for k in (1, 3, 2)
        ]

    meta_cp = meta_stage(0, 1)
    g1 = [
        [sems.copy(a1.at[p, 0], a1.at[p, 4 - k], peer(p, k)) for k in (1, 3, 2)]
        for p in range(3)
    ]

    branch = jax.nn.sigmoid(
        jnp.sum(post.astype(f32) * rows_s[pl.ds(2, 1), :][None], axis=-1, keepdims=True)
    )

    g2 = []
    for p in range(3):
        if p == 0:
            for cp in meta_cp:
                cp.wait_recv()
            meta_cp = meta_stage(1, 4)
        for cp in g1[p]:
            cp.wait_recv()
        for pair in range(2):
            rows = jnp.concatenate(
                [a1[p, 2 * pair].astype(f32), a1[p, 2 * pair + 1].astype(f32)], axis=0
            )
            xs[core, 0, pl.ds(p * 128 + pair * 16, 16)] = rows.astype(bf16)
        line = xs.at[core, 0, pl.ds(p * 128, 32)]
        g2.append([
            sems.copy(line, xs.at[core, 0, pl.ds(p * 128 + (4 - k) * 32, 32)], peer((p + 1) % 3, k))
            for k in (1, 3, 2)
        ])

    g3, d2d = [], [[] for _ in range(4)]

    def share(slot, p, start, size):
        view = xs.at[core, slot, pl.ds(p * 128 + start, size)]
        d2d[slot].append(sems.copy(view, view, partner))

    lo, hi = (lambda p: pl.ds(p * 128, 64)), (lambda p: pl.ds(p * 128 + 64, 64))
    first, second = (lambda p: pl.ds(p * 128, 32)), (lambda p: pl.ds(p * 128 + 32, 32))
    own = xs.at[core, 0]
    early = [
        [
            sems.copy(own.at[first(p)], xs.at[core, slot, first(p)], peer((p + 2) % 3, k))
            for slot, k in ((1, 1), (2, 3))
        ]
        for p in range(3)
    ]
    for p in range(3):
        if p == 0:
            for cp in meta_cp:
                cp.wait_recv()
            meta_cp = meta_stage(2, 16)
        for cp in g2[p]:
            cp.wait_recv()
        cdim = (p + 2) % 3
        g3.append([
            sems.copy(own.at[rows], xs.at[core, slot, rows], peer(cdim, k))
            for slot, k, rows in ((1, 1, second(p)), (2, 3, hi(p)), (1, 1, hi(p)), (2, 3, second(p)))
        ])
        share(0, p, 0, 128)

    for cp in meta_cp:
        cp.wait_recv()
    for d in range(64):
        meta_tab[pl.ds(d, 1), :] = meta_all[d]
    table = meta_tab[...].astype(jnp.int32)
    lane = lax.broadcasted_iota(jnp.int32, (64, 128), 1)
    dev = lax.broadcasted_iota(jnp.int32, (64, 1), 0)
    shift = [(dev >> s) & 3 for s in (0, 2, 4)]
    starts = []
    for p in range(3):
        ka, kb, kc = shift[p], shift[(p + 1) % 3], shift[(p + 2) % 3]
        slot = jnp.where(kc == 0, 0, jnp.where(kc == 1, 2, jnp.where(kc == 2, 3, 1)))
        starts.append(slot * 384 + p * 128 + kb * 32 + ka * 8)
    row_ids = []
    for s in range(2):
        want = me * 2 + s
        hit = (lane < 24) & (((table & 127) == want) | ((table >> 7) == want))
        tok = jnp.sum(jnp.where(hit, lane + 1, 0), axis=1, keepdims=True) - 1
        start = jnp.where(tok < 8, starts[0], jnp.where(tok < 16, starts[1], starts[2]))
        row_ids.append(jnp.where(tok < 0, -1, start + (tok & 7)))
    row_id = jnp.concatenate(row_ids, axis=0)
    cols = lax.broadcasted_iota(jnp.int32, (128, 384), 1)

    def select(slot):
        pick = jnp.where(row_id == cols + slot * 384, 1.0, 0.0).astype(bf16)
        for h in range(2):
            got = jnp.dot(pick, xs[h, slot], preferred_element_type=f32)
            if slot:
                got = xg[h] + got
            xg[h] = got

    h_cp = [None] * 4

    def half_up(h, slot, rows):
        w = wgu[pl.ds(pl.multiple_of(h * 1024, 1024), 1024)]
        return jnp.dot(xs[h, slot, rows], w, preferred_element_type=f32)

    def own_up(slot):
        return half_up(core, slot, pl.ds(0, 384))

    def up_proj(slot, v):
        v = v + half_up(other, slot, pl.ds(0, 384))
        hid[slot, :, pl.ds(ccol, 128)] = (silu(v[:, :128]) * v[:, 128:]).astype(bf16)
        view = hid.at[slot, :, pl.ds(ccol, 128)]
        h_cp[slot] = sems.copy(view, view, partner)

    ones = jnp.ones((8, 256), bf16)

    def far_up(p, v):
        rows = pl.ds(p * 128, 128)
        v = v + half_up(other, 3, rows)
        hid[3, rows, pl.ds(ccol, 128)] = (silu(v[:, :128]) * v[:, 128:]).astype(bf16)
        view = hid.at[3, rows, pl.ds(ccol, 128)]
        return sems.copy(view, view, partner)

    def down_proj(slot):
        h_cp[slot].wait_recv()
        dens[slot] = jnp.dot(hid[slot], wd[...], preferred_element_type=f32).astype(bf16)

    def squares(slot):
        hf = hid[slot].astype(f32)
        s = lax.dot_general(
            ones, (hf * hf).astype(bf16), (((1,), (1,)), ((), ())), preferred_element_type=f32
        )
        for p in range(3):
            sq[slot, p] = s[0:1, p * 128:(p + 1) * 128]

    def arrive(slot):
        for cp in d2d[slot]:
            cp.wait_recv()

    loads[0].wait()
    loads[1].wait()
    v0 = own_up(0)
    arrive(0)
    up_proj(0, v0)
    select(0)

    relay = []
    for p in range(3):
        cdim = (p + 2) % 3
        early[p][0].wait_recv()
        g3[p][0].wait_recv()
        relay.append(sems.copy(xs.at[core, 1, lo(p)], xs.at[core, 3, lo(p)], peer(cdim, 1)))
        g3[p][1].wait_recv()
        relay.append(sems.copy(xs.at[core, 2, hi(p)], xs.at[core, 3, hi(p)], peer(cdim, 3)))
        share(1, p, 0, 64)
        share(2, p, 64, 64)
    for p in range(3):
        g3[p][2].wait_recv()
        share(1, p, 64, 64)
        early[p][1].wait_recv()
        g3[p][3].wait_recv()
        share(2, p, 0, 64)

    v1, v2 = own_up(1), own_up(2)
    arrive(1)
    up_proj(1, v1)
    arrive(2)
    up_proj(2, v2)
    loads[2].wait()
    wd_cp.wait_recv()
    down_proj(1)
    for p in range(3):
        relay[2 * p].wait_recv()
        share(3, p, 0, 64)
        relay[2 * p + 1].wait_recv()
        share(3, p, 64, 64)
    down_proj(2)

    s1 = []
    for p in range(3):
        cdim = (p + 2) % 3
        s1.append([
            sems.copy(dens.at[2, hi(p)], rl.at[p, hi(0)], peer(cdim, 1)),
            sems.copy(dens.at[1, lo(p)], rr.at[p, lo(0)], peer(cdim, 3)),
        ])

    far_cp = []
    far_own = [half_up(core, 3, pl.ds(p * 128, 128)) for p in range(3)]
    for p in range(3):
        for cp in d2d[3][2 * p:2 * p + 2]:
            cp.wait_recv()
        far_cp.append(far_up(p, far_own[p]))
    select(1)
    select(2)
    far = []
    for p in range(3):
        cdim = (p + 2) % 3
        far_cp[p].wait_recv()
        rows = pl.ds(p * 128, 128)
        dens[3, rows] = jnp.dot(hid[3, rows], wd[...], preferred_element_type=f32).astype(bf16)
        far.append([
            sems.copy(dens.at[3, pl.ds(p * 128 + q * 32, 32)], buf.at[p, q % 2], peer(cdim, k))
            for q, buf, k in ((1, ql, 1), (2, qr, 3), (0, ql, 1), (3, qr, 3))
        ])
    select(3)
    for slot in (1, 2, 3):
        squares(slot)
    for p in range(3):
        cdim = (p + 2) % 3
        s1[p] += [
            sems.copy(sq.at[2, p], sq1.at[p, 0], peer(cdim, 1)),
            sems.copy(sq.at[1, p], sq1.at[p, 1], peer(cdim, 3)),
            sems.copy(sq.at[3, p], sq1.at[p, 2], peer(cdim, 2)),
        ]

    for i in (3, 4, 5):
        loads[i].wait()
    x0, x1 = xg[0].astype(bf16), xg[1].astype(bf16)
    gate = jnp.dot(x0, eg[pl.ds(0, 1024)], preferred_element_type=f32)
    gate = gate + jnp.dot(x1, eg[pl.ds(1024, 1024)], preferred_element_type=f32)
    up = jnp.dot(x0, eu[pl.ds(0, 1024)], preferred_element_type=f32)
    up = up + jnp.dot(x1, eu[pl.ds(1024, 1024)], preferred_element_type=f32)
    act = (silu(gate) * up).astype(bf16)
    ep_send[...] = jnp.dot(act, ed[:, pl.ds(ohalf, 1024)], preferred_element_type=f32).astype(bf16)
    ep_cp = sems.copy(ep_send, ep_recv, partner)
    mine = jnp.dot(act, ed[:, pl.ds(half, 1024)], preferred_element_type=f32).astype(bf16)

    down_proj(0)
    squares(0)

    sums = [[None] * 4 for _ in range(3)]
    for i, (q, near, came, out, to, k) in enumerate((
        (1, 2, ql, sl, rl, 1), (2, 1, qr, sr, rr, 3), (0, 2, ql, sl, rl, 1), (3, 1, qr, sr, rr, 3)
    )):
        for p in range(3):
            far[p][i].wait_recv()
            mix = dens[near, pl.ds(p * 128 + q * 32, 32)].astype(f32) + came[p, q % 2].astype(f32)
            out[p, q % 2] = mix.astype(bf16)
            sums[p][q] = sems.copy(
                out.at[p, q % 2], to.at[p, pl.ds(q * 32, 32)], peer((p + 2) % 3, k)
            )

    ep_cp.wait_recv()
    rows = (mine.astype(f32) + ep_recv[...].astype(f32)).astype(bf16).astype(f32)
    for s in range(2):
        for t in range(8):
            ret_f[pl.ds(s * 8 + t, 64, stride=16), :] = rows[s * 64:(s + 1) * 64, t * 128:(t + 1) * 128]
    ret_b[...] = ret_f[...].astype(bf16).reshape(64, 16, 128)

    s2 = [[] for _ in range(3)]
    for p in range(3):
        for cp in s1[p]:
            cp.wait_recv()
        v = sq[0, p] + sq1[p, 0] + sq1[p, 1] + sq1[p, 2]
        sq2[p, 0] = v
        for k in range(1, 4):
            sq2[p, k] = pltpu.roll(v, 128 - 32 * k, 1)
            s2[p].append(sems.copy(sq2.at[p, k], sq2r.at[p, k - 1], peer((p + 1) % 3, k)))
    for q in (2, 1, 3, 0):
        for p in range(3):
            sums[p][q].wait_recv()
            rows = pl.ds(q * 32, 32)
            total = dens[0, pl.ds(p * 128 + q * 32, 32)].astype(f32)
            total = total + rl[p, rows].astype(f32) + rr[p, rows].astype(f32)
            t2[p, q] = total.astype(bf16)
            if q:
                s2[p].append(sems.copy(t2.at[p, q], r2.at[p, q - 1], peer((p + 1) % 3, q)))

    @pl.loop(1, 64)
    def _(i):
        owner = (coords[0] + i % 4) % 4 + (coords[1] + (i // 4) % 4) % 4 * 4 + (coords[2] + i // 16) % 4 * 16
        pltpu.make_async_remote_copy(
            src_ref=ret_b.at[i],
            dst_ref=back.at[me],
            send_sem=back_sems.at[0],
            recv_sem=back_sems.at[1],
            device_id=(owner, core),
            device_id_type=MESH,
        ).start()

    back[me] = ret_b[0]
    s3 = []
    for p in range(3):
        for cp in s2[p]:
            cp.wait_recv()
        total = t2[p, 0].astype(f32)
        for k in range(3):
            total = total + r2[p, k].astype(f32)
        for k in range(4):
            t3[p, k] = total[k * 8:(k + 1) * 8].astype(bf16)
        v = sq2[p, 0] + sq2r[p, 0] + sq2r[p, 1] + sq2r[p, 2]
        sq3[p, 0] = v
        for k in range(1, 4):
            sq3[p, k] = pltpu.roll(v, 128 - 8 * k, 1)
        s3.append([
            sems.copy(t3.at[p, k], r3.at[p, k - 1], peer(p, k)) for k in (1, 3, 2)
        ] + [
            sems.copy(sq3.at[p, k], sq3r.at[p, k - 1], peer(p, k)) for k in (1, 3, 2)
        ])

    pltpu.make_async_copy(back.at[pl.ds(0, 63)], back.at[pl.ds(0, 63)], back_sems.at[1]).wait()
    ret_f[...] = back[...].reshape(1024, 128).astype(f32)
    mixes = []
    for t in range(8):
        m = 0.0
        for s in range(2):
            m = m + jnp.dot(
                comb_s[s], ret_f[pl.ds(s * 8 + t, 64, stride=16), :],
                preferred_element_type=f32, precision=lax.Precision.HIGHEST,
            )
        mixes.append(m)
    expert_sum = jnp.concatenate(mixes, axis=1)

    eye = lax.broadcasted_iota(jnp.int32, (8, 128), 0) == lax.broadcasted_iota(jnp.int32, (8, 128), 1)
    for p in range(3):
        for cp in s3[p]:
            cp.wait_recv()
        total = t3[p, 0].astype(f32)
        v = sq3[p, 0]
        for k in range(3):
            total = total + r3[p, k].astype(f32)
            v = v + sq3r[p, k]
        square = jnp.sum(jnp.where(eye, v, 0.0), axis=1, keepdims=True)
        dense = (total * lax.rsqrt(square / FF2 + norm_eps)).astype(bf16).astype(f32)
        mixed = resid_s[p, :, pl.ds(half, 1024)] + expert_sum[p * 8:(p + 1) * 8] + branch[p] * dense
        out_ref[p] = mixed.astype(bf16)

    for cp in sems.sent:
        cp.wait_send()
    pltpu.make_async_copy(back.at[pl.ds(0, 63)], back.at[pl.ds(0, 63)], back_sems.at[0]).wait()


def fused_layer(lens, *args):
    V = pltpu.VMEM
    vm = pl.BlockSpec(memory_space=pltpu.VMEM)
    hbm = pl.BlockSpec(memory_space=pl.ANY)
    scratch = [
        V((24, 2048), bf16),
        V((16, 128), bf16),
        V((16, 128), bf16),
        V((16, 128), bf16),
        V((1, 64), bf16),
        V((1, 64), bf16),
        V((1, 16), f32),
        V((2, 24), jnp.int32),
        V((2, 24), f32),
        V((2048, 512), bf16),
        V((2048, 128), bf16),
        V((2048, 128), bf16),
        V((16, 2048), bf16),
        V((24, 64, 1024), bf16),
        V((24, 64, 1024), bf16),
        V((24, 8, 1024), f32),
        V((512, 2048), bf16),
        V((8, 2048), f32),
        V((192, 128), f32),
        V((24, 64), f32),
        V((24, 64), f32),
        V((192, 128), f32),
        V((24, 512), f32),
        V((2, 24, 64), f32),
        V((3, 8, 2048), bf16),
        V((3, 8, 2048), bf16),
        V((3, 8, 2048), f32),
        V((3, 8, 2048), bf16),
        V((3, 4, 8, 1024), bf16),
        V((2, 4, 384, 1024), bf16),
        V((4, 384, 256), bf16),
        V((2048, 256), bf16),
        V((256, 1024), bf16),
        V((2048, 512), bf16),
        V((2048, 512), bf16),
        V((512, 2048), bf16),
        V((64, 1, 128), f32),
        V((64, 128), f32),
        V((2, 128, 1024), f32),
        V((4, 384, 1024), bf16),
        V((3, 128, 1024), bf16),
        V((3, 128, 1024), bf16),
        V((3, 2, 32, 1024), bf16),
        V((3, 2, 32, 1024), bf16),
        V((3, 2, 32, 1024), bf16),
        V((3, 2, 32, 1024), bf16),
        V((3, 4, 32, 1024), bf16),
        V((3, 3, 32, 1024), bf16),
        V((3, 4, 8, 1024), bf16),
        V((3, 3, 8, 1024), bf16),
        V((4, 3, 1, 128), f32),
        V((3, 3, 1, 128), f32),
        V((3, 4, 1, 128), f32),
        V((3, 3, 1, 128), f32),
        V((3, 4, 1, 128), f32),
        V((3, 3, 1, 128), f32),
        V((128, 1024), bf16),
        V((128, 1024), bf16),
        V((1024, 128), f32),
        V((64, 16, 128), bf16),
        V((64, 16, 128), bf16),
        pltpu.SemaphoreType.DMA((192,)),
        pltpu.SemaphoreType.DMA((192,)),
        pltpu.SemaphoreType.DMA((7,)),
        pltpu.SemaphoreType.DMA((13,)),
        pltpu.SemaphoreType.DMA((3, 24 // GROUP)),
        pltpu.SemaphoreType.DMA((2,)),
    ]
    return pl.pallas_call(
        layer_kernel,
        out_shape=(
            jax.ShapeDtypeStruct((3, 8, 1024), bf16),
            jax.ShapeDtypeStruct((24, 64), bf16),
            jax.ShapeDtypeStruct((24, 64), bf16),
            jax.ShapeDtypeStruct((8, 24), f32),
        ),
        in_specs=[pl.BlockSpec(memory_space=pltpu.SMEM)] + [hbm] * len(args),
        out_specs=(vm,) * 4,
        scratch_shapes=scratch,
        compiler_params=pltpu.CompilerParams(
            collective_id=0, has_side_effects=True, vmem_limit_bytes=56 * 1024 * 1024
        ),
    )(lens, *args)


def finish(*arrays):
    def kernel(*refs):
        for src, dst in zip(refs[:4], refs[4:]):
            dst[...] = src[...]

    return pl.pallas_call(
        kernel,
        out_shape=tuple(jax.ShapeDtypeStruct(a.shape, a.dtype) for a in arrays),
        in_specs=[pl.BlockSpec(memory_space=pltpu.VMEM)] * 4,
        out_specs=(pl.BlockSpec(memory_space=pltpu.VMEM),) * 4,
    )(*arrays)


def body(
    tokens,
    norm_gain,
    query_w,
    key_w,
    value_w,
    forget_w,
    forget_bias,
    query_gain,
    key_gain,
    cache_key,
    cache_value,
    cache_gate,
    cache_len,
    out_w,
    post_gain,
    branch_gate,
    dense_gate_w,
    dense_up_w,
    dense_down_w,
    expert_choice,
    route_weight,
    expert_gate_w,
    expert_up_w,
    expert_down_w,
):
    mixed, fresh_key, fresh_value, fresh_gate = fused_layer(
        cache_len,
        tokens,
        norm_gain.reshape(16, 128),
        post_gain.reshape(16, 128),
        branch_gate.reshape(16, 128),
        query_gain.reshape(1, 64),
        key_gain.reshape(1, 64),
        forget_bias.reshape(1, 16),
        expert_choice.T,
        route_weight.T,
        query_w,
        key_w,
        value_w,
        forget_w.T,
        cache_key.reshape(24, 64, 1024),
        cache_value.reshape(24, 64, 1024),
        cache_gate,
        out_w,
        dense_gate_w,
        dense_up_w,
        dense_down_w,
        expert_gate_w.reshape(2048, 512),
        expert_up_w.reshape(2048, 512),
        expert_down_w.reshape(512, 2048),
    )
    mixed, fresh_key, fresh_value, fresh_gate = finish(
        mixed.reshape(24, 1024), fresh_key, fresh_value, fresh_gate
    )
    return (
        mixed,
        fresh_key.reshape(24, 1, 64),
        fresh_value.reshape(24, 1, 64),
        fresh_gate.T,
    )


def solution(mesh):
    placed = (
        P("ep", None),
        P(),
        P(None, "tp"),
        P(),
        P(),
        P(),
        P(),
        P(),
        P(),
        P("ep", "tp", None, None),
        P("ep", "tp", None, None),
        P("ep", "tp", None),
        P("ep"),
        P("tp", None),
        P(),
        P(),
        P(None, ("ep", "tp")),
        P(None, ("ep", "tp")),
        P(("ep", "tp"), None),
        P("ep", None),
        P("ep", None),
        P("ep", None, "tp"),
        P("ep", None, "tp"),
        P("ep", "tp", None),
    )
    return jax.shard_map(
        body,
        mesh=mesh,
        in_specs=placed,
        out_specs=(P("ep", "tp"), P("ep", "tp", None), P("ep", "tp", None), P("ep", "tp")),
        check_vma=False,
    )
```
